256 devices in a mesh: sp: 32 (over z, x), tp: 8 (over y, core).
Axes of the slice: x: 4, y: 4, z: 8, core: 2. Of those that a mesh axis runs over, the one named last changes fastest.
Arguments:
- tokens: bfloat16 [12288, 2048], P(('sp', 'tp')), may hold values from -6 to 6
- norm_gain: bfloat16 [2048], replicated, may hold values from 0.099609375 to 1.8984375
- query_down_weight: bfloat16 [2048, 512], replicated, may hold values from -0.125 to 0.125
- query_latent_norm_gain: bfloat16 [512], replicated, may hold values from 0.099609375 to 1.8984375
- key_value_down_weight: bfloat16 [2048, 256], replicated, may hold values from -0.125 to 0.125
- key_value_latent_gain: bfloat16 [256], replicated, may hold values from 0.099609375 to 1.8984375
- w_rope_key: bfloat16 [2048, 32], replicated, may hold values from -0.125 to 0.125
- w_pool_in: bfloat16 [2048, 512], replicated, may hold values from -0.125 to 0.125
- query_up_weight: bfloat16 [512, 2304], P(None, 'tp'), may hold values from -0.25 to 0.25
- key_value_up_weight: bfloat16 [256, 3072], P(None, 'tp'), may hold values from -0.375 to 0.375
- query_gain: bfloat16 [96], replicated, may hold values from 1 to 16
- key_gain: bfloat16 [96], replicated, may hold values from 1 to 16
- w_pool_mix: bfloat16 [8, 64, 64], P('tp'), may hold values from -0.75 to 0.75
- pool_scale: bfloat16 [512], P('tp'), may hold values from 1 to 10
- w_out_attn: bfloat16 [1536, 2048], P('tp'), may hold values from -0.3125 to 0.3125
- w_out_pool: bfloat16 [512, 2048], P('tp'), may hold values from -0.25 to 0.25
Outputs:
- mixed: bfloat16 [12288, 2048], P(('sp', 'tp'))
- row_logsum: float32 [24, 12288], P('tp', 'sp')
The draws below stay inside these ranges and needn't reach their ends.
All inputs are finite; a program needn't handle non-finite values.
Results may differ from the reference program's by a relative error of at most 0.035.
Values may be sent and summed in bfloat16 or wider, within the bound.
No kernel may reach another device: no remote copies, remote signals or barrier semaphores. Data moves between devices by JAX's collectives and lax.ppermute only.
A program may use at most 128 MiB of HBM per device.

```python
import math
import jax
import jax.numpy as jnp
from jax import lax

MODEL_WIDTH = 2048
HEAD_COUNT = 24
PLAIN_HEAD_SIZE = 64
ROTARY_SIZE = 32
VALUE_HEAD_SIZE = 64
QUERY_RANK = 512
KEY_VALUE_RANK = 256
GROUPS = 8
GDIM = 64
TOKENS = 12288
N_TP = 8


def head_gain(key, salt):
    base = jax.random.uniform(jax.random.fold_in(key, salt), (PLAIN_HEAD_SIZE + ROTARY_SIZE,), jnp.float32, 1.0, 2.0)
    return base.astype(jnp.bfloat16)


def draw_query_gain(key, part):
    return head_gain(key, 1)


def draw_key_gain(key, part):
    return head_gain(key, 2)


def levels(rng, shape, split, least, high):
    level, own = 1.0, jax.random.fold_in(rng, 6)
    for dim, parts in split:
        draws = jnp.exp(jax.random.uniform(jax.random.fold_in(own, dim), (parts,), jnp.float32, least / len(split), high / len(split)))
        level = level * jnp.repeat(draws, shape[dim] // parts).reshape([-1 if axis == dim else 1 for axis in range(len(shape))])
    return level


def noise(rng, shape, spread, limit, split=(), held_as=jnp.bfloat16):
    level = levels(rng, shape, split, -0.22, 0.18) if split else 1.0
    values = jax.random.normal(rng, shape, jnp.float32) * spread * level
    return jnp.minimum(jnp.maximum(values, -limit), limit).astype(held_as)


def setup_inputs(seed: int = 0) -> dict:
    arg_keys = jax.random.split(jax.random.key(seed), 17)
    return {
        "tokens": noise(arg_keys[0], (TOKENS, MODEL_WIDTH), 1.0, 6.0, ((0, 256),)),
        "norm_gain": jnp.clip(1.0 + 0.18 * jax.random.normal(arg_keys[1], (MODEL_WIDTH,), jnp.float32), 0.099609375, 1.8984375).astype(jnp.bfloat16),
        "query_down_weight": noise(arg_keys[2], (MODEL_WIDTH, QUERY_RANK), MODEL_WIDTH ** -0.5, 0.125),
        "query_latent_norm_gain": jnp.clip(1.0 + 0.18 * jax.random.normal(arg_keys[3], (QUERY_RANK,), jnp.float32), 0.099609375, 1.8984375).astype(jnp.bfloat16),
        "key_value_down_weight": noise(arg_keys[4], (MODEL_WIDTH, KEY_VALUE_RANK), MODEL_WIDTH ** -0.5, 0.125),
        "key_value_latent_gain": jnp.clip(1.0 + 0.18 * jax.random.normal(arg_keys[5], (KEY_VALUE_RANK,), jnp.float32), 0.099609375, 1.8984375).astype(jnp.bfloat16),
        "w_rope_key": noise(arg_keys[6], (MODEL_WIDTH, ROTARY_SIZE), MODEL_WIDTH ** -0.5, 0.125),
        "w_pool_in": noise(arg_keys[7], (MODEL_WIDTH, GROUPS * GDIM), MODEL_WIDTH ** -0.5, 0.125),
        "query_up_weight": noise(arg_keys[8], (QUERY_RANK, HEAD_COUNT * (PLAIN_HEAD_SIZE + ROTARY_SIZE)), QUERY_RANK ** -0.5, 0.25, ((1, 8),)),
        "key_value_up_weight": noise(arg_keys[9], (KEY_VALUE_RANK, HEAD_COUNT * (PLAIN_HEAD_SIZE + VALUE_HEAD_SIZE)), KEY_VALUE_RANK ** -0.5, 0.375, ((1, 8),)),
        "query_gain": draw_query_gain(jax.random.fold_in(arg_keys[16], 71), 0),
        "key_gain": draw_key_gain(jax.random.fold_in(arg_keys[16], 71), 0),
        "w_pool_mix": noise(arg_keys[12], (GROUPS, GDIM, GDIM), GDIM ** -0.5, 0.75, ((0, 8),)),
        "pool_scale": jnp.clip(jnp.exp(math.log(10.0) - 2.3025851 * jax.random.uniform(arg_keys[13], (GROUPS * GDIM,), jnp.float32) ** levels(arg_keys[13], (GROUPS * GDIM,), ((0, 8),), -0.2, 0.2)), 1.0, 10.0).astype(jnp.bfloat16),
        "w_out_attn": noise(arg_keys[14], (HEAD_COUNT * VALUE_HEAD_SIZE, MODEL_WIDTH), (HEAD_COUNT * VALUE_HEAD_SIZE // 4) ** -0.5, 0.3125, ((0, 8),)),
        "w_out_pool": noise(arg_keys[15], (GROUPS * GDIM, MODEL_WIDTH), (GROUPS * GDIM) ** -0.5, 0.25, ((0, 8),)),
    }


epsilon = 1e-06
rope_base = 10000.0
query_rows = 128

def norm_rows(values, gain):
    mean_square = lax.optimization_barrier(jnp.mean(values * values, axis=-1, keepdims=True))
    return values * lax.rsqrt(mean_square + epsilon) * gain.astype(jnp.float32)

def rotate_tail(values, positions):
    half = ROTARY_SIZE // 2
    freqs = rope_base ** (-jnp.arange(half, dtype=jnp.float32) / half)
    angles = positions[:, None] * freqs[None, :]
    cosine = jnp.cos(angles)[:, None, :]
    sine = jnp.sin(angles)[:, None, :]
    first = values[..., PLAIN_HEAD_SIZE:PLAIN_HEAD_SIZE + half]
    second = values[..., PLAIN_HEAD_SIZE + half:]
    return jnp.concatenate([values[..., :PLAIN_HEAD_SIZE], first * cosine - second * sine, first * sine + second * cosine], axis=-1)

def reference(tokens, norm_gain, query_down_weight, query_latent_norm_gain, key_value_down_weight, key_value_latent_gain, w_rope_key, w_pool_in, query_up_weight, key_value_up_weight, query_gain, key_gain, w_pool_mix, pool_scale, w_out_attn, w_out_pool):
    length = tokens.shape[0]
    normed = norm_rows(tokens.astype(jnp.float32), norm_gain).astype(jnp.bfloat16)
    query_latent = norm_rows(jnp.dot(normed, query_down_weight, preferred_element_type=jnp.float32), query_latent_norm_gain).astype(jnp.bfloat16)
    kv_latent = norm_rows(jnp.dot(normed, key_value_down_weight, preferred_element_type=jnp.float32), key_value_latent_gain).astype(jnp.bfloat16)
    rope_key = jnp.dot(normed, w_rope_key, preferred_element_type=jnp.float32).astype(jnp.bfloat16)
    pool_input = jnp.dot(normed, w_pool_in, preferred_element_type=jnp.float32).astype(jnp.bfloat16)
    positions = jnp.arange(length, dtype=jnp.int32).astype(jnp.float32)
    query_vectors = jnp.dot(query_latent, query_up_weight, preferred_element_type=jnp.float32).reshape(length, HEAD_COUNT, PLAIN_HEAD_SIZE + ROTARY_SIZE)
    query_vectors = rotate_tail(norm_rows(query_vectors, query_gain), positions).astype(jnp.bfloat16)
    key_value_pair = jnp.dot(kv_latent, key_value_up_weight, preferred_element_type=jnp.float32).reshape(length, HEAD_COUNT, PLAIN_HEAD_SIZE + VALUE_HEAD_SIZE)
    shared = jnp.broadcast_to(rope_key.astype(jnp.float32)[:, None, :], (length, HEAD_COUNT, ROTARY_SIZE))
    keys = jnp.concatenate([key_value_pair[..., :PLAIN_HEAD_SIZE], shared], axis=-1)
    keys = rotate_tail(norm_rows(keys, key_gain), positions).astype(jnp.bfloat16)
    values = key_value_pair[..., PLAIN_HEAD_SIZE:].astype(jnp.bfloat16)
    scale = (PLAIN_HEAD_SIZE + ROTARY_SIZE) ** (-0.5)
    key_float = keys.astype(jnp.float32)
    value_float = values.astype(jnp.float32)
    query_blocks = query_vectors.astype(jnp.float32).reshape(length // query_rows, query_rows, HEAD_COUNT, PLAIN_HEAD_SIZE + ROTARY_SIZE)

    def attend(query_block):
        scores = jnp.einsum('qhd,khd->hqk', query_block, key_float) * scale
        row_max = lax.optimization_barrier(jnp.max(scores, axis=-1))
        exp_scores = jnp.exp(scores - row_max[:, :, None])
        row_total = lax.optimization_barrier(jnp.sum(exp_scores, axis=-1))
        weights = lax.optimization_barrier(exp_scores.astype(jnp.bfloat16)).astype(jnp.float32)
        summed = jnp.einsum('hqk,khd->qhd', weights, value_float)
        output = (summed / jnp.transpose(row_total)[:, :, None]).astype(jnp.bfloat16)
        return (output, row_max + jnp.log(row_total))
    outputs, logsums = lax.map(attend, query_blocks)
    attention = outputs.reshape(length, HEAD_COUNT * VALUE_HEAD_SIZE)
    row_logsum = jnp.transpose(logsums, (1, 0, 2)).reshape(HEAD_COUNT, length)
    pool_float = pool_input.astype(jnp.float32)
    running = jnp.concatenate([jnp.zeros((1, GROUPS * GDIM), jnp.float32), jnp.cumsum(pool_float, axis=0)], axis=0)
    places = jnp.arange(length, dtype=jnp.int32)
    pieces = []
    for group in range(GROUPS):
        half = 2 ** (group % 4)
        upper = jnp.minimum(places + half, length)
        lower = jnp.maximum(places - half, 0)
        first_col = group * GDIM
        window = running[upper, first_col:first_col + GDIM] - running[lower, first_col:first_col + GDIM]
        total_count = (upper - lower).astype(jnp.float32)[:, None]
        pooled = (window / total_count - pool_float[:, first_col:first_col + GDIM]).astype(jnp.bfloat16)
        mapped = jnp.dot(pooled, w_pool_mix[group], preferred_element_type=jnp.float32)
        pieces.append((mapped * pool_scale[first_col:first_col + GDIM].astype(jnp.float32)).astype(jnp.bfloat16))
    pool_out = jnp.concatenate(pieces, axis=1)
    head_cols = HEAD_COUNT * VALUE_HEAD_SIZE // N_TP
    pool_cols = GROUPS * GDIM // N_TP
    mixed = jnp.zeros((length, MODEL_WIDTH), jnp.float32)
    for member in range(N_TP):
        head_start = member * head_cols
        pool_start = member * pool_cols
        partial_sum = jnp.dot(attention[:, head_start:head_start + head_cols], w_out_attn[head_start:head_start + head_cols], preferred_element_type=jnp.float32)
        partial_sum = partial_sum + jnp.dot(pool_out[:, pool_start:pool_start + pool_cols], w_out_pool[pool_start:pool_start + pool_cols], preferred_element_type=jnp.float32)
        mixed = mixed + lax.optimization_barrier(partial_sum.astype(jnp.bfloat16)).astype(jnp.float32)
    return (mixed.astype(jnp.bfloat16), row_logsum)
```

```python
import jax
import jax.numpy as jnp
import numpy as np
from jax import lax
from jax.experimental import pallas as pl
from jax.experimental.pallas import tpu as pltpu
from jax.sharding import Mesh, PartitionSpec as P

NOPE = 64
ROT = 32
HALF = 16
HEAD = 96
VAL = 64
HEADS = 3
QR = 512
KR = 256
EPS = 1e-06
WIDTH = 2048
ROWS = 48
BLOCK = 384
SIDE = 192
TOKENS = 12288
LOG2E = 1.4426950408889634
LN2 = 0.6931471805599453
MSG = 208
VROWS = 80
QTILE = 512
NX = 4
NY = 4
NZ = 8
NQ = NX * BLOCK

bf16 = jnp.bfloat16
f32 = jnp.float32

COFF = None


def trig_tables():
    freqs = 10000.0 ** (-np.arange(HALF, dtype=np.float64) / HALF)
    inner = freqs[:, None] * np.arange(BLOCK, dtype=np.float64)[None, :]
    outer = freqs[:, None] * (BLOCK * np.arange(NZ * NX, dtype=np.float64))[None, :]
    pad = np.zeros((HALF, 128 - NZ * NX))
    cast = lambda a: a.astype(np.float32)
    return (
        cast(np.cos(inner)),
        cast(np.sin(inner)),
        cast(np.concatenate([np.cos(outer), pad], 1)),
        cast(np.concatenate([np.sin(outer), pad], 1)),
    )


def vmem():
    return pl.BlockSpec(memory_space=pltpu.VMEM)


def smem():
    return pl.BlockSpec(memory_space=pltpu.SMEM)


def nt(a, b):
    return lax.dot_general(a, b, (((1,), (1,)), ((), ())), preferred_element_type=f32)


def nn(a, b):
    return lax.dot_general(a, b, (((1,), (0,)), ((), ())), preferred_element_type=f32)


def params(**kw):
    return pltpu.CompilerParams(vmem_limit_bytes=56 * 1024 * 1024, **kw)


KSTEP = 512


def latents_body(tok, gain, qdw, qg, kdw, kg, rw, pw, out, inv, aq, ak, ar, ap):
    k = pl.program_id(0)

    @pl.when(k == 0)
    def _():
        x = tok[...].astype(f32)
        inv[...] = jnp.broadcast_to(
            lax.rsqrt(jnp.mean(x * x, axis=-1, keepdims=True) + EPS), (ROWS, 128)
        )
        aq[...] = jnp.zeros_like(aq)
        ak[...] = jnp.zeros_like(ak)
        ar[...] = jnp.zeros_like(ar)
        ap[...] = jnp.zeros_like(ap)

    cols = pl.ds(pl.multiple_of(k * KSTEP, KSTEP), KSTEP)
    x = tok[:, cols].astype(f32)
    normed = (x * inv[:, 0:1] * gain[:, cols].astype(f32)).astype(bf16)
    aq[...] += nn(normed, qdw[...])
    ak[...] += nn(normed, kdw[...])
    ar[...] += nn(normed, rw[...])
    ap[...] += nn(normed, pw[...])

    @pl.when(k == pl.num_programs(0) - 1)
    def _():
        def norm(v, g):
            return (
                v * lax.rsqrt(jnp.mean(v * v, axis=-1, keepdims=True) + EPS) * g.astype(f32)
            ).astype(bf16)

        q = norm(aq[...], qg[...])
        kv = norm(ak[...], kg[...])
        rope = jnp.concatenate(
            [ar[...].astype(bf16), jnp.zeros((ROWS, 128 - ROT), bf16)], axis=1
        )
        pool = ap[...].astype(bf16)
        for y in range(NY):
            out[y, :, 0:QR] = q
            out[y, :, QR : QR + KR] = kv
            out[y, :, QR + KR : QR + KR + 128] = rope
            out[y, :, QR + KR + 128 :] = pool[:, y * 128 : (y + 1) * 128]


def latents(tok, gain, qdw, qg, kdw, kg, rw, pw):
    steps = WIDTH // KSTEP
    whole = lambda *s: pl.BlockSpec(s, lambda k: (0,) * len(s))
    part = lambda n: pl.BlockSpec((KSTEP, n), lambda k: (k, 0))
    return pl.pallas_call(
        latents_body,
        grid=(steps,),
        in_specs=[
            whole(ROWS, WIDTH),
            whole(1, WIDTH),
            part(QR),
            whole(1, QR),
            part(KR),
            whole(1, KR),
            part(ROT),
            part(512),
        ],
        out_specs=whole(NY, ROWS, 1024),
        out_shape=jax.ShapeDtypeStruct((NY, ROWS, 1024), bf16),
        scratch_shapes=[
            pltpu.VMEM((ROWS, 128), f32),
            pltpu.VMEM((ROWS, QR), f32),
            pltpu.VMEM((ROWS, KR), f32),
            pltpu.VMEM((ROWS, ROT), f32),
            pltpu.VMEM((ROWS, 512), f32),
        ],
        compiler_params=params(dimension_semantics=("arbitrary",)),
        name="latents",
    )(tok, gain.reshape(1, -1), qdw, qg.reshape(1, -1), kdw, kg.reshape(1, -1), rw, pw)


def interleaved(c, own, other):
    first = jnp.where(c == 0, own, other)
    second = jnp.where(c == 0, other, own)
    rows = []
    for y in range(NY):
        rows.append(first[y * ROWS : (y + 1) * ROWS])
        rows.append(second[y * ROWS : (y + 1) * ROWS])
    return jnp.concatenate(rows, axis=0)


def angles(coff, soff, cb, sb, idx):
    lanes = lax.broadcasted_iota(jnp.int32, (HALF, 128), 1)
    hit = lanes == idx
    cbase = jnp.sum(jnp.where(hit, cb, 0.0), axis=1, keepdims=True)
    sbase = jnp.sum(jnp.where(hit, sb, 0.0), axis=1, keepdims=True)
    return cbase * coff - sbase * soff, sbase * coff + cbase * soff


def rotated(v, cosine, sine):
    a = v[NOPE : NOPE + HALF]
    b = v[NOPE + HALF :]
    return jnp.concatenate(
        [v[:NOPE], a * cosine - b * sine, a * sine + b * cosine, jnp.zeros_like(v[:ROT])],
        axis=0,
    )


def queries_body(sc, own, other, wqt, qgain, coff, soff, cb, sb, out):
    c = sc[0]
    for x in range(NX):
        lat = interleaved(c, own[x], other[x])
        q = nt(wqt[...], lat)
        cosine, sine = angles(coff[...], soff[...], cb[...], sb[...], sc[2] * NX + x)
        for h in range(HEADS):
            v = q[h * HEAD : (h + 1) * HEAD]
            inv = lax.rsqrt(jnp.mean(v * v, axis=0, keepdims=True) + EPS)
            v = v * inv * qgain[...]
            v = rotated(v, cosine, sine) * (LOG2E * HEAD**-0.5)
            out[h, :, x * BLOCK : (x + 1) * BLOCK] = v.astype(bf16)


def queries(sc, own, other, wqt, qgain, tables):
    return pl.pallas_call(
        queries_body,
        in_specs=[smem()] + [vmem()] * 8,
        out_specs=vmem(),
        out_shape=jax.ShapeDtypeStruct((HEADS, 128, NQ), bf16),
        compiler_params=params(),
        name="queries",
    )(sc, own, other, wqt, qgain, *tables)


def attend_body(nb, slot0, first, last, *refs):
    refs = list(refs)
    sc = refs.pop(0)
    own = [refs.pop(0) for _ in range(nb)]
    other = [refs.pop(0) for _ in range(nb)]
    qt, wkvt, kgain, coff, soff, cb, sb = refs[:7]
    refs = refs[7:]
    if not first:
        acc_in, m_in = refs[:2]
        refs = refs[2:]
    if last:
        msg = refs.pop(0)
    else:
        acc_out, m_out = refs[:2]
        refs = refs[2:]
    kbuf, vbuf = refs
    c = sc[0]
    pick = (
        lax.broadcasted_iota(jnp.int32, (ROT, 128), 0)
        == lax.broadcasted_iota(jnp.int32, (ROT, 128), 1)
    ).astype(bf16)
    ones = (lax.broadcasted_iota(jnp.int32, (VROWS - VAL, BLOCK), 0) == 0).astype(bf16)
    for b in range(nb):
        lat = interleaved(c, own[b][...], other[b][...])
        kv = nt(wkvt[...], lat[:, :KR])
        rope = nt(pick, lat[:, KR:])
        rope_square = jnp.sum(rope * rope, axis=0, keepdims=True)
        cosine, sine = angles(coff[...], soff[...], cb[...], sb[...], sc[4 + slot0 + b])
        for h in range(HEADS):
            plain = kv[h * 128 : h * 128 + NOPE]
            total = jnp.sum(plain * plain, axis=0, keepdims=True) + rope_square
            inv = lax.rsqrt(total * (1.0 / HEAD) + EPS)
            k = jnp.concatenate([plain, rope], axis=0) * inv * kgain[...]
            k = rotated(k, cosine, sine).astype(bf16)
            kbuf[h, b * BLOCK : (b + 1) * BLOCK, :] = k.T
            vbuf[h, 0:VAL, b * BLOCK : (b + 1) * BLOCK] = kv[
                h * 128 + NOPE : (h + 1) * 128
            ].astype(bf16)
            vbuf[h, VAL:, b * BLOCK : (b + 1) * BLOCK] = ones

    def tile(i, carry):
        h = i // (NQ // QTILE)
        col = pl.ds(pl.multiple_of((i % (NQ // QTILE)) * QTILE, QTILE), QTILE)
        q = qt[h, :, col]
        if first:
            m = jnp.full((1, QTILE), -1e30, f32)
            acc = jnp.zeros((VROWS, QTILE), f32)
        else:
            m = m_in[h, :, col]
            acc = acc_in[h, :, col]
        for b in range(nb):
            keys = slice(b * BLOCK, (b + 1) * BLOCK)
            s = nn(kbuf[h, keys, :], q)
            new = jnp.maximum(m, jnp.max(s, axis=0, keepdims=True))
            p = jnp.exp2(s - new).astype(bf16)
            acc = acc * jnp.exp2(m - new) + nn(vbuf[h, :, keys], p)
            m = new
        if last:
            acc_s[h, :, col] = acc
            m_s[h, :, col] = m
        else:
            acc_out[h, :, col] = acc
            m_out[h, :, col] = m
        return carry

    if last:
        def run(acc_ref, m_ref):
            nonlocal acc_s, m_s
            acc_s, m_s = acc_ref, m_ref
            lax.fori_loop(0, HEADS * (NQ // QTILE), tile, 0)
            for x in range(NX):
                cols = slice(x * BLOCK, (x + 1) * BLOCK)
                stats = []
                for h in range(HEADS):
                    total = acc_ref[h, VAL : VAL + 1, cols]
                    part = acc_ref[h, 0:VAL, cols] / total
                    msg[x, h * VAL : (h + 1) * VAL, :] = part.astype(bf16)
                    lse = (m_ref[h, :, cols] + jnp.log2(total)) * LN2
                    hi = lse.astype(bf16)
                    rest = lse - hi.astype(f32)
                    mid = rest.astype(bf16)
                    low = (rest - mid.astype(f32)).astype(bf16)
                    stats += [hi.astype(f32), mid.astype(f32), low.astype(f32)]
                stats.append(jnp.zeros((MSG - HEADS * VAL - 9, BLOCK), f32))
                msg[x, HEADS * VAL :, :] = jnp.concatenate(stats, axis=0).astype(bf16)

        acc_s = m_s = None
        pl.run_scoped(
            run, pltpu.VMEM((HEADS, VROWS, NQ), f32), pltpu.VMEM((HEADS, 1, NQ), f32)
        )
    else:
        lax.fori_loop(0, HEADS * (NQ // QTILE), tile, 0)


def attend(sc, own, other, slot0, qt, wkvt, kgain, tables, carry, last):
    nb = len(own)
    first = carry is None
    if last:
        out_shape = jax.ShapeDtypeStruct((NX, MSG, BLOCK), bf16)
        out_specs = vmem()
    else:
        out_shape = (
            jax.ShapeDtypeStruct((HEADS, VROWS, NQ), f32),
            jax.ShapeDtypeStruct((HEADS, 1, NQ), f32),
        )
        out_specs = (vmem(), vmem())
    args = [sc, *own, *other, qt, wkvt, kgain, *tables] + ([] if first else list(carry))

    def body(*refs):
        attend_body(nb, slot0, first, last, *refs)

    return pl.pallas_call(
        body,
        in_specs=[smem()] + [vmem()] * (len(args) - 1),
        out_specs=out_specs,
        out_shape=out_shape,
        scratch_shapes=[
            pltpu.VMEM((HEADS, nb * BLOCK, 128), bf16),
            pltpu.VMEM((HEADS, VROWS, nb * BLOCK), bf16),
        ],
        compiler_params=params(),
        name=f"attend{slot0}",
    )(*args)


def merge_body(sc, msg, keep, send, lse_out, buf):
    c = sc[0]
    for h in range(HEADS):
        logs = []
        for x in range(NX):
            at = HEADS * VAL + 3 * h
            tail = msg[x, HEADS * VAL :, :].astype(f32)
            r = 3 * h
            logs.append(tail[r : r + 1] + tail[r + 1 : r + 2] + tail[r + 2 : r + 3])
        top = jnp.maximum(jnp.maximum(logs[0], logs[1]), jnp.maximum(logs[2], logs[3]))
        weights = [jnp.exp(v - top) for v in logs]
        total = weights[0] + weights[1] + weights[2] + weights[3]
        lse_out[h : h + 1, :] = top + jnp.log(total)
        inv = 1.0 / total
        acc = jnp.zeros((VAL, BLOCK), f32)
        for x in range(NX):
            acc = acc + msg[x, h * VAL : (h + 1) * VAL, :].astype(f32) * (weights[x] * inv)
        buf[:, h * VAL : (h + 1) * VAL] = acc.T.astype(bf16)
    for y in range(NY):
        dst = slice(y * ROWS, (y + 1) * ROWS)
        at = pl.multiple_of(y * 2 * ROWS + c * ROWS, ROWS)
        keep[dst, :] = buf[pl.ds(at, ROWS), :]
        to = pl.multiple_of(y * 2 * ROWS + (1 - c) * ROWS, ROWS)
        send[dst, :] = buf[pl.ds(to, ROWS), :]


def merge(sc, msg):
    return pl.pallas_call(
        merge_body,
        in_specs=[smem(), vmem()],
        out_specs=(vmem(), vmem(), vmem()),
        out_shape=(
            jax.ShapeDtypeStruct((SIDE, HEADS * VAL), bf16),
            jax.ShapeDtypeStruct((SIDE, HEADS * VAL), bf16),
            jax.ShapeDtypeStruct((HEADS, BLOCK), f32),
        ),
        scratch_shapes=[pltpu.VMEM((BLOCK, HEADS * VAL), bf16)],
        compiler_params=params(),
        name="merge",
    )(sc, msg)


def pool_body(sc, own, other, low, high, mixw, scale, out, xs):
    c, y0, z, x0 = sc[0], sc[1], sc[2], sc[3]
    xs[0:8, :] = jnp.zeros((8, 128), f32)
    xs[8:16, :] = low[...].astype(f32)
    xs[16 + BLOCK : 24 + BLOCK, :] = high[...].astype(f32)
    xs[24 + BLOCK : 32 + BLOCK, :] = jnp.zeros((8, 128), f32)
    for y in range(NY):
        src = slice(y * ROWS, (y + 1) * ROWS)
        at = pl.multiple_of(16 + y * 2 * ROWS + c * ROWS, 16)
        xs[pl.ds(at, ROWS), :] = own[src, :].astype(f32)
        to = pl.multiple_of(16 + y * 2 * ROWS + (1 - c) * ROWS, 16)
        xs[pl.ds(to, ROWS), :] = other[src, :].astype(f32)
    lane = lax.broadcasted_iota(jnp.int32, (ROWS, 128), 1)
    second = lane >= 64
    wide = (y0 % 2) == 1
    half = jnp.where(wide, jnp.where(second, 8, 4), jnp.where(second, 2, 1))
    for y in range(NY):
        row0 = y * 2 * ROWS + c * ROWS
        window = xs[pl.ds(pl.multiple_of(row0, 16), ROWS + 32), :]
        n = ROWS + 32
        x = window[16 : 16 + ROWS]
        s1 = window[0 : n - 1] + window[1:n]
        s2 = s1[0 : n - 3] + s1[2 : n - 1]
        s4 = s2[0 : n - 7] + s2[4 : n - 3]
        s8 = s4[0 : n - 15] + s4[8 : n - 7]
        w1 = s1[15 : 15 + ROWS]
        w2 = s2[14 : 14 + ROWS]
        w4 = s4[12 : 12 + ROWS]
        w8 = s8[8 : 8 + ROWS]
        total = jnp.where(wide, jnp.where(second, w8, w4), jnp.where(second, w2, w1))
        place = (
            (z * NX + x0) * BLOCK + row0 + lax.broadcasted_iota(jnp.int32, (ROWS, 128), 0)
        )
        count = (jnp.minimum(place + half, TOKENS) - jnp.maximum(place - half, 0)).astype(f32)
        pooled = (total / count - x).astype(bf16)
        mapped = nn(pooled, mixw[...])
        out[y * ROWS : (y + 1) * ROWS, :] = (mapped * scale[...]).astype(bf16)


def pooling(sc, own, other, low, high, mixw, scale):
    return pl.pallas_call(
        pool_body,
        in_specs=[smem()] + [vmem()] * 6,
        out_specs=vmem(),
        out_shape=jax.ShapeDtypeStruct((SIDE, 128), bf16),
        scratch_shapes=[pltpu.VMEM((BLOCK + 32, 128), f32)],
        compiler_params=params(),
        name="pooling",
    )(sc, own, other, low, high, mixw, scale)


def project_body(mine, theirs, pooled, wa, wb, wp, out):
    total = nn(mine[...], wa[...]) + nn(theirs[...], wb[...]) + nn(pooled[...], wp[...])
    for y in range(NY):
        out[y, :, :] = total[y * ROWS : (y + 1) * ROWS].astype(bf16)


def project(mine, theirs, pooled, wa, wb, wp):
    step = 512
    whole = lambda *s: pl.BlockSpec(s, lambda k: (0,) * len(s))
    part = lambda n: pl.BlockSpec((n, step), lambda k: (0, k))
    return pl.pallas_call(
        project_body,
        grid=(WIDTH // step,),
        in_specs=[
            whole(SIDE, 192),
            whole(SIDE, 192),
            whole(SIDE, 128),
            part(192),
            part(192),
            part(128),
        ],
        out_specs=pl.BlockSpec((NY, ROWS, step), lambda k: (0, 0, k)),
        out_shape=jax.ShapeDtypeStruct((NY, ROWS, WIDTH), bf16),
        compiler_params=params(dimension_semantics=("arbitrary",)),
        name="project",
    )(mine, theirs, pooled, wa, wb, wp)


def across(x):
    return lax.ppermute(x, "c", [(0, 1), (1, 0)])


def along_z(x, shift):
    return lax.ppermute(x, "z", [(i, (i + shift) % NZ) for i in range(NZ)])


def shards(
    tokens,
    norm_gain,
    query_down_weight,
    query_latent_norm_gain,
    key_value_down_weight,
    key_value_latent_gain,
    w_rope_key,
    w_pool_in,
    query_up_weight,
    key_value_up_weight,
    query_gain,
    key_gain,
    w_pool_mix,
    pool_scale,
    w_out_attn,
    w_out_pool,
):
    z = lax.axis_index("z")
    x = lax.axis_index("x")
    y = lax.axis_index("y")
    c = lax.axis_index("c")
    offsets = [0, -1, 1, -2, 2, -3, 3, -4]
    sc = jnp.stack(
        [c, y, z, x] + [((z + o) % NZ) * NX + x for o in offsets]
    ).astype(jnp.int32)
    tables = trig_tables()
    wqt = query_up_weight.T
    wkvt = key_value_up_weight.T
    qgain = query_gain.astype(f32).reshape(HEAD, 1)
    kgain = key_gain.astype(f32).reshape(HEAD, 1)

    wb = across(w_out_attn)
    wp_other = across(w_out_pool)
    mix_other = across(w_pool_mix[0])
    scale_other = across(pool_scale)
    wp = jnp.where(
        c == 0,
        jnp.concatenate([w_out_pool, wp_other], 0),
        jnp.concatenate([wp_other, w_out_pool], 0),
    )
    zero = jnp.zeros((64, 64), bf16)
    mix0 = jnp.where(c == 0, w_pool_mix[0], mix_other)
    mix1 = jnp.where(c == 0, mix_other, w_pool_mix[0])
    mixw = jnp.concatenate(
        [jnp.concatenate([mix0, zero], 1), jnp.concatenate([zero, mix1], 1)], 0
    )
    scale = jnp.where(
        c == 0,
        jnp.concatenate([pool_scale, scale_other]),
        jnp.concatenate([scale_other, pool_scale]),
    ).astype(f32).reshape(1, 128)

    message = latents(
        tokens,
        norm_gain,
        query_down_weight,
        query_latent_norm_gain,
        key_value_down_weight,
        key_value_latent_gain,
        w_rope_key,
        w_pool_in,
    )
    got = lax.all_to_all(message, "y", 0, 0, tiled=True).reshape(SIDE, 1024)
    kv0 = got[:, QR : QR + KR + 128]
    q_side = got[:, :QR]
    pool_own = got[:, QR + KR + 128 :]

    blocks = [kv0]
    fwd = back = kv0
    for step in range(1, 4):
        fwd = along_z(fwd, 1)
        back = along_z(back, -1)
        blocks += [fwd, back]
    fwd = along_z(fwd, 1)
    blocks.append(fwd)
    others = [across(b) for b in blocks]

    q_own = lax.all_gather(q_side, "x", axis=0)
    q_other = across(q_own)
    qt = queries(sc, q_own, q_other, wqt, qgain, tables)

    carry = attend(sc, blocks[:5], others[:5], 0, qt, wkvt, kgain, tables, None, False)
    partial = attend(sc, blocks[5:], others[5:], 5, qt, wkvt, kgain, tables, carry, True)

    pool_other = across(pool_own)
    tail_rows = jnp.where(c == 1, pool_own[SIDE - 8 :], pool_other[SIDE - 8 :])
    head_rows = jnp.where(c == 0, pool_own[:8], pool_other[:8])
    count = NZ * NX
    low = lax.ppermute(tail_rows, ("z", "x"), [(i, i + 1) for i in range(count - 1)])
    high = lax.ppermute(head_rows, ("z", "x"), [(i + 1, i) for i in range(count - 1)])
    pooled = pooling(sc, pool_own, pool_other, low, high, mixw, scale)

    merged = lax.all_to_all(partial, "x", 0, 0, tiled=True)
    keep, send, row_logsum = merge(sc, merged)
    theirs = across(send)
    parts = project(keep, theirs, pooled, w_out_attn, wb, wp)
    parts = lax.all_to_all(parts, "y", 0, 0, tiled=True)
    mixed = jnp.sum(parts.astype(f32), axis=0).astype(bf16)
    return mixed, row_logsum


def solution(mesh):
    fine = Mesh(mesh.devices.reshape(NZ, NX, NY, 2), ("z", "x", "y", "c"))
    tp = ("y", "c")
    placed = (
        P(("z", "x", "y", "c"), None),
        P(),
        P(),
        P(),
        P(),
        P(),
        P(),
        P(),
        P(None, tp),
        P(None, tp),
        P(),
        P(),
        P(tp, None, None),
        P(tp),
        P(tp, None),
        P(tp, None),
    )
    return jax.shard_map(
        shards,
        mesh=fine,
        in_specs=placed,
        out_specs=(P(("z", "x", "y", "c"), None), P(tp, ("z", "x"))),
        check_vma=False,
    )
```

```python
import jax
import jax.numpy as jnp
import numpy as np
from jax import lax
from jax.experimental import pallas as pl
from jax.experimental.pallas import tpu as pltpu
from jax.sharding import Mesh, PartitionSpec as P

NOPE = 64
ROT = 32
HALF = 16
HEAD = 96
VAL = 64
HEADS = 3
QR = 512
KR = 256
EPS = 1e-06
WIDTH = 2048
ROWS = 48
BLOCK = 384
SIDE = 192
TOKENS = 12288
LOG2E = 1.4426950408889634
LN2 = 0.6931471805599453
MSG = 208
VROWS = 80
QTILE = 512
NX = 4
NY = 4
NZ = 8
NQ = NX * BLOCK

bf16 = jnp.bfloat16
f32 = jnp.float32

def trig_tables():
    freqs = 10000.0 ** (-np.arange(HALF, dtype=np.float64) / HALF)
    inner = freqs[:, None] * np.arange(BLOCK, dtype=np.float64)[None, :]
    outer = freqs[:, None] * (BLOCK * np.arange(NZ * NX, dtype=np.float64))[None, :]
    pad = np.zeros((HALF, 128 - NZ * NX))
    cast = lambda a: a.astype(np.float32)
    return (
        cast(np.cos(inner)),
        cast(np.sin(inner)),
        cast(np.concatenate([np.cos(outer), pad], 1)),
        cast(np.concatenate([np.sin(outer), pad], 1)),
    )


def vmem():
    return pl.BlockSpec(memory_space=pltpu.VMEM)


def smem():
    return pl.BlockSpec(memory_space=pltpu.SMEM)


def nt(a, b):
    return lax.dot_general(a, b, (((1,), (1,)), ((), ())), preferred_element_type=f32)


def nn(a, b):
    return lax.dot_general(a, b, (((1,), (0,)), ((), ())), preferred_element_type=f32)


def params(**kw):
    return pltpu.CompilerParams(vmem_limit_bytes=56 * 1024 * 1024, **kw)


KSTEP = 512


def latents_body(tok, gain, qdw, qg, kdw, kg, rw, pw, out, inv, aq, ak, ar, ap):
    k = pl.program_id(0)

    @pl.when(k == 0)
    def _():
        x = tok[...].astype(f32)
        inv[...] = jnp.broadcast_to(
            lax.rsqrt(jnp.mean(x * x, axis=-1, keepdims=True) + EPS), (ROWS, 128)
        )
        aq[...] = jnp.zeros_like(aq)
        ak[...] = jnp.zeros_like(ak)
        ar[...] = jnp.zeros_like(ar)
        ap[...] = jnp.zeros_like(ap)

    cols = pl.ds(pl.multiple_of(k * KSTEP, KSTEP), KSTEP)
    x = tok[:, cols].astype(f32)
    normed = (x * inv[:, 0:1] * gain[cols].astype(f32).reshape(1, KSTEP)).astype(bf16)
    aq[...] += nn(normed, qdw[...])
    ak[...] += nn(normed, kdw[...])
    ar[...] += nt(normed, rw[...])
    ap[...] += nn(normed, pw[...])

    @pl.when(k == pl.num_programs(0) - 1)
    def _():
        def norm(v, g):
            return (
                v
                * lax.rsqrt(jnp.mean(v * v, axis=-1, keepdims=True) + EPS)
                * g.astype(f32).reshape(1, -1)
            ).astype(bf16)

        q = norm(aq[...], qg[...])
        kv = norm(ak[...], kg[...])
        rope = jnp.concatenate(
            [ar[...].astype(bf16), jnp.zeros((ROWS, 128 - ROT), bf16)], axis=1
        )
        pool = ap[...].astype(bf16)
        for y in range(NY):
            out[y, :, 0:QR] = q
            out[y, :, QR : QR + KR] = kv
            out[y, :, QR + KR : QR + KR + 128] = rope
            out[y, :, QR + KR + 128 :] = pool[:, y * 128 : (y + 1) * 128]


def latents(tok, gain, qdw, qg, kdw, kg, rw, pw):
    steps = WIDTH // KSTEP
    whole = lambda *s: pl.BlockSpec(s, lambda k: (0,) * len(s))
    part = lambda n: pl.BlockSpec((KSTEP, n), lambda k: (k, 0))
    return pl.pallas_call(
        latents_body,
        grid=(steps,),
        in_specs=[
            whole(ROWS, WIDTH),
            whole(WIDTH),
            part(QR),
            whole(QR),
            part(KR),
            whole(KR),
            pl.BlockSpec((ROT, KSTEP), lambda k: (0, k)),
            part(512),
        ],
        out_specs=whole(NY, ROWS, 1024),
        out_shape=jax.ShapeDtypeStruct((NY, ROWS, 1024), bf16),
        scratch_shapes=[
            pltpu.VMEM((ROWS, 128), f32),
            pltpu.VMEM((ROWS, QR), f32),
            pltpu.VMEM((ROWS, KR), f32),
            pltpu.VMEM((ROWS, ROT), f32),
            pltpu.VMEM((ROWS, 512), f32),
        ],
        compiler_params=params(dimension_semantics=("arbitrary",)),
        name="latents",
    )(tok, gain, qdw, qg, kdw, kg, rw.T, pw)


def interleaved(c, own, other):
    first = jnp.where(c == 0, own, other)
    second = jnp.where(c == 0, other, own)
    rows = []
    for y in range(NY):
        rows.append(first[y * ROWS : (y + 1) * ROWS])
        rows.append(second[y * ROWS : (y + 1) * ROWS])
    return jnp.concatenate(rows, axis=0)


def angles(coff, soff, cb, sb, idx):
    lanes = lax.broadcasted_iota(jnp.int32, (HALF, 128), 1)
    hit = lanes == idx
    cbase = jnp.sum(jnp.where(hit, cb, 0.0), axis=1, keepdims=True)
    sbase = jnp.sum(jnp.where(hit, sb, 0.0), axis=1, keepdims=True)
    return cbase * coff - sbase * soff, sbase * coff + cbase * soff


def rotated(v, cosine, sine):
    a = v[NOPE : NOPE + HALF]
    b = v[NOPE + HALF :]
    return jnp.concatenate(
        [v[:NOPE], a * cosine - b * sine, a * sine + b * cosine, jnp.zeros_like(v[:ROT])],
        axis=0,
    )


def queries_body(sc, own, other, wqt, qgain, coff, soff, cb, sb, out):
    c = sc[0]
    for x in range(NX):
        lat = interleaved(c, own[x], other[x])
        q = nt(wqt[...], lat)
        cosine, sine = angles(coff[...], soff[...], cb[...], sb[...], sc[2] * NX + x)
        for h in range(HEADS):
            v = q[h * HEAD : (h + 1) * HEAD]
            inv = lax.rsqrt(jnp.mean(v * v, axis=0, keepdims=True) + EPS)
            v = v * inv * qgain[...]
            v = rotated(v, cosine, sine) * (LOG2E * HEAD**-0.5)
            out[h, :, x * BLOCK : (x + 1) * BLOCK] = v.astype(bf16)


def queries(sc, own, other, wqt, qgain, tables):
    return pl.pallas_call(
        queries_body,
        in_specs=[smem()] + [vmem()] * 8,
        out_specs=vmem(),
        out_shape=jax.ShapeDtypeStruct((HEADS, 128, NQ), bf16),
        compiler_params=params(),
        name="queries",
    )(sc, own, other, wqt, qgain, *tables)


def keys_body(nb, slot0, *refs):
    sc = refs[0]
    own = refs[1 : 1 + nb]
    other = refs[1 + nb : 1 + 2 * nb]
    wkvt, kgain, coff, soff, cb, sb, kbuf, vbuf = refs[1 + 2 * nb :]
    c = sc[0]
    pick = (
        lax.broadcasted_iota(jnp.int32, (ROT, 128), 0)
        == lax.broadcasted_iota(jnp.int32, (ROT, 128), 1)
    ).astype(bf16)
    ones = (lax.broadcasted_iota(jnp.int32, (VROWS - VAL, BLOCK), 0) == 0).astype(bf16)
    for b in range(nb):
        lat = interleaved(c, own[b][...], other[b][...])
        kv = nt(wkvt[...], lat[:, :KR])
        rope = nt(pick, lat[:, KR:])
        rope_square = jnp.sum(rope * rope, axis=0, keepdims=True)
        cosine, sine = angles(coff[...], soff[...], cb[...], sb[...], sc[4 + slot0 + b])
        for h in range(HEADS):
            plain = kv[h * 128 : h * 128 + NOPE]
            total = jnp.sum(plain * plain, axis=0, keepdims=True) + rope_square
            inv = lax.rsqrt(total * (1.0 / HEAD) + EPS)
            k = jnp.concatenate([plain, rope], axis=0) * inv * kgain[...]
            k = rotated(k, cosine, sine).astype(bf16)
            kbuf[h, b * BLOCK : (b + 1) * BLOCK, :] = k.T
            vbuf[h, 0:VAL, b * BLOCK : (b + 1) * BLOCK] = kv[
                h * 128 + NOPE : (h + 1) * 128
            ].astype(bf16)
            vbuf[h, VAL:, b * BLOCK : (b + 1) * BLOCK] = ones


def keys_values(sc, own, other, slot0, wkvt, kgain, tables):
    nb = len(own)

    def body(*refs):
        keys_body(nb, slot0, *refs)

    args = [sc, *own, *other, wkvt, kgain, *tables]
    return pl.pallas_call(
        body,
        in_specs=[smem()] + [vmem()] * (len(args) - 1),
        out_specs=(vmem(), vmem()),
        out_shape=(
            jax.ShapeDtypeStruct((HEADS, nb * BLOCK, 128), bf16),
            jax.ShapeDtypeStruct((HEADS, VROWS, nb * BLOCK), bf16),
        ),
        compiler_params=params(),
        name=f"keys{slot0}",
    )(*args)


CHUNK = 256
SUB = 128
TILES = HEADS * (NQ // QTILE)


def attend_body(sizes, first, last, extra, *refs):
    refs = list(refs)
    refs = refs[extra:]
    pairs = [(refs.pop(0), refs.pop(0)) for _ in sizes]
    qt = refs.pop(0)
    if not first:
        acc_in, m_in = refs[:2]
        refs = refs[2:]
    if last:
        msg = refs.pop(0)
        acc_s, m_s = refs[2:]
    else:
        acc_s, m_s = refs[:2]
        refs = refs[2:]
    bufs = refs[:2]
    chunks = []
    base = 0
    for (kr, vr), n in zip(pairs, sizes):
        for at in range(0, n, CHUNK):
            size = min(CHUNK, n - at)
            chunks.append((base + at, size, kr, vr, at))
        base += n

    def where(i):
        per = NQ // QTILE
        return i // per, pl.ds(pl.multiple_of((i % per) * QTILE, QTILE), QTILE)

    def score(i, chunk, buf, top):
        row, size, kr, _, at = chunk
        h, col = where(i)
        for sub in range(0, size, SUB):
            s = nn(kr[h, at + sub : at + sub + SUB, :], qt[h, :, col])
            buf[row + sub : row + sub + SUB, :] = s
            top = jnp.maximum(top, jnp.max(s.reshape(SUB // 8, 8, QTILE), axis=0))
        return top

    def weigh(i, chunk, buf, m):
        row, size, _, vr, at = chunk
        h, _ = where(i)
        p = jnp.exp2(buf[row : row + size, :] - m).astype(bf16)
        return nn(vr[h, :, at : at + size], p)

    low = jnp.full((8, QTILE), -1e30, f32)

    def settle(i, top):
        m = jnp.max(top, axis=0, keepdims=True)
        if first:
            return m
        h, col = where(i)
        return jnp.maximum(m, m_in[h, :, col])

    def finish(i, m, acc):
        h, col = where(i)
        if not first:
            acc = acc + acc_in[h, :, col] * jnp.exp2(m_in[h, :, col] - m)
        acc_s[h, :, col] = acc
        m_s[h, :, col] = m

    def both(i, m, buf, nxt):
        acc = None
        top = low
        for chunk in chunks:
            part = weigh(i, chunk, buf, m)
            acc = part if acc is None else acc + part
            top = score(i + 1, chunk, nxt, top)
        finish(i, m, acc)
        return settle(i + 1, top)

    top = low
    for chunk in chunks:
        top = score(0, chunk, bufs[0], top)
    m = settle(0, top)

    def pair(j, m):
        m = both(2 * j, m, bufs[0], bufs[1])
        return both(2 * j + 1, m, bufs[1], bufs[0])

    m = lax.fori_loop(0, (TILES - 1) // 2, pair, m)
    acc = None
    for chunk in chunks:
        part = weigh(TILES - 1, chunk, bufs[0], m)
        acc = part if acc is None else acc + part
    finish(TILES - 1, m, acc)

    if last:
        for x in range(NX):
            cols = slice(x * BLOCK, (x + 1) * BLOCK)
            stats = []
            for h in range(HEADS):
                total = acc_s[h, VAL : VAL + 1, cols]
                part = acc_s[h, 0:VAL, cols] * (1.0 / total)
                msg[x, h * VAL : (h + 1) * VAL, :] = part.astype(bf16)
                lse = (m_s[h, :, cols] + jnp.log2(total)) * LN2
                hi = lse.astype(bf16)
                rest = lse - hi.astype(f32)
                mid = rest.astype(bf16)
                low_part = (rest - mid.astype(f32)).astype(bf16)
                stats += [hi.astype(f32), mid.astype(f32), low_part.astype(f32)]
            stats.append(jnp.zeros((MSG - HEADS * VAL - 9, BLOCK), f32))
            msg[x, HEADS * VAL :, :] = jnp.concatenate(stats, axis=0).astype(bf16)


def attend(pairs, qt, carry, last, name, after=()):
    sizes = [k.shape[1] for k, _ in pairs]
    first = carry is None
    state = (
        jax.ShapeDtypeStruct((HEADS, VROWS, NQ), f32),
        jax.ShapeDtypeStruct((HEADS, 1, NQ), f32),
    )
    if last:
        out_shape = jax.ShapeDtypeStruct((NX, MSG, BLOCK), bf16)
        out_specs = vmem()
    else:
        out_shape = state
        out_specs = (vmem(), vmem())
    args = [a for pair in pairs for a in pair] + [qt] + ([] if first else list(carry))
    scratch = [pltpu.VMEM((sum(sizes), QTILE), f32) for _ in range(2)]
    if last:
        scratch += [pltpu.VMEM(s.shape, s.dtype) for s in state]

    def body(*refs):
        attend_body(sizes, first, last, len(after), *refs)

    return pl.pallas_call(
        body,
        in_specs=[pl.BlockSpec(memory_space=pl.ANY)] * len(after) + [vmem()] * len(args),
        out_specs=out_specs,
        out_shape=out_shape,
        scratch_shapes=scratch,
        compiler_params=params(),
        name=name,
    )(*after, *args)


def merge_body(sc, msg, keep, send, lse_out, buf):
    c = sc[0]
    for h in range(HEADS):
        logs = []
        for x in range(NX):
            at = HEADS * VAL + 3 * h
            tail = msg[x, HEADS * VAL :, :].astype(f32)
            r = 3 * h
            logs.append(tail[r : r + 1] + tail[r + 1 : r + 2] + tail[r + 2 : r + 3])
        top = jnp.maximum(jnp.maximum(logs[0], logs[1]), jnp.maximum(logs[2], logs[3]))
        weights = [jnp.exp(v - top) for v in logs]
        total = weights[0] + weights[1] + weights[2] + weights[3]
        lse_out[h : h + 1, :] = top + jnp.log(total)
        inv = 1.0 / total
        acc = jnp.zeros((VAL, BLOCK), f32)
        for x in range(NX):
            acc = acc + msg[x, h * VAL : (h + 1) * VAL, :].astype(f32) * (weights[x] * inv)
        buf[:, h * VAL : (h + 1) * VAL] = acc.T.astype(bf16)
    for y in range(NY):
        dst = slice(y * ROWS, (y + 1) * ROWS)
        at = pl.multiple_of(y * 2 * ROWS + c * ROWS, ROWS)
        keep[dst, :] = buf[pl.ds(at, ROWS), :]
        to = pl.multiple_of(y * 2 * ROWS + (1 - c) * ROWS, ROWS)
        send[dst, :] = buf[pl.ds(to, ROWS), :]


def merge(sc, msg):
    return pl.pallas_call(
        merge_body,
        in_specs=[smem(), vmem()],
        out_specs=(vmem(), vmem(), vmem()),
        out_shape=(
            jax.ShapeDtypeStruct((SIDE, HEADS * VAL), bf16),
            jax.ShapeDtypeStruct((SIDE, HEADS * VAL), bf16),
            jax.ShapeDtypeStruct((HEADS, BLOCK), f32),
        ),
        scratch_shapes=[pltpu.VMEM((BLOCK, HEADS * VAL), bf16)],
        compiler_params=params(),
        name="merge",
    )(sc, msg)


def pool_body(sc, own, other, low, high, mixw, scale, out, xs):
    c, y0, z, x0 = sc[0], sc[1], sc[2], sc[3]
    xs[0:8, :] = jnp.zeros((8, 128), f32)
    xs[8:16, :] = low[...].astype(f32)
    xs[16 + BLOCK : 24 + BLOCK, :] = high[...].astype(f32)
    xs[24 + BLOCK : 32 + BLOCK, :] = jnp.zeros((8, 128), f32)
    for y in range(NY):
        src = slice(y * ROWS, (y + 1) * ROWS)
        at = pl.multiple_of(16 + y * 2 * ROWS + c * ROWS, 16)
        xs[pl.ds(at, ROWS), :] = own[src, :].astype(f32)
        to = pl.multiple_of(16 + y * 2 * ROWS + (1 - c) * ROWS, 16)
        xs[pl.ds(to, ROWS), :] = other[src, :].astype(f32)
    lane = lax.broadcasted_iota(jnp.int32, (ROWS, 128), 1)
    second = lane >= 64
    wide = (y0 % 2) == 1
    half = jnp.where(wide, jnp.where(second, 8, 4), jnp.where(second, 2, 1))
    for y in range(NY):
        row0 = y * 2 * ROWS + c * ROWS
        window = xs[pl.ds(pl.multiple_of(row0, 16), ROWS + 32), :]
        n = ROWS + 32
        x = window[16 : 16 + ROWS]
        s1 = window[0 : n - 1] + window[1:n]
        s2 = s1[0 : n - 3] + s1[2 : n - 1]
        s4 = s2[0 : n - 7] + s2[4 : n - 3]
        s8 = s4[0 : n - 15] + s4[8 : n - 7]
        w1 = s1[15 : 15 + ROWS]
        w2 = s2[14 : 14 + ROWS]
        w4 = s4[12 : 12 + ROWS]
        w8 = s8[8 : 8 + ROWS]
        total = jnp.where(wide, jnp.where(second, w8, w4), jnp.where(second, w2, w1))
        place = (
            (z * NX + x0) * BLOCK + row0 + lax.broadcasted_iota(jnp.int32, (ROWS, 128), 0)
        )
        count = (jnp.minimum(place + half, TOKENS) - jnp.maximum(place - half, 0)).astype(f32)
        pooled = (total / count - x).astype(bf16)
        mapped = nn(pooled, mixw[...])
        out[y * ROWS : (y + 1) * ROWS, :] = (mapped * scale[...]).astype(bf16)


def pooling(sc, own, other, low, high, mixw, scale):
    return pl.pallas_call(
        pool_body,
        in_specs=[smem()] + [vmem()] * 6,
        out_specs=vmem(),
        out_shape=jax.ShapeDtypeStruct((SIDE, 128), bf16),
        scratch_shapes=[pltpu.VMEM((BLOCK + 32, 128), f32)],
        compiler_params=params(),
        name="pooling",
    )(sc, own, other, low, high, mixw, scale)


def project_body(mine, theirs, pooled, wa, wb, wp, out):
    total = nn(mine[...], wa[...]) + nn(theirs[...], wb[...]) + nn(pooled[...], wp[...])
    for y in range(NY):
        out[y, :, :] = total[y * ROWS : (y + 1) * ROWS].astype(bf16)


def project(mine, theirs, pooled, wa, wb, wp):
    step = 512
    whole = lambda *s: pl.BlockSpec(s, lambda k: (0,) * len(s))
    part = lambda n: pl.BlockSpec((n, step), lambda k: (0, k))
    return pl.pallas_call(
        project_body,
        grid=(WIDTH // step,),
        in_specs=[
            whole(SIDE, 192),
            whole(SIDE, 192),
            whole(SIDE, 128),
            part(192),
            part(192),
            part(128),
        ],
        out_specs=pl.BlockSpec((NY, ROWS, step), lambda k: (0, 0, k)),
        out_shape=jax.ShapeDtypeStruct((NY, ROWS, WIDTH), bf16),
        compiler_params=params(dimension_semantics=("arbitrary",)),
        name="project",
    )(mine, theirs, pooled, wa, wb, wp)


def across(x):
    return lax.ppermute(x, "c", [(0, 1), (1, 0)])


def along_z(x, shift):
    return lax.ppermute(x, "z", [(i, (i + shift) % NZ) for i in range(NZ)])


def shards(
    tokens,
    norm_gain,
    query_down_weight,
    query_latent_norm_gain,
    key_value_down_weight,
    key_value_latent_gain,
    w_rope_key,
    w_pool_in,
    query_up_weight,
    key_value_up_weight,
    query_gain,
    key_gain,
    w_pool_mix,
    pool_scale,
    w_out_attn,
    w_out_pool,
):
    z = lax.axis_index("z")
    x = lax.axis_index("x")
    y = lax.axis_index("y")
    c = lax.axis_index("c")
    offsets = [0, -1, 1, -2, 2, -3, 3, -4]
    sc = jnp.stack(
        [c, y, z, x] + [((z + o) % NZ) * NX + x for o in offsets]
    ).astype(jnp.int32)
    tables = trig_tables()
    wqt = query_up_weight.T
    wkvt = key_value_up_weight.T
    qgain = query_gain.astype(f32).reshape(HEAD, 1)
    kgain = key_gain.astype(f32).reshape(HEAD, 1)

    wb = across(w_out_attn)
    wp_other = across(w_out_pool)
    mix_other = across(w_pool_mix[0])
    scale_other = across(pool_scale)
    wp = jnp.where(
        c == 0,
        jnp.concatenate([w_out_pool, wp_other], 0),
        jnp.concatenate([wp_other, w_out_pool], 0),
    )
    zero = jnp.zeros((64, 64), bf16)
    mix0 = jnp.where(c == 0, w_pool_mix[0], mix_other)
    mix1 = jnp.where(c == 0, mix_other, w_pool_mix[0])
    mixw = jnp.concatenate(
        [jnp.concatenate([mix0, zero], 1), jnp.concatenate([zero, mix1], 1)], 0
    )
    scale = jnp.where(
        c == 0,
        jnp.concatenate([pool_scale, scale_other]),
        jnp.concatenate([scale_other, pool_scale]),
    ).astype(f32).reshape(1, 128)

    message = latents(
        tokens,
        norm_gain,
        query_down_weight,
        query_latent_norm_gain,
        key_value_down_weight,
        key_value_latent_gain,
        w_rope_key,
        w_pool_in,
    )
    got = lax.all_to_all(message, "y", 0, 0, tiled=True).reshape(SIDE, 1024)
    kv0 = got[:, QR : QR + KR + 128]
    q_side = got[:, :QR]
    pool_own = got[:, QR + KR + 128 :]

    pool_other = across(pool_own)
    tail_rows = jnp.where(c == 1, pool_own[SIDE - 8 :], pool_other[SIDE - 8 :])
    head_rows = jnp.where(c == 0, pool_own[:8], pool_other[:8])
    count = NZ * NX
    low = lax.ppermute(tail_rows, ("z", "x"), [(i, i + 1) for i in range(count - 1)])
    high = lax.ppermute(head_rows, ("z", "x"), [(i + 1, i) for i in range(count - 1)])
    pooled = pooling(sc, pool_own, pool_other, low, high, mixw, scale)

    blocks = [kv0]
    fwd = back = kv0
    for step in range(1, 4):
        fwd = along_z(fwd, 1)
        back = along_z(back, -1)
        blocks += [fwd, back]
    fwd = along_z(fwd, 1)
    blocks.append(fwd)
    others = [across(b) for b in blocks]

    q_own = lax.all_to_all(
        jnp.broadcast_to(q_side[None], (NX, SIDE, QR)), "x", 0, 0, tiled=True
    )
    q_other = across(q_own)
    qt = queries(sc, q_own, q_other, wqt, qgain, tables)

    def kv(a, b):
        return keys_values(sc, blocks[a:b], others[a:b], a, wkvt, kgain, tables)

    carry = attend([kv(0, 3), kv(3, 5)], qt, None, False, "attend0", (pooled, wp, wb))
    partial = attend([kv(5, 7), kv(7, 8)], qt, carry, True, "attend1")

    merged = lax.all_to_all(partial, "x", 0, 0, tiled=True)
    keep, send, row_logsum = merge(sc, merged)
    theirs = across(send)
    parts = project(keep, theirs, pooled, w_out_attn, wb, wp)
    parts = lax.all_to_all(parts, "y", 0, 0, tiled=True)
    mixed = jnp.sum(parts.astype(f32), axis=0).astype(bf16)
    return mixed, row_logsum


def solution(mesh):
    fine = Mesh(mesh.devices.reshape(NZ, NX, NY, 2), ("z", "x", "y", "c"))
    tp = ("y", "c")
    placed = (
        P(("z", "x", "y", "c"), None),
        P(),
        P(),
        P(),
        P(),
        P(),
        P(),
        P(),
        P(None, tp),
        P(None, tp),
        P(),
        P(),
        P(tp, None, None),
        P(tp),
        P(tp, None),
        P(tp, None),
    )
    return jax.shard_map(
        shards,
        mesh=fine,
        in_specs=placed,
        out_specs=(P(("z", "x", "y", "c"), None), P(tp, ("z", "x"))),
        check_vma=False,
    )
```

```python
import jax
import jax.numpy as jnp
import numpy as np
from jax import lax
from jax.experimental import pallas as pl
from jax.experimental.pallas import tpu as pltpu
from jax.sharding import Mesh, PartitionSpec as P

NOPE = 64
ROT = 32
HALF = 16
HEAD = 96
VAL = 64
HEADS = 3
QR = 512
KR = 256
EPS = 1e-06
WIDTH = 2048
ROWS = 48
BLOCK = 384
SIDE = 192
TOKENS = 12288
LOG2E = 1.4426950408889634
LN2 = 0.6931471805599453
MSG = 208
VROWS = 80
QTILE = 512
NX = 4
NY = 4
NZ = 8
NQ = NX * BLOCK

bf16 = jnp.bfloat16
f32 = jnp.float32


def trig_tables(inner_places, outer_step, outer_count):
    freqs = 10000.0 ** (-np.arange(HALF, dtype=np.float64) / HALF)
    inner = freqs[:, None] * inner_places[None, :]
    outer = freqs[:, None] * (outer_step * np.arange(outer_count, dtype=np.float64))[None, :]
    pad = np.zeros((HALF, 128 - outer_count))
    cast = lambda a: a.astype(np.float32)
    return (
        cast(np.cos(inner)),
        cast(np.sin(inner)),
        cast(np.concatenate([np.cos(outer), pad], 1)),
        cast(np.concatenate([np.sin(outer), pad], 1)),
    )


def query_tables():
    return trig_tables(np.arange(BLOCK, dtype=np.float64), BLOCK, NZ * NX)


def key_tables():
    z = np.arange(NZ, dtype=np.float64)
    places = (NX * BLOCK * z[:, None] + np.arange(ROWS, dtype=np.float64)[None, :]).reshape(-1)
    return trig_tables(places, ROWS, NX * NY * 2)


def near(x):
    return pltpu.with_memory_space_constraint(x, pltpu.VMEM)


def vmem():
    return pl.BlockSpec(memory_space=pltpu.VMEM)


def smem():
    return pl.BlockSpec(memory_space=pltpu.SMEM)


def nt(a, b):
    return lax.dot_general(a, b, (((1,), (1,)), ((), ())), preferred_element_type=f32)


def nn(a, b):
    return lax.dot_general(a, b, (((1,), (0,)), ((), ())), preferred_element_type=f32)


def params(limit=24, **kw):
    return pltpu.CompilerParams(vmem_limit_bytes=limit * 1024 * 1024, **kw)


KSTEP = 512


def latents_body(
    tok, gain, qdw, qg, kdw, kg, rw, pw, q_out, kv_out, pool_out, inv, aq, ak, ar, ap
):
    k = pl.program_id(0)

    @pl.when(k == 0)
    def _():
        x = tok[...].astype(f32)
        inv[...] = jnp.broadcast_to(
            lax.rsqrt(jnp.mean(x * x, axis=-1, keepdims=True) + EPS), (ROWS, 128)
        )
        aq[...] = jnp.zeros_like(aq)
        ak[...] = jnp.zeros_like(ak)
        ar[...] = jnp.zeros_like(ar)
        ap[...] = jnp.zeros_like(ap)

    cols = pl.ds(pl.multiple_of(k * KSTEP, KSTEP), KSTEP)
    x = tok[:, cols].astype(f32)
    normed = (x * inv[:, 0:1] * gain[cols].astype(f32).reshape(1, KSTEP)).astype(bf16)
    aq[...] += nn(normed, qdw[...])
    ak[...] += nn(normed, kdw[...])
    ar[...] += nt(normed, rw[...])
    ap[...] += nn(normed, pw[...])

    @pl.when(k == pl.num_programs(0) - 1)
    def _():
        def norm(v, g):
            return (
                v
                * lax.rsqrt(jnp.mean(v * v, axis=-1, keepdims=True) + EPS)
                * g.astype(f32).reshape(1, -1)
            ).astype(bf16)

        q = norm(aq[...], qg[...])
        kv = norm(ak[...], kg[...])
        rope = jnp.concatenate(
            [ar[...].astype(bf16), jnp.zeros((ROWS, 128 - ROT), bf16)], axis=1
        )
        pool_out[...] = ap[...].astype(bf16)
        q_out[...] = q
        for n in range(NZ):
            kv_out[n, :, 0:KR] = kv
            kv_out[n, :, KR:] = rope


def latents(tok, gain, qdw, qg, kdw, kg, rw, pw):
    steps = WIDTH // KSTEP
    whole = lambda *s: pl.BlockSpec(s, lambda k: (0,) * len(s))
    part = lambda n: pl.BlockSpec((KSTEP, n), lambda k: (k, 0))
    return pl.pallas_call(
        latents_body,
        grid=(steps,),
        in_specs=[
            whole(ROWS, WIDTH),
            whole(WIDTH),
            part(QR),
            whole(QR),
            part(KR),
            whole(KR),
            pl.BlockSpec((ROT, KSTEP), lambda k: (0, k)),
            part(512),
        ],
        out_specs=(
            whole(ROWS, QR),
            whole(NZ, ROWS, KR + 128),
            whole(ROWS, 512),
        ),
        out_shape=(
            jax.ShapeDtypeStruct((ROWS, QR), bf16),
            jax.ShapeDtypeStruct((NZ, ROWS, KR + 128), bf16),
            jax.ShapeDtypeStruct((ROWS, 512), bf16),
        ),
        scratch_shapes=[
            pltpu.VMEM((ROWS, 128), f32),
            pltpu.VMEM((ROWS, QR), f32),
            pltpu.VMEM((ROWS, KR), f32),
            pltpu.VMEM((ROWS, ROT), f32),
            pltpu.VMEM((ROWS, 512), f32),
        ],
        compiler_params=params(dimension_semantics=("arbitrary",)),
        name="latents",
    )(tok, gain, qdw, qg, kdw, kg, rw.T, pw)


def angles(coff, soff, cb, sb, idx):
    lanes = lax.broadcasted_iota(jnp.int32, (HALF, 128), 1)
    hit = lanes == idx
    cbase = jnp.sum(jnp.where(hit, cb, 0.0), axis=1, keepdims=True)
    sbase = jnp.sum(jnp.where(hit, sb, 0.0), axis=1, keepdims=True)
    return cbase * coff - sbase * soff, sbase * coff + cbase * soff


def rotated(v, cosine, sine):
    a = v[NOPE : NOPE + HALF]
    b = v[NOPE + HALF :]
    return jnp.concatenate(
        [v[:NOPE], a * cosine - b * sine, a * sine + b * cosine, jnp.zeros_like(v[:ROT])],
        axis=0,
    )


def queries_body(sc, own0, own1, own2, own3, other, wqt, qgain, coff, soff, cb, sb, out):
    c = sc[0]
    own = (own0, own1, own2, own3)
    for x in range(NX):
        mine = own[x][...]
        twin = other[x]
        rows = []
        for y in range(NY):
            piece = slice(y * ROWS, (y + 1) * ROWS)
            rows.append(jnp.where(c == 0, mine[piece], twin[piece]))
            rows.append(jnp.where(c == 0, twin[piece], mine[piece]))
        q = nt(wqt[...], jnp.concatenate(rows, axis=0))
        place = sc[2] * NX + (sc[3] + NX - x) % NX
        cosine, sine = angles(coff[...], soff[...], cb[...], sb[...], place)
        at = pl.multiple_of(((sc[3] + NX - x) % NX) * BLOCK, BLOCK)
        for h in range(HEADS):
            v = q[h * HEAD : (h + 1) * HEAD]
            inv = lax.rsqrt(jnp.mean(v * v, axis=0, keepdims=True) + EPS)
            v = v * inv * qgain[...]
            v = rotated(v, cosine, sine) * (LOG2E * HEAD**-0.5)
            out[h, :, pl.ds(at, BLOCK)] = v.astype(bf16)


def queries(sc, own, other, wqt, qgain, tables):
    return pl.pallas_call(
        queries_body,
        in_specs=[smem()] + [vmem()] * 11,
        out_specs=vmem(),
        out_shape=jax.ShapeDtypeStruct((HEADS, 128, NQ), bf16),
        compiler_params=params(),
        name="queries",
    )(sc, *own, other, wqt, qgain, *tables)


def keys_body(a0, a1, a2, a3, a4, sc, own, other, wkvt, kgain, coff, soff, cb, sb, kbuf, vbuf):
    c, x = sc[0], sc[3]
    pick = (
        lax.broadcasted_iota(jnp.int32, (ROT, 128), 0)
        == lax.broadcasted_iota(jnp.int32, (ROT, 128), 1)
    ).astype(bf16)
    ones = (lax.broadcasted_iota(jnp.int32, (VROWS - VAL, BLOCK), 0) == 0).astype(bf16)
    blocks = [(own, k, k, c) for k in range(NY)] + [(other, k, k, 1 - c) for k in range(NY)]
    for b, (ref, at, y_from, c_from) in enumerate(blocks):
        lat = ref[at]
        kv = nt(wkvt[...], lat[:, :KR])
        rope = nt(pick, lat[:, KR:])
        rope_square = jnp.sum(rope * rope, axis=0, keepdims=True)
        place = (x * NY + y_from) * 2 + c_from
        cosine, sine = angles(coff[...], soff[...], cb[...], sb[...], place)
        cols = slice(b * BLOCK, (b + 1) * BLOCK)
        for h in range(HEADS):
            plain = kv[h * 128 : h * 128 + NOPE]
            total = jnp.sum(plain * plain, axis=0, keepdims=True) + rope_square
            inv = lax.rsqrt(total * (1.0 / HEAD) + EPS)
            k = jnp.concatenate([plain, rope], axis=0) * inv * kgain[...]
            k = rotated(k, cosine, sine).astype(bf16)
            kbuf[h, cols, :] = k.T
            vbuf[h, 0:VAL, cols] = kv[h * 128 + NOPE : (h + 1) * 128].astype(bf16)
            vbuf[h, VAL:, cols] = ones


def keys_values(after, sc, own, other, wkvt, kgain, tables):
    count = 2 * NY * BLOCK
    return pl.pallas_call(
        keys_body,
        in_specs=[pl.BlockSpec(memory_space=pl.ANY)] * 5 + [smem()] + [vmem()] * 8,
        out_specs=(vmem(), vmem()),
        out_shape=(
            pltpu.VMEM((HEADS, count, 128), bf16),
            pltpu.VMEM((HEADS, VROWS, count), bf16),
        ),
        compiler_params=params(),
        name="keys",
    )(*after, sc, own, other, wkvt, kgain, *tables)


CHUNK = 256
SUB = 128
TILES = HEADS * (NQ // QTILE)


def attend_body(sizes, first, last, extra, *refs):
    refs = list(refs)
    refs = refs[extra:]
    pairs = [(refs.pop(0), refs.pop(0)) for _ in sizes]
    qt = refs.pop(0)
    if not first:
        acc_in, m_in = refs[:2]
        refs = refs[2:]
    if last:
        msg = refs.pop(0)
        acc_s, m_s = refs[2:]
    else:
        acc_s, m_s = refs[:2]
        refs = refs[2:]
    bufs = refs[:2]
    chunks = []
    base = 0
    for (kr, vr), n in zip(pairs, sizes):
        for at in range(0, n, CHUNK):
            size = min(CHUNK, n - at)
            chunks.append((base + at, size, kr, vr, at))
        base += n

    def where(i):
        per = NQ // QTILE
        return i // per, pl.ds(pl.multiple_of((i % per) * QTILE, QTILE), QTILE)

    def score(i, chunk, buf, top):
        row, size, kr, _, at = chunk
        h, col = where(i)
        for sub in range(0, size, SUB):
            s = nn(kr[h, at + sub : at + sub + SUB, :], qt[h, :, col])
            buf[row + sub : row + sub + SUB, :] = s
            top = jnp.maximum(top, jnp.max(s.reshape(SUB // 8, 8, QTILE), axis=0))
        return top

    def weigh(i, chunk, buf, m):
        row, size, _, vr, at = chunk
        h, _ = where(i)
        p = jnp.exp2(buf[row : row + size, :] - m).astype(bf16)
        return nn(vr[h, :, at : at + size], p)

    low = jnp.full((8, QTILE), -1e30, f32)

    def settle(i, top):
        m = jnp.max(top, axis=0, keepdims=True)
        if first:
            return m
        h, col = where(i)
        return jnp.maximum(m, m_in[h, :, col])

    def finish(i, m, acc):
        h, col = where(i)
        if not first:
            acc = acc + acc_in[h, :, col] * jnp.exp2(m_in[h, :, col] - m)
        acc_s[h, :, col] = acc
        m_s[h, :, col] = m

    def both(i, m, buf, nxt):
        acc = None
        top = low
        for chunk in chunks:
            part = weigh(i, chunk, buf, m)
            acc = part if acc is None else acc + part
            top = score(i + 1, chunk, nxt, top)
        finish(i, m, acc)
        return settle(i + 1, top)

    top = low
    for chunk in chunks:
        top = score(0, chunk, bufs[0], top)
    m = settle(0, top)

    def pair(j, m):
        m = both(2 * j, m, bufs[0], bufs[1])
        return both(2 * j + 1, m, bufs[1], bufs[0])

    m = lax.fori_loop(0, (TILES - 1) // 2, pair, m)
    acc = None
    for chunk in chunks:
        part = weigh(TILES - 1, chunk, bufs[0], m)
        acc = part if acc is None else acc + part
    finish(TILES - 1, m, acc)

    if last:
        for x in range(NX):
            cols = slice(x * BLOCK, (x + 1) * BLOCK)
            stats = []
            for h in range(HEADS):
                total = acc_s[h, VAL : VAL + 1, cols]
                part = acc_s[h, 0:VAL, cols] * (1.0 / total)
                msg[x, h * VAL : (h + 1) * VAL, :] = part.astype(bf16)
                lse = (m_s[h, :, cols] + jnp.log2(total)) * LN2
                hi = lse.astype(bf16)
                rest = lse - hi.astype(f32)
                mid = rest.astype(bf16)
                low_part = (rest - mid.astype(f32)).astype(bf16)
                stats += [hi.astype(f32), mid.astype(f32), low_part.astype(f32)]
            stats.append(jnp.zeros((MSG - HEADS * VAL - 9, BLOCK), f32))
            msg[x, HEADS * VAL :, :] = jnp.concatenate(stats, axis=0).astype(bf16)


def attend(pairs, qt, carry, last, after=()):
    sizes = [k.shape[1] for k, _ in pairs]
    first = carry is None
    state = (
        jax.ShapeDtypeStruct((HEADS, VROWS, NQ), f32),
        jax.ShapeDtypeStruct((HEADS, 1, NQ), f32),
    )
    if last:
        out_shape = pltpu.VMEM((NX, MSG, BLOCK), bf16)
        out_specs = vmem()
    else:
        out_shape = state
        out_specs = (vmem(), vmem())
    args = [near(a) for pair in pairs for a in pair] + [qt] + ([] if first else list(carry))
    scratch = [pltpu.VMEM((sum(sizes), QTILE), f32) for _ in range(2)]
    if last:
        scratch += [pltpu.VMEM(t.shape, t.dtype) for t in state]

    def body(*refs):
        attend_body(sizes, first, last, len(after), *refs)

    return pl.pallas_call(
        body,
        in_specs=[pl.BlockSpec(memory_space=pl.ANY)] * len(after) + [vmem()] * len(args),
        out_specs=out_specs,
        out_shape=out_shape,
        scratch_shapes=scratch,
        compiler_params=params(40),
    )(*after, *args)


def merge_body(sc, msg, keep, send, lse_out, buf):
    c = sc[0]
    for h in range(HEADS):
        logs = []
        for x in range(NX):
            tail = msg[x, HEADS * VAL :, :].astype(f32)
            r = 3 * h
            logs.append(tail[r : r + 1] + tail[r + 1 : r + 2] + tail[r + 2 : r + 3])
        top = jnp.maximum(jnp.maximum(logs[0], logs[1]), jnp.maximum(logs[2], logs[3]))
        weights = [jnp.exp(v - top) for v in logs]
        total = weights[0] + weights[1] + weights[2] + weights[3]
        lse_out[h : h + 1, :] = top + jnp.log(total)
        inv = 1.0 / total
        acc = jnp.zeros((VAL, BLOCK), f32)
        for x in range(NX):
            acc = acc + msg[x, h * VAL : (h + 1) * VAL, :].astype(f32) * (weights[x] * inv)
        buf[:, h * VAL : (h + 1) * VAL] = acc.T.astype(bf16)
    for y in range(NY):
        dst = slice(y * ROWS, (y + 1) * ROWS)
        at = pl.multiple_of(y * 2 * ROWS + c * ROWS, ROWS)
        keep[dst, :] = buf[pl.ds(at, ROWS), :]
        to = pl.multiple_of(y * 2 * ROWS + (1 - c) * ROWS, ROWS)
        send[dst, :] = buf[pl.ds(to, ROWS), :]


def merge(sc, msg):
    return pl.pallas_call(
        merge_body,
        in_specs=[smem(), vmem()],
        out_specs=(vmem(), vmem(), vmem()),
        out_shape=(
            pltpu.VMEM((SIDE, HEADS * VAL), bf16),
            pltpu.VMEM((SIDE, HEADS * VAL), bf16),
            jax.ShapeDtypeStruct((HEADS, BLOCK), f32),
        ),
        scratch_shapes=[pltpu.VMEM((BLOCK, HEADS * VAL), bf16)],
        compiler_params=params(),
        name="merge",
    )(sc, near(msg))


def pool_body(sc, own, low, high, out):
    first = ((sc[2] * NX + sc[3]) * NY * 2 + sc[1] * 2 + sc[0]) * ROWS
    x = own[...].astype(f32)
    side = jnp.zeros((8, 512), f32)
    window = jnp.concatenate(
        [side, low[...].astype(f32), x, high[...].astype(f32), side], axis=0
    )
    n = ROWS + 32
    s1 = window[0 : n - 1] + window[1:n]
    s2 = s1[0 : n - 3] + s1[2 : n - 1]
    s4 = s2[0 : n - 7] + s2[4 : n - 3]
    s8 = s4[0 : n - 15] + s4[8 : n - 7]
    w1 = s1[15 : 15 + ROWS]
    w2 = s2[14 : 14 + ROWS]
    w4 = s4[12 : 12 + ROWS]
    w8 = s8[8 : 8 + ROWS]
    group = (lax.broadcasted_iota(jnp.int32, (ROWS, 512), 1) // 64) % 4
    total = jnp.where(
        group == 0, w1, jnp.where(group == 1, w2, jnp.where(group == 2, w4, w8))
    )
    half = jnp.where(group == 0, 1, jnp.where(group == 1, 2, jnp.where(group == 2, 4, 8)))
    place = first + lax.broadcasted_iota(jnp.int32, (ROWS, 512), 0)
    count = (jnp.minimum(place + half, TOKENS) - jnp.maximum(place - half, 0)).astype(f32)
    pooled = (total / count - x).astype(bf16)
    for y in range(NY):
        out[y, :, :] = pooled[:, y * 128 : (y + 1) * 128]


def pooling(sc, own, low, high):
    return pl.pallas_call(
        pool_body,
        in_specs=[smem()] + [vmem()] * 3,
        out_specs=vmem(),
        out_shape=jax.ShapeDtypeStruct((NY, ROWS, 128), bf16),
        compiler_params=params(),
        name="pooling",
    )(sc, own, low, high)


def project_body(mine, theirs, pooled, mixw, scale, wa, wb, wp, out):
    mapped = nn(pooled[...].reshape(SIDE, 128), mixw[...])
    extra = (mapped * scale[...]).astype(bf16)
    total = nn(mine[...], wa[...]) + nn(theirs[...], wb[...]) + nn(extra, wp[...])
    for y in range(NY):
        out[y, :, :] = total[y * ROWS : (y + 1) * ROWS].astype(bf16)


def project(mine, theirs, pooled, mixw, scale, wa, wb, wp):
    args = [near(a) for a in (mine, theirs, pooled, mixw, scale, wa, wb, wp)]
    return pl.pallas_call(
        project_body,
        in_specs=[vmem()] * 8,
        out_specs=vmem(),
        out_shape=pltpu.VMEM((NY, ROWS, WIDTH), bf16),
        compiler_params=params(),
        name="project",
    )(*args)


def across(x):
    return lax.ppermute(x, "c", [(0, 1), (1, 0)])


def shifted(x, axis, places):
    count = lax.axis_size(axis)
    return lax.ppermute(x, axis, [(i, (i + places) % count) for i in range(count)])


def order_body(y_ref, a, b, c, d, out):
    y = y_ref[0]
    for k, ref in enumerate((a, b, c, d)):
        at = pl.multiple_of(((y + NY - k) % NY) * ROWS, ROWS)
        out[pl.ds(at, ROWS), :] = ref[...]


def in_order(pieces, y):
    return pl.pallas_call(
        order_body,
        in_specs=[smem()] + [vmem()] * NY,
        out_specs=vmem(),
        out_shape=jax.ShapeDtypeStruct((NY * ROWS, QR), bf16),
        compiler_params=params(),
        name="order",
    )(y.astype(jnp.int32).reshape(1), *pieces)


def shards(
    tokens,
    norm_gain,
    query_down_weight,
    query_latent_norm_gain,
    key_value_down_weight,
    key_value_latent_gain,
    w_rope_key,
    w_pool_in,
    query_up_weight,
    key_value_up_weight,
    query_gain,
    key_gain,
    w_pool_mix,
    pool_scale,
    w_out_attn,
    w_out_pool,
):
    z = lax.axis_index("z")
    x = lax.axis_index("x")
    y = lax.axis_index("y")
    c = lax.axis_index("c")
    sc = jnp.stack([c, y, z, x]).astype(jnp.int32)
    wqt = query_up_weight.T
    wkvt = key_value_up_weight.T
    qgain = query_gain.astype(f32).reshape(HEAD, 1)
    kgain = key_gain.astype(f32).reshape(HEAD, 1)

    wb = across(w_out_attn)
    wp_other = across(w_out_pool)
    mix_other = across(w_pool_mix[0])
    scale_other = across(pool_scale)
    wp = jnp.where(
        c == 0,
        jnp.concatenate([w_out_pool, wp_other], 0),
        jnp.concatenate([wp_other, w_out_pool], 0),
    )
    zero = jnp.zeros((64, 64), bf16)
    mix0 = jnp.where(c == 0, w_pool_mix[0], mix_other)
    mix1 = jnp.where(c == 0, mix_other, w_pool_mix[0])
    mixw = jnp.concatenate(
        [jnp.concatenate([mix0, zero], 1), jnp.concatenate([zero, mix1], 1)], 0
    )
    scale = jnp.where(
        c == 0,
        jnp.concatenate([pool_scale, scale_other]),
        jnp.concatenate([scale_other, pool_scale]),
    ).astype(f32).reshape(1, 128)

    q_all, kv_all, pool_in = latents(
        tokens,
        norm_gain,
        query_down_weight,
        query_latent_norm_gain,
        key_value_down_weight,
        key_value_latent_gain,
        w_rope_key,
        w_pool_in,
    )
    q_side = [q_all] + [shifted(q_all, "y", k) for k in range(1, NY)]
    kv_own = lax.all_to_all(kv_all, "z", 0, 0, tiled=True).reshape(NZ * ROWS, KR + 128)
    kv = lax.all_to_all(jnp.broadcast_to(kv_own[None], (NY, *kv_own.shape)), "y", 0, 0, tiled=True)
    q_side = in_order(q_side, lax.axis_index("y"))
    q_own = [q_side] + [shifted(q_side, "x", k) for k in range(1, NX)]

    count = NZ * NX * NY * 2
    every = ("z", "x", "y", "c")
    low = lax.ppermute(
        pool_in[ROWS - 8 :], every, [(i, i + 1) for i in range(count - 1)]
    )
    high = lax.ppermute(pool_in[:8], every, [(i + 1, i) for i in range(count - 1)])
    pooled = pooling(sc, pool_in, low, high)
    pooled = lax.all_to_all(pooled, "y", 0, 0, tiled=True)

    q_pile = jnp.stack(q_own)
    q_twin = across(q_pile)
    qt = queries(sc, q_own, q_twin, wqt, qgain, query_tables())
    kv_twin = across(kv)
    after = (pooled, wp, wb, mixw, scale)
    pair = keys_values(after, sc, kv, kv_twin, wkvt, kgain, key_tables())
    partial = attend([pair], qt, None, True)

    merged = lax.all_to_all(partial, "x", 0, 0, tiled=True)
    keep, send, row_logsum = merge(sc, merged)
    parts = project(keep, across(send), pooled, mixw, scale, w_out_attn, wb, wp)
    parts = lax.all_to_all(parts, "y", 0, 0, tiled=True)
    mixed = jnp.sum(parts.astype(f32), axis=0).astype(bf16)
    return mixed, row_logsum


def solution(mesh):
    fine = Mesh(mesh.devices.reshape(NZ, NX, NY, 2), ("z", "x", "y", "c"))
    tp = ("y", "c")
    placed = (
        P(("z", "x", "y", "c"), None),
        P(),
        P(),
        P(),
        P(),
        P(),
        P(),
        P(),
        P(None, tp),
        P(None, tp),
        P(),
        P(),
        P(tp, None, None),
        P(tp),
        P(tp, None),
        P(tp, None),
    )

    return jax.shard_map(
        shards,
        mesh=fine,
        in_specs=placed,
        out_specs=(P(("z", "x", "y", "c"), None), P(tp, ("z", "x"))),
        check_vma=False,
    )
```

```python
import jax
import jax.numpy as jnp
import numpy as np
from jax import lax
from jax.experimental import pallas as pl
from jax.experimental.pallas import tpu as pltpu
from jax.sharding import Mesh, PartitionSpec as P

NOPE = 64
ROT = 32
HALF = 16
HEAD = 96
VAL = 64
HEADS = 3
QR = 512
KR = 256
EPS = 1e-06
WIDTH = 2048
ROWS = 48
BLOCK = 384
SIDE = 192
TOKENS = 12288
LOG2E = 1.4426950408889634
LN2 = 0.6931471805599453
MSG = 208
VROWS = 80
QTILE = 512
NX = 4
NY = 4
NZ = 8
NQ = NX * BLOCK

bf16 = jnp.bfloat16
f32 = jnp.float32


def trig_tables(inner_places, outer_step, outer_count):
    freqs = 10000.0 ** (-np.arange(HALF, dtype=np.float64) / HALF)
    inner = freqs[:, None] * inner_places[None, :]
    outer = freqs[:, None] * (outer_step * np.arange(outer_count, dtype=np.float64))[None, :]
    pad = np.zeros((HALF, 128 - outer_count))
    cast = lambda a: a.astype(np.float32)
    parts = [np.cos(inner), np.sin(inner), np.cos(outer), pad, np.sin(outer), pad]
    return cast(np.concatenate(parts, 1))


def query_tables():
    return trig_tables(np.arange(BLOCK, dtype=np.float64), BLOCK, NZ * NX)


def key_tables():
    z = np.arange(NZ, dtype=np.float64)
    places = (NX * BLOCK * z[:, None] + np.arange(ROWS, dtype=np.float64)[None, :]).reshape(-1)
    return trig_tables(places, ROWS, NX * NY * 2)


def near(x):
    return pltpu.with_memory_space_constraint(x, pltpu.VMEM)


def vmem():
    return pl.BlockSpec(memory_space=pltpu.VMEM)


def nt(a, b):
    return lax.dot_general(a, b, (((1,), (1,)), ((), ())), preferred_element_type=f32)


def nn(a, b):
    return lax.dot_general(a, b, (((1,), (0,)), ((), ())), preferred_element_type=f32)


def params(limit=56, **kw):
    return pltpu.CompilerParams(vmem_limit_bytes=limit * 1024 * 1024, **kw)


KSTEP = 1024


def latents_body(
    tok, gain, qdw, qg, kdw, kg, rw, pw, m0, m1, m2, m3, kv_out, inv, aq, ak, ar, ap, pb
):
    k = pl.program_id(0)

    @pl.when(k == 0)
    def _():
        x = tok[...].astype(f32)
        inv[...] = jnp.broadcast_to(
            lax.rsqrt(jnp.mean(x * x, axis=-1, keepdims=True) + EPS), (ROWS, 128)
        )
        aq[...] = jnp.zeros_like(aq)
        ak[...] = jnp.zeros_like(ak)
        ar[...] = jnp.zeros_like(ar)
        ap[...] = jnp.zeros_like(ap)

    cols = pl.ds(pl.multiple_of(k * KSTEP, KSTEP), KSTEP)
    x = tok[:, cols].astype(f32)
    normed = (x * inv[:, 0:1] * gain[cols].astype(f32).reshape(1, KSTEP)).astype(bf16)
    aq[...] += nn(normed, qdw[...])
    ak[...] += nn(normed, kdw[...])
    ar[...] += nt(normed, rw[...])
    ap[...] += nn(normed, pw[...])

    @pl.when(k == pl.num_programs(0) - 1)
    def _():
        def norm(v, g):
            return (
                v
                * lax.rsqrt(jnp.mean(v * v, axis=-1, keepdims=True) + EPS)
                * g.astype(f32).reshape(1, -1)
            ).astype(bf16)

        q = norm(aq[...], qg[...])
        kv = norm(ak[...], kg[...])
        rope = jnp.concatenate(
            [ar[...].astype(bf16), jnp.zeros((ROWS, 128 - ROT), bf16)], axis=1
        )
        pb[...] = ap[...].astype(bf16)
        y = lax.axis_index("y")
        for n, out in enumerate((m0, m1, m2, m3)):
            cols = pl.ds(pl.multiple_of(((y + n) % NY) * 128, 128), 128)
            out[:, 0:QR] = q
            out[:, QR:] = pb[:, cols]
        for n in range(NZ):
            kv_out[n, :, 0:KR] = kv
            kv_out[n, :, KR:] = rope


def latents(tok, gain, qdw, qg, kdw, kg, rw, pw):
    steps = WIDTH // KSTEP
    whole = lambda *s: pl.BlockSpec(s, lambda k: (0,) * len(s))
    part = lambda n: pl.BlockSpec((KSTEP, n), lambda k: (k, 0))
    return pl.pallas_call(
        latents_body,
        grid=(steps,),
        in_specs=[
            whole(ROWS, WIDTH),
            whole(WIDTH),
            part(QR),
            whole(QR),
            part(KR),
            whole(KR),
            pl.BlockSpec((ROT, KSTEP), lambda k: (0, k)),
            part(512),
        ],
        out_specs=(
            *[whole(ROWS, QR + 128)] * NY,
            whole(NZ, ROWS, KR + 128),
        ),
        out_shape=(
            *[jax.ShapeDtypeStruct((ROWS, QR + 128), bf16)] * NY,
            jax.ShapeDtypeStruct((NZ, ROWS, KR + 128), bf16),
        ),
        scratch_shapes=[
            pltpu.VMEM((ROWS, 128), f32),
            pltpu.VMEM((ROWS, QR), f32),
            pltpu.VMEM((ROWS, KR), f32),
            pltpu.VMEM((ROWS, ROT), f32),
            pltpu.VMEM((ROWS, 512), f32),
            pltpu.VMEM((ROWS, 512), bf16),
        ],
        compiler_params=params(dimension_semantics=("arbitrary",)),
        name="latents",
    )(tok, gain, qdw, qg, kdw, kg, rw.T, pw)


def angles(table, idx):
    lanes = lax.broadcasted_iota(jnp.int32, (HALF, 128), 1)
    hit = lanes == idx
    coff = table[:, 0:BLOCK]
    soff = table[:, BLOCK : 2 * BLOCK]
    cb = table[:, 2 * BLOCK : 2 * BLOCK + 128]
    sb = table[:, 2 * BLOCK + 128 :]
    cbase = jnp.sum(jnp.where(hit, cb, 0.0), axis=1, keepdims=True)
    sbase = jnp.sum(jnp.where(hit, sb, 0.0), axis=1, keepdims=True)
    return cbase * coff - sbase * soff, sbase * coff + cbase * soff


def column(gain):
    row = jnp.broadcast_to(gain[...].astype(f32).reshape(1, HEAD), (8, HEAD)).astype(bf16)
    eye = (
        lax.broadcasted_iota(jnp.int32, (HEAD, HEAD), 0)
        == lax.broadcasted_iota(jnp.int32, (HEAD, HEAD), 1)
    ).astype(bf16)
    return nt(eye, row)[:, 0:1]


def rotated(v, cosine, sine):
    a = v[NOPE : NOPE + HALF]
    b = v[NOPE + HALF :]
    return jnp.concatenate(
        [v[:NOPE], a * cosine - b * sine, a * sine + b * cosine, jnp.zeros_like(v[:ROT])],
        axis=0,
    )


def queries_body(own0, own1, own2, own3, other, wqt, gain, table, out):
    c = lax.axis_index("c")
    z = lax.axis_index("z")
    here = lax.axis_index("x")
    qgain = column(gain)
    own = (own0, own1, own2, own3)
    for x in range(NX):
        mine = own[x][...]
        twin = other[x]
        rows = []
        for y in range(NY):
            piece = slice(y * ROWS, (y + 1) * ROWS)
            rows.append(jnp.where(c == 0, mine[piece], twin[piece]))
            rows.append(jnp.where(c == 0, twin[piece], mine[piece]))
        q = nt(wqt[...], jnp.concatenate(rows, axis=0))
        block = (here + NX - x) % NX
        place = z * NX + block
        cosine, sine = angles(table, place)
        at = pl.multiple_of(block * BLOCK, BLOCK)
        for h in range(HEADS):
            v = q[h * HEAD : (h + 1) * HEAD]
            inv = lax.rsqrt(jnp.mean(v * v, axis=0, keepdims=True) + EPS)
            v = v * inv * qgain
            v = rotated(v, cosine, sine) * (LOG2E * HEAD**-0.5)
            out[h, :, pl.ds(at, BLOCK)] = v.astype(bf16)


def queries(own, other, wqt, qgain, table):
    return pl.pallas_call(
        queries_body,
        in_specs=[vmem()] * 8,
        out_specs=vmem(),
        out_shape=pltpu.VMEM((HEADS, 128, NQ), bf16),
        compiler_params=params(),
        name="queries",
    )(*own, other, wqt, qgain, table)


def keys_body(count, *refs):
    own, other, wkvt, gain, table, kbuf, vbuf = refs[count:]
    c = lax.axis_index("c")
    x = lax.axis_index("x")
    kgain = column(gain)
    pick = (
        lax.broadcasted_iota(jnp.int32, (ROT, 128), 0)
        == lax.broadcasted_iota(jnp.int32, (ROT, 128), 1)
    ).astype(bf16)
    ones = (lax.broadcasted_iota(jnp.int32, (VROWS - VAL, BLOCK), 0) == 0).astype(bf16)
    blocks = [(own, k, k, c) for k in range(NY)] + [(other, k, k, 1 - c) for k in range(NY)]
    for b, (ref, at, y_from, c_from) in enumerate(blocks):
        lat = ref[at]
        kv = nt(wkvt[...], lat[:, :KR])
        rope = nt(pick, lat[:, KR:])
        rope_square = jnp.sum(rope * rope, axis=0, keepdims=True)
        place = (x * NY + y_from) * 2 + c_from
        cosine, sine = angles(table, place)
        cols = slice(b * BLOCK, (b + 1) * BLOCK)
        for h in range(HEADS):
            plain = kv[h * 128 : h * 128 + NOPE]
            total = jnp.sum(plain * plain, axis=0, keepdims=True) + rope_square
            inv = lax.rsqrt(total * (1.0 / HEAD) + EPS)
            k = jnp.concatenate([plain, rope], axis=0) * inv * kgain
            k = rotated(k, cosine, sine).astype(bf16)
            kbuf[h, cols, :] = k.T
            vbuf[h, 0:VAL, cols] = kv[h * 128 + NOPE : (h + 1) * 128].astype(bf16)
            vbuf[h, VAL:, cols] = ones


def keys_values(after, own, other, wkvt, kgain, table):
    count = 2 * NY * BLOCK

    def body(*refs):
        keys_body(len(after), *refs)

    return pl.pallas_call(
        body,
        in_specs=[pl.BlockSpec(memory_space=pl.ANY)] * len(after) + [vmem()] * 5,
        out_specs=(vmem(), vmem()),
        out_shape=(
            pltpu.VMEM((HEADS, count, 128), bf16),
            pltpu.VMEM((HEADS, VROWS, count), bf16),
        ),
        compiler_params=params(),
        name="keys",
    )(*after, own, other, wkvt, kgain, table)


CHUNK = 256
SUB = 128
TILES = HEADS * (NQ // QTILE)


def attend_body(sizes, first, last, extra, *refs):
    refs = list(refs)
    refs = refs[extra:]
    pairs = [(refs.pop(0), refs.pop(0)) for _ in sizes]
    qt = refs.pop(0)
    if not first:
        acc_in, m_in = refs[:2]
        refs = refs[2:]
    if last:
        msg = refs.pop(0)
        acc_s, m_s = refs[2:]
    else:
        acc_s, m_s = refs[:2]
        refs = refs[2:]
    bufs = refs[:2]
    chunks = []
    base = 0
    for (kr, vr), n in zip(pairs, sizes):
        for at in range(0, n, CHUNK):
            size = min(CHUNK, n - at)
            chunks.append((base + at, size, kr, vr, at))
        base += n

    def where(i):
        per = NQ // QTILE
        return i // per, pl.ds(pl.multiple_of((i % per) * QTILE, QTILE), QTILE)

    def score(i, chunk, buf, top):
        row, size, kr, _, at = chunk
        h, col = where(i)
        for sub in range(0, size, SUB):
            s = nn(kr[h, at + sub : at + sub + SUB, :], qt[h, :, col])
            buf[row + sub : row + sub + SUB, :] = s
            top = jnp.maximum(top, jnp.max(s.reshape(SUB // 8, 8, QTILE), axis=0))
        return top

    def weigh(i, chunk, buf, m):
        row, size, _, vr, at = chunk
        h, _ = where(i)
        p = jnp.exp2(buf[row : row + size, :] - m).astype(bf16)
        return nn(vr[h, :, at : at + size], p)

    low = jnp.full((8, QTILE), -1e30, f32)

    def settle(i, top):
        m = jnp.max(top, axis=0, keepdims=True)
        if first:
            return m
        h, col = where(i)
        return jnp.maximum(m, m_in[h, :, col])

    def finish(i, m, acc):
        h, col = where(i)
        if not first:
            acc = acc + acc_in[h, :, col] * jnp.exp2(m_in[h, :, col] - m)
        acc_s[h, :, col] = acc
        m_s[h, :, col] = m

    def both(i, m, buf, nxt):
        acc = None
        top = low
        for chunk in chunks:
            part = weigh(i, chunk, buf, m)
            acc = part if acc is None else acc + part
            top = score(i + 1, chunk, nxt, top)
        finish(i, m, acc)
        return settle(i + 1, top)

    top = low
    for chunk in chunks:
        top = score(0, chunk, bufs[0], top)
    m = settle(0, top)

    def pair(j, m):
        m = both(2 * j, m, bufs[0], bufs[1])
        return both(2 * j + 1, m, bufs[1], bufs[0])

    m = lax.fori_loop(0, (TILES - 1) // 2, pair, m)
    acc = None
    for chunk in chunks:
        part = weigh(TILES - 1, chunk, bufs[0], m)
        acc = part if acc is None else acc + part
    finish(TILES - 1, m, acc)

    if last:
        for x in range(NX):
            cols = slice(x * BLOCK, (x + 1) * BLOCK)
            stats = []
            for h in range(HEADS):
                total = acc_s[h, VAL : VAL + 1, cols]
                part = acc_s[h, 0:VAL, cols] * (1.0 / total)
                msg[x, h * VAL : (h + 1) * VAL, :] = part.astype(bf16)
                lse = (m_s[h, :, cols] + jnp.log2(total)) * LN2
                hi = lse.astype(bf16)
                rest = lse - hi.astype(f32)
                mid = rest.astype(bf16)
                low_part = (rest - mid.astype(f32)).astype(bf16)
                stats += [hi.astype(f32), mid.astype(f32), low_part.astype(f32)]
            stats.append(jnp.zeros((MSG - HEADS * VAL - 9, BLOCK), f32))
            msg[x, HEADS * VAL :, :] = jnp.concatenate(stats, axis=0).astype(bf16)


def attend(pairs, qt, carry, last, after=()):
    sizes = [k.shape[1] for k, _ in pairs]
    first = carry is None
    state = (
        jax.ShapeDtypeStruct((HEADS, VROWS, NQ), f32),
        jax.ShapeDtypeStruct((HEADS, 1, NQ), f32),
    )
    if last:
        out_shape = pltpu.VMEM((NX, MSG, BLOCK), bf16)
        out_specs = vmem()
    else:
        out_shape = state
        out_specs = (vmem(), vmem())
    args = [near(a) for pair in pairs for a in pair] + [near(qt)]
    args += [] if first else list(carry)
    scratch = [pltpu.VMEM((sum(sizes), QTILE), f32) for _ in range(2)]
    if last:
        scratch += [pltpu.VMEM(t.shape, t.dtype) for t in state]

    def body(*refs):
        attend_body(sizes, first, last, len(after), *refs)

    return pl.pallas_call(
        body,
        in_specs=[pl.BlockSpec(memory_space=pl.ANY)] * len(after) + [vmem()] * len(args),
        out_specs=out_specs,
        out_shape=out_shape,
        scratch_shapes=scratch,
        compiler_params=params(40),
    )(*after, *args)


def merge_body(msg, keep, send, lse_out, buf):
    c = lax.axis_index("c")
    for h in range(HEADS):
        logs = []
        for x in range(NX):
            tail = msg[x, HEADS * VAL :, :].astype(f32)
            r = 3 * h
            logs.append(tail[r : r + 1] + tail[r + 1 : r + 2] + tail[r + 2 : r + 3])
        top = jnp.maximum(jnp.maximum(logs[0], logs[1]), jnp.maximum(logs[2], logs[3]))
        weights = [jnp.exp(v - top) for v in logs]
        total = weights[0] + weights[1] + weights[2] + weights[3]
        lse_out[h : h + 1, :] = top + jnp.log(total)
        inv = 1.0 / total
        acc = jnp.zeros((VAL, BLOCK), f32)
        for x in range(NX):
            acc = acc + msg[x, h * VAL : (h + 1) * VAL, :].astype(f32) * (weights[x] * inv)
        buf[:, h * VAL : (h + 1) * VAL] = acc.T.astype(bf16)
    for y in range(NY):
        dst = slice(y * ROWS, (y + 1) * ROWS)
        at = pl.multiple_of(y * 2 * ROWS + c * ROWS, ROWS)
        keep[dst, :] = buf[pl.ds(at, ROWS), :]
        to = pl.multiple_of(y * 2 * ROWS + (1 - c) * ROWS, ROWS)
        send[dst, :] = buf[pl.ds(to, ROWS), :]


def merge(msg):
    return pl.pallas_call(
        merge_body,
        in_specs=[vmem()],
        out_specs=(vmem(), vmem(), vmem()),
        out_shape=(
            pltpu.VMEM((SIDE, HEADS * VAL), bf16),
            pltpu.VMEM((SIDE, HEADS * VAL), bf16),
            jax.ShapeDtypeStruct((HEADS, BLOCK), f32),
        ),
        scratch_shapes=[pltpu.VMEM((BLOCK, HEADS * VAL), bf16)],
        compiler_params=params(24),
        name="merge",
    )(near(msg))


def pool_body(own, other, low, high, mixw, scale, out, xs):
    c, y0, z, x0 = [lax.axis_index(n) for n in "cyzx"]
    xs[0:8, :] = jnp.zeros((8, 128), f32)
    xs[8:16, :] = low[...].astype(f32)
    xs[16 + BLOCK : 24 + BLOCK, :] = high[...].astype(f32)
    xs[24 + BLOCK : 32 + BLOCK, :] = jnp.zeros((8, 128), f32)
    for y in range(NY):
        src = slice(y * ROWS, (y + 1) * ROWS)
        at = pl.multiple_of(16 + y * 2 * ROWS + c * ROWS, 16)
        xs[pl.ds(at, ROWS), :] = own[src, :].astype(f32)
        to = pl.multiple_of(16 + y * 2 * ROWS + (1 - c) * ROWS, 16)
        xs[pl.ds(to, ROWS), :] = other[src, :].astype(f32)
    lane = lax.broadcasted_iota(jnp.int32, (ROWS, 128), 1)
    second = lane >= 64
    wide = (y0 % 2) == 1
    half = jnp.where(wide, jnp.where(second, 8, 4), jnp.where(second, 2, 1))
    for y in range(NY):
        row0 = y * 2 * ROWS + c * ROWS
        window = xs[pl.ds(pl.multiple_of(row0, 16), ROWS + 32), :]
        n = ROWS + 32
        x = window[16 : 16 + ROWS]
        s1 = window[0 : n - 1] + window[1:n]
        s2 = s1[0 : n - 3] + s1[2 : n - 1]
        s4 = s2[0 : n - 7] + s2[4 : n - 3]
        s8 = s4[0 : n - 15] + s4[8 : n - 7]
        w1 = s1[15 : 15 + ROWS]
        w2 = s2[14 : 14 + ROWS]
        w4 = s4[12 : 12 + ROWS]
        w8 = s8[8 : 8 + ROWS]
        total = jnp.where(wide, jnp.where(second, w8, w4), jnp.where(second, w2, w1))
        place = (
            (z * NX + x0) * BLOCK + row0 + lax.broadcasted_iota(jnp.int32, (ROWS, 128), 0)
        )
        count = (jnp.minimum(place + half, TOKENS) - jnp.maximum(place - half, 0)).astype(f32)
        pooled = (total / count - x).astype(bf16)
        mapped = nn(pooled, mixw[...])
        out[y * ROWS : (y + 1) * ROWS, :] = (mapped * scale[...]).astype(bf16)


def pooling(own, other, low, high, mixw, scale):
    return pl.pallas_call(
        pool_body,
        in_specs=[vmem()] * 6,
        out_specs=vmem(),
        out_shape=jax.ShapeDtypeStruct((SIDE, 128), bf16),
        scratch_shapes=[pltpu.VMEM((BLOCK + 32, 128), f32)],
        compiler_params=params(),
        name="pooling",
    )(own, other, low, high, mixw, scale)


def project_body(mine, theirs, pooled, wa, wb, wp, out):
    total = nn(mine[...], wa[...]) + nn(theirs[...], wb[...]) + nn(pooled[...], wp[...])
    for y in range(NY):
        out[y, :, :] = total[y * ROWS : (y + 1) * ROWS].astype(bf16)


def project(mine, theirs, pooled, wa, wb, wp):
    args = [near(a) for a in (mine, theirs, pooled, wa, wb, wp)]
    return pl.pallas_call(
        project_body,
        in_specs=[vmem()] * 6,
        out_specs=vmem(),
        out_shape=pltpu.VMEM((NY, ROWS, WIDTH), bf16),
        compiler_params=params(24),
        name="project",
    )(*args)


def across(x):
    return lax.ppermute(x, "c", [(0, 1), (1, 0)])


def shifted(x, axis, places):
    count = lax.axis_size(axis)
    return lax.ppermute(x, axis, [(i, (i + places) % count) for i in range(count)])


def order_body(a, b, c, d, q_out, pool_out):
    y = lax.axis_index("y")
    for k, ref in enumerate((a, b, c, d)):
        at = pl.multiple_of(((y + NY - k) % NY) * ROWS, ROWS)
        q_out[pl.ds(at, ROWS), :] = ref[:, 0:QR]
        pool_out[pl.ds(at, ROWS), :] = ref[:, QR:]


def in_order(pieces):
    return pl.pallas_call(
        order_body,
        in_specs=[vmem()] * NY,
        out_specs=(vmem(), vmem()),
        out_shape=(
            jax.ShapeDtypeStruct((NY * ROWS, QR), bf16),
            jax.ShapeDtypeStruct((NY * ROWS, 128), bf16),
        ),
        compiler_params=params(),
        name="order",
    )(*pieces)


def shards(
    tokens,
    norm_gain,
    query_down_weight,
    query_latent_norm_gain,
    key_value_down_weight,
    key_value_latent_gain,
    w_rope_key,
    w_pool_in,
    query_up_weight,
    key_value_up_weight,
    query_gain,
    key_gain,
    w_pool_mix,
    pool_scale,
    w_out_attn,
    w_out_pool,
):
    c = lax.axis_index("c")
    wqt = query_up_weight.T
    wkvt = key_value_up_weight.T

    wb = across(w_out_attn)
    wp_other = across(w_out_pool)
    mix_other = across(w_pool_mix[0])
    scale_other = across(pool_scale)
    wp = jnp.where(
        c == 0,
        jnp.concatenate([w_out_pool, wp_other], 0),
        jnp.concatenate([wp_other, w_out_pool], 0),
    )
    zero = jnp.zeros((64, 64), bf16)
    mix0 = jnp.where(c == 0, w_pool_mix[0], mix_other)
    mix1 = jnp.where(c == 0, mix_other, w_pool_mix[0])
    mixw = jnp.concatenate(
        [jnp.concatenate([mix0, zero], 1), jnp.concatenate([zero, mix1], 1)], 0
    )
    scale = jnp.where(
        c == 0,
        jnp.concatenate([pool_scale, scale_other]),
        jnp.concatenate([scale_other, pool_scale]),
    ).astype(f32).reshape(1, 128)

    *messages, kv_all = latents(
        tokens,
        norm_gain,
        query_down_weight,
        query_latent_norm_gain,
        key_value_down_weight,
        key_value_latent_gain,
        w_rope_key,
        w_pool_in,
    )
    pieces = [messages[0]] + [shifted(messages[k], "y", k) for k in range(1, NY)]
    kv_own = lax.all_to_all(kv_all, "z", 0, 0, tiled=True).reshape(NZ * ROWS, KR + 128)
    kv = lax.all_to_all(
        jnp.broadcast_to(kv_own[None], (NY, *kv_own.shape)), "y", 0, 0, tiled=True
    )
    q_side, pool_own = in_order(pieces)
    q_own = [q_side] + [shifted(q_side, "x", k) for k in range(1, NX)]

    pool_other = across(pool_own)
    tail_rows = jnp.where(c == 1, pool_own[SIDE - 8 :], pool_other[SIDE - 8 :])
    head_rows = jnp.where(c == 0, pool_own[:8], pool_other[:8])
    count = NZ * NX
    low = lax.ppermute(tail_rows, ("z", "x"), [(i, i + 1) for i in range(count - 1)])
    high = lax.ppermute(head_rows, ("z", "x"), [(i + 1, i) for i in range(count - 1)])
    pooled = pooling(pool_own, pool_other, low, high, mixw, scale)

    q_pile = jnp.stack(q_own)
    q_twin = across(q_pile)
    qt = queries(q_own, q_twin, wqt, query_gain, query_tables())
    kv_twin = across(kv)
    pair = keys_values((pooled, wp, wb), kv, kv_twin, wkvt, key_gain, key_tables())
    partial = attend([pair], qt, None, True)

    merged = lax.all_to_all(partial, "x", 0, 0, tiled=True)
    keep, send, row_logsum = merge(merged)
    parts = project(keep, across(send), pooled, w_out_attn, wb, wp)
    parts = lax.all_to_all(parts, "y", 0, 0, tiled=True)
    mixed = jnp.sum(parts.astype(f32), axis=0).astype(bf16)
    return mixed, row_logsum


def solution(mesh):
    fine = Mesh(mesh.devices.reshape(NZ, NX, NY, 2), ("z", "x", "y", "c"))
    tp = ("y", "c")
    placed = (
        P(("z", "x", "y", "c"), None),
        P(),
        P(),
        P(),
        P(),
        P(),
        P(),
        P(),
        P(None, tp),
        P(None, tp),
        P(),
        P(),
        P(tp, None, None),
        P(tp),
        P(tp, None),
        P(tp, None),
    )

    return jax.shard_map(
        shards,
        mesh=fine,
        in_specs=placed,
        out_specs=(P(("z", "x", "y", "c"), None), P(tp, ("z", "x"))),
        check_vma=False,
    )
```

```python
import jax
import jax.numpy as jnp
import numpy as np
from jax import lax
from jax.experimental import pallas as pl
from jax.experimental.pallas import tpu as pltpu
from jax.sharding import Mesh, PartitionSpec as P

NOPE = 64
ROT = 32
HALF = 16
HEAD = 96
VAL = 64
HEADS = 3
QR = 512
KR = 256
EPS = 1e-06
WIDTH = 2048
ROWS = 48
BLOCK = 384
TOKENS = 12288
LOG2E = 1.4426950408889634
LN2 = 0.6931471805599453
MSG = 256
VROWS = 80
QTILE = 512
NX = 4
NY = 4
NZ = 8
NQ = NX * BLOCK

bf16 = jnp.bfloat16
f32 = jnp.float32


def trig_tables(inner_places, outer_step, outer_count):
    freqs = 10000.0 ** (-np.arange(HALF, dtype=np.float64) / HALF)
    inner = freqs[:, None] * inner_places[None, :]
    outer = freqs[:, None] * (outer_step * np.arange(outer_count, dtype=np.float64))[None, :]
    pad = np.zeros((HALF, 128 - outer_count))
    cast = lambda a: a.astype(np.float32)
    parts = [np.cos(inner), np.sin(inner), np.cos(outer), pad, np.sin(outer), pad]
    return cast(np.concatenate(parts, 1))


def query_tables():
    return trig_tables(np.arange(BLOCK, dtype=np.float64), BLOCK, NZ * NX)


def key_tables():
    z = np.arange(NZ, dtype=np.float64)
    places = (NX * BLOCK * z[:, None] + np.arange(ROWS, dtype=np.float64)[None, :]).reshape(-1)
    return trig_tables(places, ROWS, NX * NY * 2)


def near(x):
    return pltpu.with_memory_space_constraint(x, pltpu.VMEM)


def vmem():
    return pl.BlockSpec(memory_space=pltpu.VMEM)


def nt(a, b):
    return lax.dot_general(a, b, (((1,), (1,)), ((), ())), preferred_element_type=f32)


def nn(a, b):
    return lax.dot_general(a, b, (((1,), (0,)), ((), ())), preferred_element_type=f32)


def params(limit=56, **kw):
    return pltpu.CompilerParams(vmem_limit_bytes=limit * 1024 * 1024, **kw)


KSTEP = 1024


def latents_body(
    tok, gain, qdw, qg, kdw, kg, rw, pw, q_out, kv_out, pool_out, inv, aq, ak, ar, ap
):
    k = pl.program_id(0)

    @pl.when(k == 0)
    def _():
        x = tok[...].astype(f32)
        inv[...] = jnp.broadcast_to(
            lax.rsqrt(jnp.mean(x * x, axis=-1, keepdims=True) + EPS), (ROWS, 128)
        )
        aq[...] = jnp.zeros_like(aq)
        ak[...] = jnp.zeros_like(ak)
        ar[...] = jnp.zeros_like(ar)
        ap[...] = jnp.zeros_like(ap)

    cols = pl.ds(pl.multiple_of(k * KSTEP, KSTEP), KSTEP)
    x = tok[:, cols].astype(f32)
    normed = (x * inv[:, 0:1] * gain[cols].astype(f32).reshape(1, KSTEP)).astype(bf16)
    aq[...] += nn(normed, qdw[...])
    ak[...] += nn(normed, kdw[...])
    ar[...] += nt(normed, rw[...])
    ap[...] += nn(normed, pw[...])

    @pl.when(k == pl.num_programs(0) - 1)
    def _():
        def norm(v, g):
            return (
                v
                * lax.rsqrt(jnp.mean(v * v, axis=-1, keepdims=True) + EPS)
                * g.astype(f32).reshape(1, -1)
            ).astype(bf16)

        q = norm(aq[...], qg[...])
        kv = norm(ak[...], kg[...])
        rope = jnp.concatenate(
            [ar[...].astype(bf16), jnp.zeros((ROWS, 128 - ROT), bf16)], axis=1
        )
        q_out[...] = q
        pool_out[...] = ap[...].astype(bf16)
        for n in range(NZ):
            kv_out[n, :, 0:KR] = kv
            kv_out[n, :, KR:] = rope


def latents(tok, gain, qdw, qg, kdw, kg, rw, pw):
    steps = WIDTH // KSTEP
    whole = lambda *s: pl.BlockSpec(s, lambda k: (0,) * len(s))
    part = lambda n: pl.BlockSpec((KSTEP, n), lambda k: (k, 0))
    return pl.pallas_call(
        latents_body,
        grid=(steps,),
        in_specs=[
            whole(ROWS, WIDTH),
            whole(WIDTH),
            part(QR),
            whole(QR),
            part(KR),
            whole(KR),
            pl.BlockSpec((ROT, KSTEP), lambda k: (0, k)),
            part(512),
        ],
        out_specs=(
            whole(ROWS, QR),
            whole(NZ, ROWS, KR + 128),
            whole(ROWS, 512),
        ),
        out_shape=(
            jax.ShapeDtypeStruct((ROWS, QR), bf16),
            jax.ShapeDtypeStruct((NZ, ROWS, KR + 128), bf16),
            jax.ShapeDtypeStruct((ROWS, 512), bf16),
        ),
        scratch_shapes=[
            pltpu.VMEM((ROWS, 128), f32),
            pltpu.VMEM((ROWS, QR), f32),
            pltpu.VMEM((ROWS, KR), f32),
            pltpu.VMEM((ROWS, ROT), f32),
            pltpu.VMEM((ROWS, 512), f32),
        ],
        compiler_params=params(dimension_semantics=("arbitrary",)),
        name="latents",
    )(tok, gain, qdw, qg, kdw, kg, rw.T, pw)


def angles(table, idx):
    lanes = lax.broadcasted_iota(jnp.int32, (HALF, 128), 1)
    hit = lanes == idx
    coff = table[:, 0:BLOCK]
    soff = table[:, BLOCK : 2 * BLOCK]
    cb = table[:, 2 * BLOCK : 2 * BLOCK + 128]
    sb = table[:, 2 * BLOCK + 128 :]
    cbase = jnp.sum(jnp.where(hit, cb, 0.0), axis=1, keepdims=True)
    sbase = jnp.sum(jnp.where(hit, sb, 0.0), axis=1, keepdims=True)
    return cbase * coff - sbase * soff, sbase * coff + cbase * soff


def column(gain):
    row = jnp.broadcast_to(gain[...].astype(f32).reshape(1, HEAD), (8, HEAD)).astype(bf16)
    eye = (
        lax.broadcasted_iota(jnp.int32, (HEAD, HEAD), 0)
        == lax.broadcasted_iota(jnp.int32, (HEAD, HEAD), 1)
    ).astype(bf16)
    return nt(eye, row)[:, 0:1]


def rotated(v, cosine, sine):
    a = v[NOPE : NOPE + HALF]
    b = v[NOPE + HALF :]
    return jnp.concatenate(
        [v[:NOPE], a * cosine - b * sine, a * sine + b * cosine, jnp.zeros_like(v[:ROT])],
        axis=0,
    )


def queries_body(own0, own1, own2, own3, two0, two1, two2, two3, wqt, gain, table, out):
    c = lax.axis_index("c")
    z = lax.axis_index("z")
    here = lax.axis_index("x")
    qgain = column(gain)
    own = (own0, own1, own2, own3)
    other = (two0, two1, two2, two3)
    for x in range(NX):
        mine = own[x][...]
        twin = other[x][...]
        rows = []
        for y in range(NY):
            piece = slice(y * ROWS, (y + 1) * ROWS)
            rows.append(jnp.where(c == 0, mine[piece], twin[piece]))
            rows.append(jnp.where(c == 0, twin[piece], mine[piece]))
        q = nt(wqt[...], jnp.concatenate(rows, axis=0))
        block = (here + NX - x) % NX
        place = z * NX + block
        cosine, sine = angles(table, place)
        at = pl.multiple_of(block * BLOCK, BLOCK)
        for h in range(HEADS):
            v = q[h * HEAD : (h + 1) * HEAD]
            inv = lax.rsqrt(jnp.mean(v * v, axis=0, keepdims=True) + EPS)
            v = v * inv * qgain
            v = rotated(v, cosine, sine) * (LOG2E * HEAD**-0.5)
            out[h, :, pl.ds(at, BLOCK)] = v.astype(bf16)


def queries(own, other, wqt, qgain, table):
    return pl.pallas_call(
        queries_body,
        in_specs=[vmem()] * 11,
        out_specs=vmem(),
        out_shape=pltpu.VMEM((HEADS, 128, NQ), bf16),
        compiler_params=params(),
        name="queries",
    )(*own, *other, wqt, qgain, table)


def keys_body(count, *refs):
    own, other, wkvt, gain, table, kbuf, vbuf = refs[count:]
    c = lax.axis_index("c")
    x = lax.axis_index("x")
    kgain = column(gain)
    pick = (
        lax.broadcasted_iota(jnp.int32, (ROT, 128), 0)
        == lax.broadcasted_iota(jnp.int32, (ROT, 128), 1)
    ).astype(bf16)
    ones = (lax.broadcasted_iota(jnp.int32, (VROWS - VAL, BLOCK), 0) == 0).astype(bf16)
    blocks = [(own, k, k, c) for k in range(NY)] + [(other, k, k, 1 - c) for k in range(NY)]
    for b, (ref, at, y_from, c_from) in enumerate(blocks):
        lat = ref[at]
        kv = nt(wkvt[...], lat[:, :KR])
        rope = nt(pick, lat[:, KR:])
        rope_square = jnp.sum(rope * rope, axis=0, keepdims=True)
        place = (x * NY + y_from) * 2 + c_from
        cosine, sine = angles(table, place)
        cols = slice(b * BLOCK, (b + 1) * BLOCK)
        for h in range(HEADS):
            plain = kv[h * 128 : h * 128 + NOPE]
            total = jnp.sum(plain * plain, axis=0, keepdims=True) + rope_square
            inv = lax.rsqrt(total * (1.0 / HEAD) + EPS)
            k = jnp.concatenate([plain, rope], axis=0) * inv * kgain
            k = rotated(k, cosine, sine).astype(bf16)
            kbuf[h, cols, :] = k.T
            vbuf[h, 0:VAL, cols] = kv[h * 128 + NOPE : (h + 1) * 128].astype(bf16)
            vbuf[h, VAL:, cols] = ones


def keys_values(after, own, other, wkvt, kgain, table):
    count = 2 * NY * BLOCK

    def body(*refs):
        keys_body(len(after), *refs)

    return pl.pallas_call(
        body,
        in_specs=[pl.BlockSpec(memory_space=pl.ANY)] * len(after) + [vmem()] * 5,
        out_specs=(vmem(), vmem()),
        out_shape=(
            pltpu.VMEM((HEADS, count, 128), bf16),
            pltpu.VMEM((HEADS, VROWS, count), bf16),
        ),
        compiler_params=params(),
        name="keys",
    )(*after, own, other, wkvt, kgain, table)


CHUNK = 256
SUB = 128
TILES = HEADS * (NQ // QTILE)


def attend_body(kbuf, vbuf, qt, msg, l0, l1, l2, l3, buf0, buf1, acc_s, m_s, logs):
    bufs = (buf0, buf1)
    pairs = [(kbuf, vbuf)]
    sizes = [kbuf.shape[1]]
    chunks = []
    base = 0
    for (kr, vr), n in zip(pairs, sizes):
        for at in range(0, n, CHUNK):
            size = min(CHUNK, n - at)
            chunks.append((base + at, size, kr, vr, at))
        base += n

    def where(i):
        per = NQ // QTILE
        return i // per, pl.ds(pl.multiple_of((i % per) * QTILE, QTILE), QTILE)

    def score(i, chunk, buf, top):
        row, size, kr, _, at = chunk
        h, col = where(i)
        for sub in range(0, size, SUB):
            s = nn(kr[h, at + sub : at + sub + SUB, :], qt[h, :, col])
            buf[row + sub : row + sub + SUB, :] = s
            top = jnp.maximum(top, jnp.max(s.reshape(SUB // 8, 8, QTILE), axis=0))
        return top

    def weigh(i, chunk, buf, m):
        row, size, _, vr, at = chunk
        h, _ = where(i)
        p = jnp.exp2(buf[row : row + size, :] - m).astype(bf16)
        return nn(vr[h, :, at : at + size], p)

    low = jnp.full((8, QTILE), -1e30, f32)

    def settle(top):
        return jnp.max(top, axis=0, keepdims=True)

    def finish(i, m, acc):
        h, col = where(i)
        acc_s[h, :, col] = acc
        m_s[h, :, col] = m

    def both(i, m, buf, nxt):
        acc = None
        top = low
        for chunk in chunks:
            part = weigh(i, chunk, buf, m)
            acc = part if acc is None else acc + part
            top = score(i + 1, chunk, nxt, top)
        finish(i, m, acc)
        return settle(top)

    top = low
    for chunk in chunks:
        top = score(0, chunk, bufs[0], top)
    m = settle(top)

    def pair(j, m):
        m = both(2 * j, m, bufs[0], bufs[1])
        return both(2 * j + 1, m, bufs[1], bufs[0])

    m = lax.fori_loop(0, (TILES - 1) // 2, pair, m)
    acc = None
    for chunk in chunks:
        part = weigh(TILES - 1, chunk, bufs[0], m)
        acc = part if acc is None else acc + part
    finish(TILES - 1, m, acc)

    for x in range(NX):
        cols = slice(x * BLOCK, (x + 1) * BLOCK)
        parts = []
        stats = []
        for h in range(HEADS):
            total = acc_s[h, VAL : VAL + 1, cols]
            parts.append((acc_s[h, 0:VAL, cols] * (1.0 / total)).astype(bf16))
            lse = (m_s[h, :, cols] + jnp.log2(total)) * LN2
            logs[x, h : h + 1, :] = lse
            hi = lse.astype(bf16)
            rest = lse - hi.astype(f32)
            mid = rest.astype(bf16)
            low_part = (rest - mid.astype(f32)).astype(bf16)
            stats += [hi.astype(f32), mid.astype(f32), low_part.astype(f32)]
        stats.append(jnp.zeros((MSG - HEADS * VAL - 9, BLOCK), f32))
        parts.append(jnp.concatenate(stats, axis=0).astype(bf16))
        rows = jnp.concatenate(parts, axis=0).T
        for y in range(NY):
            msg[x * NY + y, :, :] = rows[y * 2 * ROWS : (y + 1) * 2 * ROWS]
    here = lax.axis_index("x")
    for k, ref in enumerate((l0, l1, l2, l3)):
        ref[...] = logs[(here + k) % NX]


def attend(kbuf, vbuf, qt):
    return pl.pallas_call(
        attend_body,
        in_specs=[vmem()] * 3,
        out_specs=(vmem(),) * 5,
        out_shape=(
            jax.ShapeDtypeStruct((NX * NY, 2 * ROWS, MSG), bf16),
            *[jax.ShapeDtypeStruct((8, BLOCK), f32)] * NX,
        ),
        scratch_shapes=[
            pltpu.VMEM((kbuf.shape[1], QTILE), f32),
            pltpu.VMEM((kbuf.shape[1], QTILE), f32),
            pltpu.VMEM((HEADS, VROWS, NQ), f32),
            pltpu.VMEM((HEADS, 1, NQ), f32),
            pltpu.VMEM((NX, 8, BLOCK), f32),
        ],
        compiler_params=params(40),
        name="attend",
    )(near(kbuf), near(vbuf), near(qt))


def logsum_body(a, b, c, d, out):
    logs = [r[0:HEADS, :] for r in (a, b, c, d)]
    top = jnp.maximum(jnp.maximum(logs[0], logs[1]), jnp.maximum(logs[2], logs[3]))
    total = sum(jnp.exp(v - top) for v in logs)
    out[...] = top + jnp.log(total)


def logsums(parts):
    return pl.pallas_call(
        logsum_body,
        in_specs=[vmem()] * NX,
        out_specs=vmem(),
        out_shape=jax.ShapeDtypeStruct((HEADS, BLOCK), f32),
        compiler_params=params(),
        name="logsums",
    )(*parts)


PLACES = (0, -1, 1, 2)


def pool_body(own, low, high, keep, send, buf):
    z, here, y0, c = [lax.axis_index(n) for n in "zxyc"]
    first = ((z * NX + here) * NY * 2 + y0 * 2 + c) * ROWS
    x = own[...].astype(f32)
    side = jnp.zeros((8, 512), f32)
    window = jnp.concatenate(
        [side, low[...].astype(f32), x, high[...].astype(f32), side], axis=0
    )
    n = ROWS + 32
    s1 = window[0 : n - 1] + window[1:n]
    s2 = s1[0 : n - 3] + s1[2 : n - 1]
    s4 = s2[0 : n - 7] + s2[4 : n - 3]
    s8 = s4[0 : n - 15] + s4[8 : n - 7]
    w1 = s1[15 : 15 + ROWS]
    w2 = s2[14 : 14 + ROWS]
    w4 = s4[12 : 12 + ROWS]
    w8 = s8[8 : 8 + ROWS]
    group = (lax.broadcasted_iota(jnp.int32, (ROWS, 512), 1) // 64) % 4
    total = jnp.where(
        group == 0, w1, jnp.where(group == 1, w2, jnp.where(group == 2, w4, w8))
    )
    half = jnp.where(group == 0, 1, jnp.where(group == 1, 2, jnp.where(group == 2, 4, 8)))
    place = first + lax.broadcasted_iota(jnp.int32, (ROWS, 512), 0)
    count = (jnp.minimum(place + half, TOKENS) - jnp.maximum(place - half, 0)).astype(f32)
    buf[...] = (total / count - x).astype(bf16)
    even, odd = [], []
    for d in PLACES:
        at = pl.multiple_of(((y0 + NY + d) % NY) * 128, 128)
        tile = buf[:, pl.ds(at, 128)]
        even.append(tile[:, 0:64])
        odd.append(tile[:, 64:128])
    even = jnp.concatenate(even, axis=1)
    odd = jnp.concatenate(odd, axis=1)
    keep[...] = jnp.where(c == 0, even, odd)
    send[...] = jnp.where(c == 0, odd, even)


def pooling(own, low, high):
    return pl.pallas_call(
        pool_body,
        in_specs=[vmem()] * 3,
        out_specs=(vmem(), vmem()),
        out_shape=(
            jax.ShapeDtypeStruct((ROWS, 256), bf16),
            jax.ShapeDtypeStruct((ROWS, 256), bf16),
        ),
        scratch_shapes=[pltpu.VMEM((ROWS, 512), bf16)],
        compiler_params=params(),
        name="pooling",
    )(own, low, high)


NSTEP = 512


def project_body(got, mine, theirs, *refs):
    wa, wp = refs[0:5], refs[5:10]
    keep, send, att, pool = refs[10:]
    y0 = lax.axis_index("y")
    c = lax.axis_index("c")

    @pl.when(pl.program_id(0) == 0)
    def _():
        row = lax.broadcasted_iota(jnp.int32, (128, HEADS * VAL), 0)
        head = lax.broadcasted_iota(jnp.int32, (128, HEADS * VAL), 1) // VAL
        spread = ((row >= 64 + 3 * head) & (row < 67 + 3 * head)).astype(bf16)
        for n, d in enumerate(PLACES):
            slots = [x * NY + (y0 + NY + d) % NY for x in range(NX)]
            logs = [nn(got[slot, :, 128:256], spread) for slot in slots]
            top = jnp.maximum(
                jnp.maximum(logs[0], logs[1]), jnp.maximum(logs[2], logs[3])
            )
            weights = [jnp.exp(v - top) for v in logs]
            total = weights[0] + weights[1] + weights[2] + weights[3]
            acc = jnp.zeros((2 * ROWS, HEADS * VAL), f32)
            for slot, w in zip(slots, weights):
                acc = acc + got[slot, :, 0 : HEADS * VAL].astype(f32) * w
            att[n, :, :] = (acc / total).astype(bf16)
        pool[0:ROWS, :] = jnp.where(c == 0, mine[...], theirs[...])
        pool[ROWS:, :] = jnp.where(c == 0, theirs[...], mine[...])

    total = nn(pool[...], jnp.concatenate([w[...] for w in wp], axis=0))
    for n in range(3):
        total = total + nn(att[n], wa[n][...])
    total = total + nn(att[3], jnp.concatenate([wa[3][...], wa[4][...]], axis=0))
    first, second = total[0:ROWS], total[ROWS:]
    keep[...] = jnp.where(c == 0, first, second)
    send[...] = jnp.where(c == 0, second, first).astype(bf16)


def project(got, mine, theirs, wa, wp):
    whole = lambda *s: pl.BlockSpec(s, lambda k: (0,) * len(s))
    part = lambda n: pl.BlockSpec((n, NSTEP), lambda k: (0, k))
    weights = [*wa, *wp]
    return pl.pallas_call(
        project_body,
        grid=(WIDTH // NSTEP,),
        in_specs=[whole(*got.shape), whole(*mine.shape), whole(*theirs.shape)]
        + [part(w.shape[0]) for w in weights],
        out_specs=(part(ROWS), part(ROWS)),
        out_shape=(
            jax.ShapeDtypeStruct((ROWS, WIDTH), f32),
            jax.ShapeDtypeStruct((ROWS, WIDTH), bf16),
        ),
        scratch_shapes=[
            pltpu.VMEM((NY, 2 * ROWS, HEADS * VAL), bf16),
            pltpu.VMEM((2 * ROWS, 256), bf16),
        ],
        compiler_params=params(dimension_semantics=("arbitrary",)),
        name="project",
    )(got, mine, theirs, *weights)


def across(x):
    return lax.ppermute(x, "c", [(0, 1), (1, 0)])


def shifted(x, axis, places):
    count = lax.axis_size(axis)
    return lax.ppermute(x, axis, [(i, (i + places) % count) for i in range(count)])


def order_body(a, b, c, d, q_out):
    y = lax.axis_index("y")
    for k, ref in enumerate((a, b, c, d)):
        at = pl.multiple_of(((y + NY - k) % NY) * ROWS, ROWS)
        q_out[pl.ds(at, ROWS), :] = ref[...]


def in_order(pieces):
    return pl.pallas_call(
        order_body,
        in_specs=[vmem()] * NY,
        out_specs=vmem(),
        out_shape=jax.ShapeDtypeStruct((NY * ROWS, QR), bf16),
        compiler_params=params(),
        name="order",
    )(*pieces)


def shards(
    tokens,
    norm_gain,
    query_down_weight,
    query_latent_norm_gain,
    key_value_down_weight,
    key_value_latent_gain,
    w_rope_key,
    w_pool_in,
    query_up_weight,
    key_value_up_weight,
    query_gain,
    key_gain,
    w_pool_mix,
    pool_scale,
    w_out_attn,
    w_out_pool,
):
    wqt = query_up_weight.T
    wkvt = key_value_up_weight.T

    q_all, kv_all, pool_in = latents(
        tokens,
        norm_gain,
        query_down_weight,
        query_latent_norm_gain,
        key_value_down_weight,
        key_value_latent_gain,
        w_rope_key,
        w_pool_in,
    )
    pieces = [q_all] + [shifted(q_all, "y", k) for k in range(1, NY)]
    kv_own = lax.all_to_all(kv_all, "z", 0, 0, tiled=True).reshape(NZ * ROWS, KR + 128)

    count = NZ * NX * NY * 2
    every = ("z", "x", "y", "c")
    low = lax.ppermute(
        pool_in[ROWS - 8 :], every, [(i, i + 1) for i in range(count - 1)]
    )
    high = lax.ppermute(pool_in[:8], every, [(i + 1, i) for i in range(count - 1)])
    pool_mine, pool_send = pooling(pool_in, low, high)
    pool_theirs = across(pool_send)

    folded = jnp.dot(
        w_pool_mix[0],
        (pool_scale.astype(f32)[:, None] * w_out_pool.astype(f32)).astype(bf16),
        preferred_element_type=f32,
    ).astype(bf16)
    wa1 = shifted(w_out_attn, "y", 1)
    wa3 = shifted(w_out_attn, "y", NY - 1)
    wp1 = shifted(folded, "y", 1)
    wp3 = shifted(folded, "y", NY - 1)
    half = HEADS * VAL // 2
    wa2a = shifted(wa1[:half], "y", 1)
    wa2b = shifted(wa3[half:], "y", NY - 1)
    wp2a = shifted(wp1[:32], "y", 1)
    wp2b = shifted(wp3[32:], "y", NY - 1)

    kv = lax.all_to_all(
        jnp.broadcast_to(kv_own[None], (NY, *kv_own.shape)), "y", 0, 0, tiled=True
    )
    q_side = in_order(pieces)
    q_own = [q_side] + [shifted(q_side, "x", k) for k in range(1, NX)]
    tag = q_own[1][:8, :128] + q_own[2][:8, :128] + q_own[3][:8, :128]
    q_twin = [across(q) for q in q_own]
    kv_twin = across(kv)
    qt = queries(q_own, q_twin, wqt, query_gain, query_tables())
    pair = keys_values((tag,), kv, kv_twin, wkvt, key_gain, key_tables())
    message, *logs = attend(*pair, qt)

    got = lax.all_to_all(message, ("x", "y"), 0, 0, tiled=True)
    logs = [logs[0]] + [shifted(logs[k], "x", k) for k in range(1, NX)]
    row_logsum = logsums(logs)
    keep, send = project(
        got,
        pool_mine,
        pool_theirs,
        (w_out_attn, wa1, wa3, wa2a, wa2b),
        (folded, wp1, wp3, wp2a, wp2b),
    )
    mixed = (keep + across(send).astype(f32)).astype(bf16)
    return mixed, row_logsum


def solution(mesh):
    fine = Mesh(mesh.devices.reshape(NZ, NX, NY, 2), ("z", "x", "y", "c"))
    tp = ("y", "c")
    placed = (
        P(("z", "x", "y", "c"), None),
        P(),
        P(),
        P(),
        P(),
        P(),
        P(),
        P(),
        P(None, tp),
        P(None, tp),
        P(),
        P(),
        P(tp, None, None),
        P(tp),
        P(tp, None),
        P(tp, None),
    )

    return jax.shard_map(
        shards,
        mesh=fine,
        in_specs=placed,
        out_specs=(P(("z", "x", "y", "c"), None), P(tp, ("z", "x"))),
        check_vma=False,
    )
```

```python
import jax
import jax.numpy as jnp
import numpy as np
from jax import lax
from jax.experimental import pallas as pl
from jax.experimental.pallas import tpu as pltpu
from jax.sharding import Mesh, PartitionSpec as P

NOPE = 64
ROT = 32
HALF = 16
HEAD = 96
VAL = 64
HEADS = 3
QR = 512
KR = 256
EPS = 1e-06
WIDTH = 2048
ROWS = 48
BLOCK = 384
TOKENS = 12288
LOG2E = 1.4426950408889634
LN2 = 0.6931471805599453
MSG = 256
VROWS = 80
QTILE = 512
NX = 4
NY = 4
NZ = 8
NQ = NX * BLOCK

bf16 = jnp.bfloat16
f32 = jnp.float32


def trig_tables(inner_places, outer_step, outer_count):
    freqs = 10000.0 ** (-np.arange(HALF, dtype=np.float64) / HALF)
    inner = freqs[:, None] * inner_places[None, :]
    outer = freqs[:, None] * (outer_step * np.arange(outer_count, dtype=np.float64))[None, :]
    pad = np.zeros((HALF, 128 - outer_count))
    cast = lambda a: a.astype(np.float32)
    parts = [np.cos(inner), np.sin(inner), np.cos(outer), pad, np.sin(outer), pad]
    return cast(np.concatenate(parts, 1))


def query_tables():
    return trig_tables(np.arange(BLOCK, dtype=np.float64), BLOCK, NZ * NX)


def key_tables():
    z = np.arange(NZ, dtype=np.float64)
    places = (NX * BLOCK * z[:, None] + np.arange(ROWS, dtype=np.float64)[None, :]).reshape(-1)
    return trig_tables(places, ROWS, NX * NY * 2)


def near(x):
    return pltpu.with_memory_space_constraint(x, pltpu.VMEM)


def vmem():
    return pl.BlockSpec(memory_space=pltpu.VMEM)


def nt(a, b):
    return lax.dot_general(a, b, (((1,), (1,)), ((), ())), preferred_element_type=f32)


def nn(a, b):
    return lax.dot_general(a, b, (((1,), (0,)), ((), ())), preferred_element_type=f32)


def params(limit=56, **kw):
    return pltpu.CompilerParams(vmem_limit_bytes=limit * 1024 * 1024, **kw)


KSTEP = 1024


def latents_body(
    tok, gain, qdw, qg, kdw, kg, rw, pw, q_out, kv_out, pool_out, inv, aq, ak, ar, ap
):
    k = pl.program_id(0)

    @pl.when(k == 0)
    def _():
        x = tok[...].astype(f32)
        inv[...] = jnp.broadcast_to(
            lax.rsqrt(jnp.mean(x * x, axis=-1, keepdims=True) + EPS), (ROWS, 128)
        )
        aq[...] = jnp.zeros_like(aq)
        ak[...] = jnp.zeros_like(ak)
        ar[...] = jnp.zeros_like(ar)
        ap[...] = jnp.zeros_like(ap)

    cols = pl.ds(pl.multiple_of(k * KSTEP, KSTEP), KSTEP)
    x = tok[:, cols].astype(f32)
    normed = (x * inv[:, 0:1] * gain[cols].astype(f32).reshape(1, KSTEP)).astype(bf16)
    aq[...] += nn(normed, qdw[...])
    ak[...] += nn(normed, kdw[...])
    ar[...] += nt(normed, rw[...])
    ap[...] += nn(normed, pw[...])

    @pl.when(k == pl.num_programs(0) - 1)
    def _():
        def norm(v, g):
            return (
                v
                * lax.rsqrt(jnp.mean(v * v, axis=-1, keepdims=True) + EPS)
                * g.astype(f32).reshape(1, -1)
            ).astype(bf16)

        q = norm(aq[...], qg[...])
        kv = norm(ak[...], kg[...])
        rope = jnp.concatenate(
            [ar[...].astype(bf16), jnp.zeros((ROWS, 128 - ROT), bf16)], axis=1
        )
        q_out[...] = q
        pool_out[...] = ap[...].astype(bf16)
        for n in range(NZ):
            kv_out[n, :, 0:KR] = kv
            kv_out[n, :, KR:] = rope


def latents(tok, gain, qdw, qg, kdw, kg, rw, pw):
    steps = WIDTH // KSTEP
    whole = lambda *s: pl.BlockSpec(s, lambda k: (0,) * len(s))
    part = lambda n: pl.BlockSpec((KSTEP, n), lambda k: (k, 0))
    return pl.pallas_call(
        latents_body,
        grid=(steps,),
        in_specs=[
            whole(ROWS, WIDTH),
            whole(WIDTH),
            part(QR),
            whole(QR),
            part(KR),
            whole(KR),
            pl.BlockSpec((ROT, KSTEP), lambda k: (0, k)),
            part(512),
        ],
        out_specs=(
            whole(ROWS, QR),
            whole(NZ, ROWS, KR + 128),
            whole(ROWS, 512),
        ),
        out_shape=(
            jax.ShapeDtypeStruct((ROWS, QR), bf16),
            jax.ShapeDtypeStruct((NZ, ROWS, KR + 128), bf16),
            jax.ShapeDtypeStruct((ROWS, 512), bf16),
        ),
        scratch_shapes=[
            pltpu.VMEM((ROWS, 128), f32),
            pltpu.VMEM((ROWS, QR), f32),
            pltpu.VMEM((ROWS, KR), f32),
            pltpu.VMEM((ROWS, ROT), f32),
            pltpu.VMEM((ROWS, 512), f32),
        ],
        compiler_params=params(dimension_semantics=("arbitrary",)),
        name="latents",
    )(tok, gain, qdw, qg, kdw, kg, rw.T, pw)


def angles(table, idx):
    lanes = lax.broadcasted_iota(jnp.int32, (HALF, 128), 1)
    hit = lanes == idx
    coff = table[:, 0:BLOCK]
    soff = table[:, BLOCK : 2 * BLOCK]
    cb = table[:, 2 * BLOCK : 2 * BLOCK + 128]
    sb = table[:, 2 * BLOCK + 128 :]
    cbase = jnp.sum(jnp.where(hit, cb, 0.0), axis=1, keepdims=True)
    sbase = jnp.sum(jnp.where(hit, sb, 0.0), axis=1, keepdims=True)
    return cbase * coff - sbase * soff, sbase * coff + cbase * soff


def column(gain):
    row = jnp.broadcast_to(gain[...].astype(f32).reshape(1, HEAD), (8, HEAD)).astype(bf16)
    eye = (
        lax.broadcasted_iota(jnp.int32, (HEAD, HEAD), 0)
        == lax.broadcasted_iota(jnp.int32, (HEAD, HEAD), 1)
    ).astype(bf16)
    return nt(eye, row)[:, 0:1]


def rotated(v, cosine, sine):
    a = v[NOPE : NOPE + HALF]
    b = v[NOPE + HALF :]
    return jnp.concatenate(
        [v[:NOPE], a * cosine - b * sine, a * sine + b * cosine, jnp.zeros_like(v[:ROT])],
        axis=0,
    )


def queries_body(own0, own1, own2, own3, two0, two1, two2, two3, wqt, gain, table, out):
    c = lax.axis_index("c")
    z = lax.axis_index("z")
    here = lax.axis_index("x")
    qgain = column(gain)
    own = (own0, own1, own2, own3)
    other = (two0, two1, two2, two3)
    for x in range(NX):
        mine = own[x][...]
        twin = other[x][...]
        rows = []
        for y in range(NY):
            piece = slice(y * ROWS, (y + 1) * ROWS)
            rows.append(jnp.where(c == 0, mine[piece], twin[piece]))
            rows.append(jnp.where(c == 0, twin[piece], mine[piece]))
        q = nt(wqt[...], jnp.concatenate(rows, axis=0))
        block = (here + NX - x) % NX
        place = z * NX + block
        cosine, sine = angles(table, place)
        at = pl.multiple_of(block * BLOCK, BLOCK)
        for h in range(HEADS):
            v = q[h * HEAD : (h + 1) * HEAD]
            inv = lax.rsqrt(jnp.mean(v * v, axis=0, keepdims=True) + EPS)
            v = v * inv * qgain
            v = rotated(v, cosine, sine) * (LOG2E * HEAD**-0.5)
            out[h, :, pl.ds(at, BLOCK)] = v.astype(bf16)


def queries(own, other, wqt, qgain, table):
    return pl.pallas_call(
        queries_body,
        in_specs=[vmem()] * 11,
        out_specs=vmem(),
        out_shape=pltpu.VMEM((HEADS, 128, NQ), bf16),
        compiler_params=params(),
        name="queries",
    )(*own, *other, wqt, qgain, table)


def keys_body(count, *refs):
    own, other, wkvt, gain, table, kbuf, vbuf = refs[count:]
    c = lax.axis_index("c")
    x = lax.axis_index("x")
    kgain = column(gain)
    pick = (
        lax.broadcasted_iota(jnp.int32, (ROT, 128), 0)
        == lax.broadcasted_iota(jnp.int32, (ROT, 128), 1)
    ).astype(bf16)
    ones = (lax.broadcasted_iota(jnp.int32, (VROWS - VAL, BLOCK), 0) == 0).astype(bf16)
    blocks = [(own, k, k, c) for k in range(NY)] + [(other, k, k, 1 - c) for k in range(NY)]
    for b, (ref, at, y_from, c_from) in enumerate(blocks):
        lat = ref[at]
        kv = nt(wkvt[...], lat[:, :KR])
        rope = nt(pick, lat[:, KR:])
        rope_square = jnp.sum(rope * rope, axis=0, keepdims=True)
        place = (x * NY + y_from) * 2 + c_from
        cosine, sine = angles(table, place)
        cols = slice(b * BLOCK, (b + 1) * BLOCK)
        for h in range(HEADS):
            plain = kv[h * 128 : h * 128 + NOPE]
            total = jnp.sum(plain * plain, axis=0, keepdims=True) + rope_square
            inv = lax.rsqrt(total * (1.0 / HEAD) + EPS)
            k = jnp.concatenate([plain, rope], axis=0) * inv * kgain
            k = rotated(k, cosine, sine).astype(bf16)
            kbuf[h, cols, :] = k.T
            vbuf[h, 0:VAL, cols] = kv[h * 128 + NOPE : (h + 1) * 128].astype(bf16)
            vbuf[h, VAL:, cols] = ones


def keys_values(after, own, other, wkvt, kgain, table):
    count = 2 * NY * BLOCK

    def body(*refs):
        keys_body(len(after), *refs)

    return pl.pallas_call(
        body,
        in_specs=[pl.BlockSpec(memory_space=pl.ANY)] * len(after) + [vmem()] * 5,
        out_specs=(vmem(), vmem()),
        out_shape=(
            pltpu.VMEM((HEADS, count, 128), bf16),
            pltpu.VMEM((HEADS, VROWS, count), bf16),
        ),
        compiler_params=params(),
        name="keys",
    )(*after, own, other, wkvt, kgain, table)


CHUNK = 256
SUB = 128
TILES = HEADS * (NQ // QTILE)


def attend_body(kbuf, vbuf, qt, msg, l0, l1, l2, l3, buf0, buf1, acc_s, m_s, logs):
    bufs = (buf0, buf1)
    pairs = [(kbuf, vbuf)]
    sizes = [kbuf.shape[1]]
    chunks = []
    base = 0
    for (kr, vr), n in zip(pairs, sizes):
        for at in range(0, n, CHUNK):
            size = min(CHUNK, n - at)
            chunks.append((base + at, size, kr, vr, at))
        base += n

    def where(i):
        per = NQ // QTILE
        return i // per, pl.ds(pl.multiple_of((i % per) * QTILE, QTILE), QTILE)

    def score(i, chunk, buf, top):
        row, size, kr, _, at = chunk
        h, col = where(i)
        for sub in range(0, size, SUB):
            s = nn(kr[h, at + sub : at + sub + SUB, :], qt[h, :, col])
            buf[row + sub : row + sub + SUB, :] = s
            top = jnp.maximum(top, jnp.max(s.reshape(SUB // 8, 8, QTILE), axis=0))
        return top

    def weigh(i, chunk, buf, m):
        row, size, _, vr, at = chunk
        h, _ = where(i)
        p = jnp.exp2(buf[row : row + size, :] - m).astype(bf16)
        return nn(vr[h, :, at : at + size], p)

    low = jnp.full((8, QTILE), -1e30, f32)

    def settle(top):
        return jnp.max(top, axis=0, keepdims=True)

    def finish(i, m, acc):
        h, col = where(i)
        acc_s[h, :, col] = acc
        m_s[h, :, col] = m

    def both(i, m, buf, nxt):
        acc = None
        top = low
        for chunk in chunks:
            part = weigh(i, chunk, buf, m)
            acc = part if acc is None else acc + part
            top = score(i + 1, chunk, nxt, top)
        finish(i, m, acc)
        return settle(top)

    top = low
    for chunk in chunks:
        top = score(0, chunk, bufs[0], top)
    m = settle(top)

    def pair(j, m):
        m = both(2 * j, m, bufs[0], bufs[1])
        return both(2 * j + 1, m, bufs[1], bufs[0])

    m = lax.fori_loop(0, (TILES - 1) // 2, pair, m)
    acc = None
    for chunk in chunks:
        part = weigh(TILES - 1, chunk, bufs[0], m)
        acc = part if acc is None else acc + part
    finish(TILES - 1, m, acc)

    for x in range(NX):
        cols = slice(x * BLOCK, (x + 1) * BLOCK)
        parts = []
        stats = []
        for h in range(HEADS):
            total = acc_s[h, VAL : VAL + 1, cols]
            parts.append((acc_s[h, 0:VAL, cols] * (1.0 / total)).astype(bf16))
            lse = (m_s[h, :, cols] + jnp.log2(total)) * LN2
            logs[x, h : h + 1, :] = lse
            hi = lse.astype(bf16)
            rest = lse - hi.astype(f32)
            mid = rest.astype(bf16)
            low_part = (rest - mid.astype(f32)).astype(bf16)
            stats += [hi.astype(f32), mid.astype(f32), low_part.astype(f32)]
        stats.append(jnp.zeros((MSG - HEADS * VAL - 9, BLOCK), f32))
        parts.append(jnp.concatenate(stats, axis=0).astype(bf16))
        rows = jnp.concatenate(parts, axis=0).T
        for y in range(NY):
            msg[x * NY + y, :, :] = rows[y * 2 * ROWS : (y + 1) * 2 * ROWS]
    here = lax.axis_index("x")
    for k, ref in enumerate((l0, l1, l2, l3)):
        ref[...] = logs[(here + k) % NX]


def attend(kbuf, vbuf, qt):
    return pl.pallas_call(
        attend_body,
        in_specs=[vmem()] * 3,
        out_specs=(vmem(),) * 5,
        out_shape=(
            jax.ShapeDtypeStruct((NX * NY, 2 * ROWS, MSG), bf16),
            *[jax.ShapeDtypeStruct((8, BLOCK), f32)] * NX,
        ),
        scratch_shapes=[
            pltpu.VMEM((kbuf.shape[1], QTILE), f32),
            pltpu.VMEM((kbuf.shape[1], QTILE), f32),
            pltpu.VMEM((HEADS, VROWS, NQ), f32),
            pltpu.VMEM((HEADS, 1, NQ), f32),
            pltpu.VMEM((NX, 8, BLOCK), f32),
        ],
        compiler_params=params(40),
        name="attend",
    )(near(kbuf), near(vbuf), near(qt))


def logsum_body(a, b, c, d, out):
    logs = [r[0:HEADS, :] for r in (a, b, c, d)]
    top = jnp.maximum(jnp.maximum(logs[0], logs[1]), jnp.maximum(logs[2], logs[3]))
    total = sum(jnp.exp(v - top) for v in logs)
    out[...] = top + jnp.log(total)


def logsums(parts):
    return pl.pallas_call(
        logsum_body,
        in_specs=[vmem()] * NX,
        out_specs=vmem(),
        out_shape=jax.ShapeDtypeStruct((HEADS, BLOCK), f32),
        compiler_params=params(),
        name="logsums",
    )(*parts)


PLACES = (0, -1, 1, 2)


def pool_body(own, low, high, keep, send, buf):
    z, here, y0, c = [lax.axis_index(n) for n in "zxyc"]
    first = ((z * NX + here) * NY * 2 + y0 * 2 + c) * ROWS
    x = own[...].astype(f32)
    side = jnp.zeros((8, 512), f32)
    window = jnp.concatenate(
        [side, low[...].astype(f32), x, high[...].astype(f32), side], axis=0
    )
    n = ROWS + 32
    s1 = window[0 : n - 1] + window[1:n]
    s2 = s1[0 : n - 3] + s1[2 : n - 1]
    s4 = s2[0 : n - 7] + s2[4 : n - 3]
    s8 = s4[0 : n - 15] + s4[8 : n - 7]
    w1 = s1[15 : 15 + ROWS]
    w2 = s2[14 : 14 + ROWS]
    w4 = s4[12 : 12 + ROWS]
    w8 = s8[8 : 8 + ROWS]
    group = (lax.broadcasted_iota(jnp.int32, (ROWS, 512), 1) // 64) % 4
    total = jnp.where(
        group == 0, w1, jnp.where(group == 1, w2, jnp.where(group == 2, w4, w8))
    )
    half = jnp.where(group == 0, 1, jnp.where(group == 1, 2, jnp.where(group == 2, 4, 8)))
    place = first + lax.broadcasted_iota(jnp.int32, (ROWS, 512), 0)
    count = (jnp.minimum(place + half, TOKENS) - jnp.maximum(place - half, 0)).astype(f32)
    buf[...] = (total / count - x).astype(bf16)
    even, odd = [], []
    for d in PLACES:
        at = pl.multiple_of(((y0 + NY + d) % NY) * 128, 128)
        tile = buf[:, pl.ds(at, 128)]
        even.append(tile[:, 0:64])
        odd.append(tile[:, 64:128])
    even = jnp.concatenate(even, axis=1)
    odd = jnp.concatenate(odd, axis=1)
    keep[...] = jnp.where(c == 0, even, odd)
    send[...] = jnp.where(c == 0, odd, even)


def pooling(own, low, high):
    return pl.pallas_call(
        pool_body,
        in_specs=[vmem()] * 3,
        out_specs=(vmem(), vmem()),
        out_shape=(
            jax.ShapeDtypeStruct((ROWS, 256), bf16),
            jax.ShapeDtypeStruct((ROWS, 256), bf16),
        ),
        scratch_shapes=[pltpu.VMEM((ROWS, 512), bf16)],
        compiler_params=params(),
        name="pooling",
    )(own, low, high)


def project_body(got, mine, theirs, w0, w1, w3, w2a, w2b, keep, send, wbuf, sems):
    y0 = lax.axis_index("y")
    c = lax.axis_index("c")
    places = ((w0, 0, 0), (w1, 1, 0), (w3, 2, 0), (w2a, 3, 0), (w2b, 3, 128))
    copies = []
    for n, (ref, slot, at) in enumerate(places):
        rows = ref.shape[0]
        copies.append(
            pltpu.make_async_copy(ref, wbuf.at[slot, at : at + rows], sems.at[n])
        )
    for copy in copies:
        copy.start()
    row = lax.broadcasted_iota(jnp.int32, (128, HEADS * VAL), 0)
    head = lax.broadcasted_iota(jnp.int32, (128, HEADS * VAL), 1) // VAL
    spread = ((row >= 64 + 3 * head) & (row < 67 + 3 * head)).astype(bf16)
    inputs = []
    for n, d in enumerate(PLACES):
        slots = [x * NY + (y0 + NY + d) % NY for x in range(NX)]
        logs = [nn(got[slot, :, 128:256], spread) for slot in slots]
        top = jnp.maximum(jnp.maximum(logs[0], logs[1]), jnp.maximum(logs[2], logs[3]))
        weights = [jnp.exp(v - top) for v in logs]
        total = weights[0] + weights[1] + weights[2] + weights[3]
        acc = jnp.zeros((2 * ROWS, HEADS * VAL), f32)
        for slot, w in zip(slots, weights):
            acc = acc + got[slot, :, 0 : HEADS * VAL].astype(f32) * w
        own = mine[:, n * 64 : (n + 1) * 64]
        twin = theirs[:, n * 64 : (n + 1) * 64]
        pool = jnp.concatenate(
            [jnp.where(c == 0, own, twin), jnp.where(c == 0, twin, own)], axis=0
        )
        inputs.append(jnp.concatenate([(acc / total).astype(bf16), pool], axis=1))
    for copy in copies:
        copy.wait()
    for col in range(0, WIDTH, 512):
        cols = slice(col, col + 512)
        result = nn(inputs[0], wbuf[0, :, cols])
        for n in range(1, NY):
            result = result + nn(inputs[n], wbuf[n, :, cols])
        first, second = result[0:ROWS], result[ROWS:]
        keep[:, cols] = jnp.where(c == 0, first, second)
        send[:, cols] = jnp.where(c == 0, second, first).astype(bf16)


def project(got, mine, theirs, weights):
    return pl.pallas_call(
        project_body,
        in_specs=[vmem()] * 3 + [pl.BlockSpec(memory_space=pl.ANY)] * 5,
        out_specs=(vmem(), vmem()),
        out_shape=(
            pltpu.VMEM((ROWS, WIDTH), f32),
            pltpu.VMEM((ROWS, WIDTH), bf16),
        ),
        scratch_shapes=[
            pltpu.VMEM((NY, 256, WIDTH), bf16),
            pltpu.SemaphoreType.DMA((5,)),
        ],
        compiler_params=params(40),
        name="project",
    )(near(got), near(mine), near(theirs), *weights)


def across(x):
    return lax.ppermute(x, "c", [(0, 1), (1, 0)])


def shifted(x, axis, places):
    count = lax.axis_size(axis)
    return lax.ppermute(x, axis, [(i, (i + places) % count) for i in range(count)])


def order_body(a, b, c, d, q_out):
    y = lax.axis_index("y")
    for k, ref in enumerate((a, b, c, d)):
        at = pl.multiple_of(((y + NY - k) % NY) * ROWS, ROWS)
        q_out[pl.ds(at, ROWS), :] = ref[...]


def in_order(pieces):
    return pl.pallas_call(
        order_body,
        in_specs=[vmem()] * NY,
        out_specs=vmem(),
        out_shape=jax.ShapeDtypeStruct((NY * ROWS, QR), bf16),
        compiler_params=params(),
        name="order",
    )(*pieces)


def shards(
    tokens,
    norm_gain,
    query_down_weight,
    query_latent_norm_gain,
    key_value_down_weight,
    key_value_latent_gain,
    w_rope_key,
    w_pool_in,
    query_up_weight,
    key_value_up_weight,
    query_gain,
    key_gain,
    w_pool_mix,
    pool_scale,
    w_out_attn,
    w_out_pool,
):
    wqt = query_up_weight.T
    wkvt = key_value_up_weight.T

    q_all, kv_all, pool_in = latents(
        tokens,
        norm_gain,
        query_down_weight,
        query_latent_norm_gain,
        key_value_down_weight,
        key_value_latent_gain,
        w_rope_key,
        w_pool_in,
    )
    pieces = [q_all] + [shifted(q_all, "y", k) for k in range(1, NY)]
    kv_own = lax.all_to_all(kv_all, "z", 0, 0, tiled=True).reshape(NZ * ROWS, KR + 128)

    count = NZ * NX * NY * 2
    every = ("z", "x", "y", "c")
    low = lax.ppermute(
        pool_in[ROWS - 8 :], every, [(i, i + 1) for i in range(count - 1)]
    )
    high = lax.ppermute(pool_in[:8], every, [(i + 1, i) for i in range(count - 1)])
    pool_mine, pool_send = pooling(pool_in, low, high)
    pool_theirs = across(pool_send)

    folded = jnp.dot(
        w_pool_mix[0],
        (pool_scale.astype(f32)[:, None] * w_out_pool.astype(f32)).astype(bf16),
        preferred_element_type=f32,
    ).astype(bf16)
    w0 = jnp.concatenate([w_out_attn, folded], axis=0)
    w1 = shifted(w0, "y", 1)
    w3 = shifted(w0, "y", NY - 1)
    w1_half, w3_half = lax.optimization_barrier((w1[:128], w3[128:]))
    w2a = shifted(w1_half, "y", 1)
    w2b = shifted(w3_half, "y", NY - 1)

    kv = lax.all_to_all(
        jnp.broadcast_to(kv_own[None], (NY, *kv_own.shape)), "y", 0, 0, tiled=True
    )
    q_side = in_order(pieces)
    q_own = [q_side] + [shifted(q_side, "x", k) for k in range(1, NX)]
    q_twin = [across(q) for q in q_own]
    kv_twin = across(kv)
    qt = queries(q_own, q_twin, wqt, query_gain, query_tables())
    pair = keys_values((), kv, kv_twin, wkvt, key_gain, key_tables())
    message, *logs = attend(*pair, qt)

    got = lax.all_to_all(message, ("x", "y"), 0, 0, tiled=True)
    logs = [logs[0]] + [shifted(logs[k], "x", k) for k in range(1, NX)]
    row_logsum = logsums(logs)
    keep, send = project(got, pool_mine, pool_theirs, (w0, w1, w3, w2a, w2b))
    received = across(send)
    mixed = (keep + received.astype(f32)).astype(bf16)
    return mixed, row_logsum


def solution(mesh):
    fine = Mesh(mesh.devices.reshape(NZ, NX, NY, 2), ("z", "x", "y", "c"))
    tp = ("y", "c")
    placed = (
        P(("z", "x", "y", "c"), None),
        P(),
        P(),
        P(),
        P(),
        P(),
        P(),
        P(),
        P(None, tp),
        P(None, tp),
        P(),
        P(),
        P(tp, None, None),
        P(tp),
        P(tp, None),
        P(tp, None),
    )

    return jax.shard_map(
        shards,
        mesh=fine,
        in_specs=placed,
        out_specs=(P(("z", "x", "y", "c"), None), P(tp, ("z", "x"))),
        check_vma=False,
    )
```

```python
import jax
import jax.numpy as jnp
import numpy as np
from jax import lax
from jax.experimental import pallas as pl
from jax.experimental.pallas import tpu as pltpu
from jax.sharding import Mesh, PartitionSpec as P

NOPE = 64
ROT = 32
HALF = 16
HEAD = 96
VAL = 64
HEADS = 3
QR = 512
KR = 256
EPS = 1e-06
WIDTH = 2048
ROWS = 48
BLOCK = 384
TOKENS = 12288
LOG2E = 1.4426950408889634
LN2 = 0.6931471805599453
MSG = 256
VROWS = 80
QTILE = 512
NX = 4
NY = 4
NZ = 8
NQ = NX * BLOCK

bf16 = jnp.bfloat16
f32 = jnp.float32


def trig_tables(inner_places, outer_step, outer_count):
    freqs = 10000.0 ** (-np.arange(HALF, dtype=np.float64) / HALF)
    inner = freqs[:, None] * inner_places[None, :]
    outer = freqs[:, None] * (outer_step * np.arange(outer_count, dtype=np.float64))[None, :]
    pad = np.zeros((HALF, 128 - outer_count))
    cast = lambda a: a.astype(np.float32)
    parts = [np.cos(inner), np.sin(inner), np.cos(outer), pad, np.sin(outer), pad]
    return cast(np.concatenate(parts, 1))


def query_tables():
    return trig_tables(np.arange(BLOCK, dtype=np.float64), BLOCK, NZ * NX)


def key_tables():
    z = np.arange(NZ, dtype=np.float64)
    places = (NX * BLOCK * z[:, None] + np.arange(ROWS, dtype=np.float64)[None, :]).reshape(-1)
    return trig_tables(places, ROWS, NX * NY * 2)


def near(x):
    return pltpu.with_memory_space_constraint(x, pltpu.VMEM)


def vmem():
    return pl.BlockSpec(memory_space=pltpu.VMEM)


def nt(a, b):
    return lax.dot_general(a, b, (((1,), (1,)), ((), ())), preferred_element_type=f32)


def nn(a, b):
    return lax.dot_general(a, b, (((1,), (0,)), ((), ())), preferred_element_type=f32)


def params(limit=56, **kw):
    return pltpu.CompilerParams(vmem_limit_bytes=limit * 1024 * 1024, **kw)


KSTEP = 1024


def latents_body(
    tok, gain, qdw, qg, kdw, kg, rw, pw, q_out, kv_out, pool_out, inv, aq, ak, ar, ap
):
    k = pl.program_id(0)

    @pl.when(k == 0)
    def _():
        x = tok[...].astype(f32)
        inv[...] = jnp.broadcast_to(
            lax.rsqrt(jnp.mean(x * x, axis=-1, keepdims=True) + EPS), (ROWS, 128)
        )
        aq[...] = jnp.zeros_like(aq)
        ak[...] = jnp.zeros_like(ak)
        ar[...] = jnp.zeros_like(ar)
        ap[...] = jnp.zeros_like(ap)

    cols = pl.ds(pl.multiple_of(k * KSTEP, KSTEP), KSTEP)
    x = tok[:, cols].astype(f32)
    normed = (x * inv[:, 0:1] * gain[cols].astype(f32).reshape(1, KSTEP)).astype(bf16)
    aq[...] += nn(normed, qdw[...])
    ak[...] += nn(normed, kdw[...])
    ar[...] += nt(normed, rw[...])
    ap[...] += nn(normed, pw[...])

    @pl.when(k == pl.num_programs(0) - 1)
    def _():
        def norm(v, g):
            return (
                v
                * lax.rsqrt(jnp.mean(v * v, axis=-1, keepdims=True) + EPS)
                * g.astype(f32).reshape(1, -1)
            ).astype(bf16)

        q = norm(aq[...], qg[...])
        kv = norm(ak[...], kg[...])
        rope = jnp.concatenate(
            [ar[...].astype(bf16), jnp.zeros((ROWS, 128 - ROT), bf16)], axis=1
        )
        q_out[...] = q
        pool_out[...] = ap[...].astype(bf16)
        for n in range(NZ):
            kv_out[n, :, 0:KR] = kv
            kv_out[n, :, KR:] = rope


def latents(tok, gain, qdw, qg, kdw, kg, rw, pw):
    steps = WIDTH // KSTEP
    whole = lambda *s: pl.BlockSpec(s, lambda k: (0,) * len(s))
    part = lambda n: pl.BlockSpec((KSTEP, n), lambda k: (k, 0))
    return pl.pallas_call(
        latents_body,
        grid=(steps,),
        in_specs=[
            whole(ROWS, WIDTH),
            whole(WIDTH),
            part(QR),
            whole(QR),
            part(KR),
            whole(KR),
            pl.BlockSpec((ROT, KSTEP), lambda k: (0, k)),
            part(512),
        ],
        out_specs=(
            whole(ROWS, QR),
            whole(NZ, ROWS, KR + 128),
            whole(ROWS, 512),
        ),
        out_shape=(
            jax.ShapeDtypeStruct((ROWS, QR), bf16),
            jax.ShapeDtypeStruct((NZ, ROWS, KR + 128), bf16),
            jax.ShapeDtypeStruct((ROWS, 512), bf16),
        ),
        scratch_shapes=[
            pltpu.VMEM((ROWS, 128), f32),
            pltpu.VMEM((ROWS, QR), f32),
            pltpu.VMEM((ROWS, KR), f32),
            pltpu.VMEM((ROWS, ROT), f32),
            pltpu.VMEM((ROWS, 512), f32),
        ],
        compiler_params=params(dimension_semantics=("arbitrary",)),
        name="latents",
    )(tok, gain, qdw, qg, kdw, kg, rw.T, pw)


def angles(table, idx):
    lanes = lax.broadcasted_iota(jnp.int32, (HALF, 128), 1)
    hit = lanes == idx
    coff = table[:, 0:BLOCK]
    soff = table[:, BLOCK : 2 * BLOCK]
    cb = table[:, 2 * BLOCK : 2 * BLOCK + 128]
    sb = table[:, 2 * BLOCK + 128 :]
    cbase = jnp.sum(jnp.where(hit, cb, 0.0), axis=1, keepdims=True)
    sbase = jnp.sum(jnp.where(hit, sb, 0.0), axis=1, keepdims=True)
    return cbase * coff - sbase * soff, sbase * coff + cbase * soff


def column(gain):
    row = jnp.broadcast_to(gain[...].astype(f32).reshape(1, HEAD), (8, HEAD)).astype(bf16)
    eye = (
        lax.broadcasted_iota(jnp.int32, (HEAD, HEAD), 0)
        == lax.broadcasted_iota(jnp.int32, (HEAD, HEAD), 1)
    ).astype(bf16)
    return nt(eye, row)[:, 0:1]


def rotated(v, cosine, sine):
    a = v[NOPE : NOPE + HALF]
    b = v[NOPE + HALF :]
    return jnp.concatenate(
        [v[:NOPE], a * cosine - b * sine, a * sine + b * cosine, jnp.zeros_like(v[:ROT])],
        axis=0,
    )


def queries_body(
    own0, own1, own2, own3, two0, two1, two2, two3, wqt, gain, table, out, lat
):
    c = lax.axis_index("c")
    z = lax.axis_index("z")
    here = lax.axis_index("x")
    qgain = column(gain)
    own = (own0, own1, own2, own3)
    other = (two0, two1, two2, two3)
    y = lax.axis_index("y")
    for x in range(NX):
        for k in range(NY):
            piece = slice(k * ROWS, (k + 1) * ROWS)
            at = ((y + NY - k) % NY) * 2 * ROWS
            first = pl.multiple_of(at + c * ROWS, ROWS)
            lat[x, pl.ds(first, ROWS), :] = own[x][piece]
            second = pl.multiple_of(at + (1 - c) * ROWS, ROWS)
            lat[x, pl.ds(second, ROWS), :] = other[x][piece]
        q = nt(wqt[...], lat[x])
        block = (here + NX - x) % NX
        place = z * NX + block
        cosine, sine = angles(table, place)
        at = pl.multiple_of(block * BLOCK, BLOCK)
        for h in range(HEADS):
            v = q[h * HEAD : (h + 1) * HEAD]
            inv = lax.rsqrt(jnp.mean(v * v, axis=0, keepdims=True) + EPS)
            v = v * inv * qgain
            v = rotated(v, cosine, sine) * (LOG2E * HEAD**-0.5)
            out[h, :, pl.ds(at, BLOCK)] = v.astype(bf16)


def queries(own, other, wqt, qgain, table):
    return pl.pallas_call(
        queries_body,
        in_specs=[vmem()] * 11,
        out_specs=vmem(),
        out_shape=pltpu.VMEM((HEADS, 128, NQ), bf16),
        scratch_shapes=[pltpu.VMEM((NX, BLOCK, QR), bf16)],
        compiler_params=params(),
        name="queries",
    )(*own, *other, wqt, qgain, table)


def keys_body(count, *refs):
    own, other, wkvt, gain, table, kbuf, vbuf = refs[count:]
    c = lax.axis_index("c")
    x = lax.axis_index("x")
    kgain = column(gain)
    pick = (
        lax.broadcasted_iota(jnp.int32, (ROT, 128), 0)
        == lax.broadcasted_iota(jnp.int32, (ROT, 128), 1)
    ).astype(bf16)
    ones = (lax.broadcasted_iota(jnp.int32, (VROWS - VAL, BLOCK), 0) == 0).astype(bf16)
    blocks = [(own, k, k, c) for k in range(NY)] + [(other, k, k, 1 - c) for k in range(NY)]
    for b, (ref, at, y_from, c_from) in enumerate(blocks):
        lat = ref[at]
        kv = nt(wkvt[...], lat[:, :KR])
        rope = nt(pick, lat[:, KR:])
        rope_square = jnp.sum(rope * rope, axis=0, keepdims=True)
        place = (x * NY + y_from) * 2 + c_from
        cosine, sine = angles(table, place)
        cols = slice(b * BLOCK, (b + 1) * BLOCK)
        for h in range(HEADS):
            plain = kv[h * 128 : h * 128 + NOPE]
            total = jnp.sum(plain * plain, axis=0, keepdims=True) + rope_square
            inv = lax.rsqrt(total * (1.0 / HEAD) + EPS)
            k = jnp.concatenate([plain, rope], axis=0) * inv * kgain
            k = rotated(k, cosine, sine).astype(bf16)
            kbuf[h, cols, :] = k.T
            vbuf[h, 0:VAL, cols] = kv[h * 128 + NOPE : (h + 1) * 128].astype(bf16)
            vbuf[h, VAL:, cols] = ones


def keys_values(after, own, other, wkvt, kgain, table):
    count = 2 * NY * BLOCK

    def body(*refs):
        keys_body(len(after), *refs)

    return pl.pallas_call(
        body,
        in_specs=[pl.BlockSpec(memory_space=pl.ANY)] * len(after) + [vmem()] * 5,
        out_specs=(vmem(), vmem()),
        out_shape=(
            pltpu.VMEM((HEADS, count, 128), bf16),
            pltpu.VMEM((HEADS, VROWS, count), bf16),
        ),
        compiler_params=params(),
        name="keys",
    )(*after, own, other, wkvt, kgain, table)


CHUNK = 256
SUB = 128
TILES = HEADS * (NQ // QTILE)


def attend_body(
    kbuf, vbuf, qt, out, l0, l1, l2, l3, buf0, buf1, acc_s, m_s, logs, msg, sems
):
    bufs = (buf0, buf1)
    pairs = [(kbuf, vbuf)]
    sizes = [kbuf.shape[1]]
    chunks = []
    base = 0
    for (kr, vr), n in zip(pairs, sizes):
        for at in range(0, n, CHUNK):
            size = min(CHUNK, n - at)
            chunks.append((base + at, size, kr, vr, at))
        base += n

    def where(i):
        per = NQ // QTILE
        return i // per, pl.ds(pl.multiple_of((i % per) * QTILE, QTILE), QTILE)

    def score(i, chunk, buf, top):
        row, size, kr, _, at = chunk
        h, col = where(i)
        for sub in range(0, size, SUB):
            s = nn(kr[h, at + sub : at + sub + SUB, :], qt[h, :, col])
            buf[row + sub : row + sub + SUB, :] = s
            top = jnp.maximum(top, jnp.max(s.reshape(SUB // 8, 8, QTILE), axis=0))
        return top

    def weigh(i, chunk, buf, m):
        row, size, _, vr, at = chunk
        h, _ = where(i)
        p = jnp.exp2(buf[row : row + size, :] - m).astype(bf16)
        return nn(vr[h, :, at : at + size], p)

    low = jnp.full((8, QTILE), -1e30, f32)

    def settle(top):
        return jnp.max(top, axis=0, keepdims=True)

    def finish(i, m, acc):
        h, col = where(i)
        acc_s[h, :, col] = acc
        m_s[h, :, col] = m

    def both(i, m, buf, nxt):
        acc = None
        top = low
        for chunk in chunks:
            part = weigh(i, chunk, buf, m)
            acc = part if acc is None else acc + part
            top = score(i + 1, chunk, nxt, top)
        finish(i, m, acc)
        return settle(top)

    top = low
    for chunk in chunks:
        top = score(0, chunk, bufs[0], top)
    m = settle(top)

    def pair(j, m):
        m = both(2 * j, m, bufs[0], bufs[1])
        return both(2 * j + 1, m, bufs[1], bufs[0])

    m = lax.fori_loop(0, (TILES - 1) // 2, pair, m)
    acc = None
    for chunk in chunks:
        part = weigh(TILES - 1, chunk, bufs[0], m)
        acc = part if acc is None else acc + part
    finish(TILES - 1, m, acc)

    for x in range(NX):
        cols = slice(x * BLOCK, (x + 1) * BLOCK)
        parts = []
        stats = []
        for h in range(HEADS):
            total = acc_s[h, VAL : VAL + 1, cols]
            parts.append((acc_s[h, 0:VAL, cols] * (1.0 / total)).astype(bf16))
            lse = (m_s[h, :, cols] + jnp.log2(total)) * LN2
            logs[x, h : h + 1, :] = lse
            hi = lse.astype(bf16)
            rest = lse - hi.astype(f32)
            mid = rest.astype(bf16)
            low_part = (rest - mid.astype(f32)).astype(bf16)
            stats += [hi.astype(f32), mid.astype(f32), low_part.astype(f32)]
        stats.append(jnp.zeros((MSG - HEADS * VAL - 9, BLOCK), f32))
        parts.append(jnp.concatenate(stats, axis=0).astype(bf16))
        rows = jnp.concatenate(parts, axis=0).T
        for y in range(NY):
            msg[x * NY + y, :, :] = rows[y * 2 * ROWS : (y + 1) * 2 * ROWS]
        pltpu.make_async_copy(
            msg.at[x * NY : (x + 1) * NY], out.at[x * NY : (x + 1) * NY], sems.at[x]
        ).start()
    here = lax.axis_index("x")
    for k, ref in enumerate((l0, l1, l2, l3)):
        ref[...] = logs[(here + k) % NX]
    for x in range(NX):
        pltpu.make_async_copy(
            msg.at[x * NY : (x + 1) * NY], out.at[x * NY : (x + 1) * NY], sems.at[x]
        ).wait()


def attend(kbuf, vbuf, qt):
    return pl.pallas_call(
        attend_body,
        in_specs=[vmem()] * 3,
        out_specs=(pl.BlockSpec(memory_space=pl.ANY), *[vmem()] * 4),
        out_shape=(
            jax.ShapeDtypeStruct((NX * NY, 2 * ROWS, MSG), bf16),
            *[jax.ShapeDtypeStruct((8, BLOCK), f32)] * NX,
        ),
        scratch_shapes=[
            pltpu.VMEM((kbuf.shape[1], QTILE), f32),
            pltpu.VMEM((kbuf.shape[1], QTILE), f32),
            pltpu.VMEM((HEADS, VROWS, NQ), f32),
            pltpu.VMEM((HEADS, 1, NQ), f32),
            pltpu.VMEM((NX, 8, BLOCK), f32),
            pltpu.VMEM((NX * NY, 2 * ROWS, MSG), bf16),
            pltpu.SemaphoreType.DMA((NX,)),
        ],
        compiler_params=params(40),
        name="attend",
    )(near(kbuf), near(vbuf), near(qt))


def logsum_body(a, b, c, d, out):
    logs = [r[0:HEADS, :] for r in (a, b, c, d)]
    top = jnp.maximum(jnp.maximum(logs[0], logs[1]), jnp.maximum(logs[2], logs[3]))
    total = sum(jnp.exp(v - top) for v in logs)
    out[...] = top + jnp.log(total)


def logsums(parts):
    return pl.pallas_call(
        logsum_body,
        in_specs=[vmem()] * NX,
        out_specs=vmem(),
        out_shape=jax.ShapeDtypeStruct((HEADS, BLOCK), f32),
        compiler_params=params(),
        name="logsums",
    )(*parts)


PLACES = (0, -1, 1, 2)


def pool_body(own, low, high, keep, send, buf):
    z, here, y0, c = [lax.axis_index(n) for n in "zxyc"]
    first = ((z * NX + here) * NY * 2 + y0 * 2 + c) * ROWS
    x = own[...].astype(f32)
    side = jnp.zeros((8, 512), f32)
    window = jnp.concatenate(
        [side, low[...].astype(f32), x, high[...].astype(f32), side], axis=0
    )
    n = ROWS + 32
    s1 = window[0 : n - 1] + window[1:n]
    s2 = s1[0 : n - 3] + s1[2 : n - 1]
    s4 = s2[0 : n - 7] + s2[4 : n - 3]
    s8 = s4[0 : n - 15] + s4[8 : n - 7]
    w1 = s1[15 : 15 + ROWS]
    w2 = s2[14 : 14 + ROWS]
    w4 = s4[12 : 12 + ROWS]
    w8 = s8[8 : 8 + ROWS]
    group = (lax.broadcasted_iota(jnp.int32, (ROWS, 512), 1) // 64) % 4
    total = jnp.where(
        group == 0, w1, jnp.where(group == 1, w2, jnp.where(group == 2, w4, w8))
    )
    half = jnp.where(group == 0, 1, jnp.where(group == 1, 2, jnp.where(group == 2, 4, 8)))
    place = first + lax.broadcasted_iota(jnp.int32, (ROWS, 512), 0)
    count = (jnp.minimum(place + half, TOKENS) - jnp.maximum(place - half, 0)).astype(f32)
    buf[...] = (total / count - x).astype(bf16)
    even, odd = [], []
    for d in PLACES:
        at = pl.multiple_of(((y0 + NY + d) % NY) * 128, 128)
        tile = buf[:, pl.ds(at, 128)]
        even.append(tile[:, 0:64])
        odd.append(tile[:, 64:128])
    even = jnp.concatenate(even, axis=1)
    odd = jnp.concatenate(odd, axis=1)
    keep[...] = jnp.where(c == 0, even, odd)
    send[...] = jnp.where(c == 0, odd, even)


def pooling(own, low, high):
    return pl.pallas_call(
        pool_body,
        in_specs=[vmem()] * 3,
        out_specs=(vmem(), vmem()),
        out_shape=(
            jax.ShapeDtypeStruct((ROWS, 256), bf16),
            jax.ShapeDtypeStruct((ROWS, 256), bf16),
        ),
        scratch_shapes=[pltpu.VMEM((ROWS, 512), bf16)],
        compiler_params=params(),
        name="pooling",
    )(own, low, high)


def project_body(got, mine, theirs, *refs):
    sources = refs[:8]
    keep, send, wbuf, sems = refs[8:]
    y0 = lax.axis_index("y")
    c = lax.axis_index("c")
    copies = []
    for n, ref in enumerate(sources):
        at = 128 * (n % 2)
        copies.append(
            pltpu.make_async_copy(ref, wbuf.at[n // 2, at : at + 128], sems.at[n])
        )
    for copy in copies:
        copy.start()
    row = lax.broadcasted_iota(jnp.int32, (128, HEADS * VAL), 0)
    head = lax.broadcasted_iota(jnp.int32, (128, HEADS * VAL), 1) // VAL
    spread = ((row >= 64 + 3 * head) & (row < 67 + 3 * head)).astype(bf16)
    inputs = []
    for n, d in enumerate(PLACES):
        slots = [x * NY + (y0 + NY + d) % NY for x in range(NX)]
        logs = [nn(got[slot, :, 128:256], spread) for slot in slots]
        top = jnp.maximum(jnp.maximum(logs[0], logs[1]), jnp.maximum(logs[2], logs[3]))
        weights = [jnp.exp(v - top) for v in logs]
        total = weights[0] + weights[1] + weights[2] + weights[3]
        acc = jnp.zeros((2 * ROWS, HEADS * VAL), f32)
        for slot, w in zip(slots, weights):
            acc = acc + got[slot, :, 0 : HEADS * VAL].astype(f32) * w
        own = mine[:, n * 64 : (n + 1) * 64]
        twin = theirs[:, n * 64 : (n + 1) * 64]
        pool = jnp.concatenate(
            [jnp.where(c == 0, own, twin), jnp.where(c == 0, twin, own)], axis=0
        )
        inputs.append(jnp.concatenate([(acc / total).astype(bf16), pool], axis=1))
    for copy in copies:
        copy.wait()
    for col in range(0, WIDTH, 512):
        cols = slice(col, col + 512)
        result = nn(inputs[0], wbuf[0, :, cols])
        for n in range(1, NY):
            result = result + nn(inputs[n], wbuf[n, :, cols])
        first, second = result[0:ROWS], result[ROWS:]
        keep[:, cols] = jnp.where(c == 0, first, second)
        send[:, cols] = jnp.where(c == 0, second, first).astype(bf16)


def project(got, mine, theirs, weights):
    return pl.pallas_call(
        project_body,
        in_specs=[vmem()] * 3 + [pl.BlockSpec(memory_space=pl.ANY)] * 8,
        out_specs=(vmem(), vmem()),
        out_shape=(
            pltpu.VMEM((ROWS, WIDTH), f32),
            pltpu.VMEM((ROWS, WIDTH), bf16),
        ),
        scratch_shapes=[
            pltpu.VMEM((NY, 256, WIDTH), bf16),
            pltpu.SemaphoreType.DMA((8,)),
        ],
        compiler_params=params(40),
        name="project",
    )(near(got), near(mine), near(theirs), *weights)


def across(x):
    return lax.ppermute(x, "c", [(0, 1), (1, 0)])


def shifted(x, axis, places):
    count = lax.axis_size(axis)
    return lax.ppermute(x, axis, [(i, (i + places) % count) for i in range(count)])


def shards(
    tokens,
    norm_gain,
    query_down_weight,
    query_latent_norm_gain,
    key_value_down_weight,
    key_value_latent_gain,
    w_rope_key,
    w_pool_in,
    query_up_weight,
    key_value_up_weight,
    query_gain,
    key_gain,
    w_pool_mix,
    pool_scale,
    w_out_attn,
    w_out_pool,
):
    wqt = query_up_weight.T
    wkvt = key_value_up_weight.T

    q_all, kv_all, pool_in = latents(
        tokens,
        norm_gain,
        query_down_weight,
        query_latent_norm_gain,
        key_value_down_weight,
        key_value_latent_gain,
        w_rope_key,
        w_pool_in,
    )
    pieces = [q_all] + [shifted(q_all, "y", k) for k in range(1, NY)]
    kv_own = lax.all_to_all(kv_all, "z", 0, 0, tiled=True).reshape(NZ * ROWS, KR + 128)

    count = NZ * NX * NY * 2
    every = ("z", "x", "y", "c")
    low = lax.ppermute(
        pool_in[ROWS - 8 :], every, [(i, i + 1) for i in range(count - 1)]
    )
    high = lax.ppermute(pool_in[:8], every, [(i + 1, i) for i in range(count - 1)])
    pool_mine, pool_send = pooling(pool_in, low, high)
    pool_theirs = across(pool_send)

    folded = jnp.dot(
        w_pool_mix[0],
        (pool_scale.astype(f32)[:, None] * w_out_pool.astype(f32)).astype(bf16),
        preferred_element_type=f32,
    ).astype(bf16)
    upper = w_out_attn[:128]
    lower = jnp.concatenate([w_out_attn[128:], folded], axis=0)
    upper1 = shifted(upper, "y", 1)
    lower3 = shifted(lower, "y", NY - 1)
    lower1 = shifted(lower, "y", 1)
    upper3 = shifted(upper, "y", NY - 1)
    upper2 = shifted(upper1, "y", 1)
    lower2 = shifted(lower3, "y", NY - 1)
    pieces_w = (upper, lower, upper1, lower1, upper3, lower3, upper2, lower2)

    kv = lax.all_to_all(
        jnp.broadcast_to(kv_own[None], (NY, *kv_own.shape)), "y", 0, 0, tiled=True
    )
    q_side = jnp.concatenate(pieces, axis=0)
    q_own = [q_side] + [shifted(q_side, "x", k) for k in range(1, NX)]
    q_twin = [across(q) for q in q_own]
    kv_twin = across(kv)
    qt = queries(q_own, q_twin, wqt, query_gain, query_tables())
    pair = keys_values((), kv, kv_twin, wkvt, key_gain, key_tables())
    message, *logs = attend(*pair, qt)

    got = lax.all_to_all(message, ("x", "y"), 0, 0, tiled=True)
    logs = [logs[0]] + [shifted(logs[k], "x", k) for k in range(1, NX)]
    row_logsum = logsums(logs)
    keep, send = project(got, pool_mine, pool_theirs, pieces_w)
    received = across(send)
    mixed = (keep + received.astype(f32)).astype(bf16)
    return mixed, row_logsum


def solution(mesh):
    fine = Mesh(mesh.devices.reshape(NZ, NX, NY, 2), ("z", "x", "y", "c"))
    tp = ("y", "c")
    placed = (
        P(("z", "x", "y", "c"), None),
        P(),
        P(),
        P(),
        P(),
        P(),
        P(),
        P(),
        P(None, tp),
        P(None, tp),
        P(),
        P(),
        P(tp, None, None),
        P(tp),
        P(tp, None),
        P(tp, None),
    )

    return jax.shard_map(
        shards,
        mesh=fine,
        in_specs=placed,
        out_specs=(P(("z", "x", "y", "c"), None), P(tp, ("z", "x"))),
        check_vma=False,
    )
```

```python
import jax
import jax.numpy as jnp
import numpy as np
from jax import lax
from jax.experimental import pallas as pl
from jax.experimental.pallas import tpu as pltpu
from jax.sharding import Mesh, PartitionSpec as P

NOPE = 64
ROT = 32
HALF = 16
HEAD = 96
VAL = 64
HEADS = 3
QR = 512
KR = 256
EPS = 1e-06
WIDTH = 2048
ROWS = 48
BLOCK = 384
TOKENS = 12288
LOG2E = 1.4426950408889634
LN2 = 0.6931471805599453
MSG = 256
VROWS = 80
QTILE = 512
NX = 4
NY = 4
NZ = 8
NQ = NX * BLOCK

bf16 = jnp.bfloat16
f32 = jnp.float32


def trig_tables(inner_places, outer_step, outer_count):
    freqs = 10000.0 ** (-np.arange(HALF, dtype=np.float64) / HALF)
    inner = freqs[:, None] * inner_places[None, :]
    outer = freqs[:, None] * (outer_step * np.arange(outer_count, dtype=np.float64))[None, :]
    pad = np.zeros((HALF, 128 - outer_count))
    cast = lambda a: a.astype(np.float32)
    parts = [np.cos(inner), np.sin(inner), np.cos(outer), pad, np.sin(outer), pad]
    return cast(np.concatenate(parts, 1))


def query_tables():
    return trig_tables(np.arange(BLOCK, dtype=np.float64), BLOCK, NZ * NX)


def key_tables():
    z = np.arange(NZ, dtype=np.float64)
    places = (NX * BLOCK * z[:, None] + np.arange(ROWS, dtype=np.float64)[None, :]).reshape(-1)
    return trig_tables(places, ROWS, NX * NY * 2)


def near(x):
    return pltpu.with_memory_space_constraint(x, pltpu.VMEM)


def vmem():
    return pl.BlockSpec(memory_space=pltpu.VMEM)


def nt(a, b):
    return lax.dot_general(a, b, (((1,), (1,)), ((), ())), preferred_element_type=f32)


def nn(a, b):
    return lax.dot_general(a, b, (((1,), (0,)), ((), ())), preferred_element_type=f32)


def params(limit=56, **kw):
    return pltpu.CompilerParams(vmem_limit_bytes=limit * 1024 * 1024, **kw)


KSTEP = 1024


def latents_body(
    tok, gain, qdw, qg, kdw, kg, rw, pw, q_out, kv_out, pool_out, inv, aq, ak, ar, ap
):
    k = pl.program_id(0)

    @pl.when(k == 0)
    def _():
        x = tok[...].astype(f32)
        inv[...] = jnp.broadcast_to(
            lax.rsqrt(jnp.mean(x * x, axis=-1, keepdims=True) + EPS), (ROWS, 128)
        )
        aq[...] = jnp.zeros_like(aq)
        ak[...] = jnp.zeros_like(ak)
        ar[...] = jnp.zeros_like(ar)
        ap[...] = jnp.zeros_like(ap)

    cols = pl.ds(pl.multiple_of(k * KSTEP, KSTEP), KSTEP)
    x = tok[:, cols].astype(f32)
    normed = (x * inv[:, 0:1] * gain[cols].astype(f32).reshape(1, KSTEP)).astype(bf16)
    aq[...] += nn(normed, qdw[...])
    ak[...] += nn(normed, kdw[...])
    ar[...] += nt(normed, rw[...])
    ap[...] += nn(normed, pw[...])

    @pl.when(k == pl.num_programs(0) - 1)
    def _():
        def norm(v, g):
            return (
                v
                * lax.rsqrt(jnp.mean(v * v, axis=-1, keepdims=True) + EPS)
                * g.astype(f32).reshape(1, -1)
            ).astype(bf16)

        q = norm(aq[...], qg[...])
        kv = norm(ak[...], kg[...])
        groups = [ar[8 * g : 8 * g + 8, :] for g in range(ROWS // 8)]
        groups.append(jnp.zeros((8, KR - ROT * (ROWS // 8)), f32))
        rope = jnp.concatenate(groups, axis=1).astype(bf16)
        q_out[...] = q
        pool_out[...] = ap[...].astype(bf16)
        for n in range(NZ):
            kv_out[n, 0:ROWS, :] = kv
            kv_out[n, ROWS:, :] = rope


def latents(tok, gain, qdw, qg, kdw, kg, rw, pw):
    steps = WIDTH // KSTEP
    whole = lambda *s: pl.BlockSpec(s, lambda k: (0,) * len(s))
    part = lambda n: pl.BlockSpec((KSTEP, n), lambda k: (k, 0))
    return pl.pallas_call(
        latents_body,
        grid=(steps,),
        in_specs=[
            whole(ROWS, WIDTH),
            whole(WIDTH),
            part(QR),
            whole(QR),
            part(KR),
            whole(KR),
            pl.BlockSpec((ROT, KSTEP), lambda k: (0, k)),
            part(512),
        ],
        out_specs=(
            whole(ROWS, QR),
            whole(NZ, ROWS + 8, KR),
            whole(ROWS, 512),
        ),
        out_shape=(
            jax.ShapeDtypeStruct((ROWS, QR), bf16),
            jax.ShapeDtypeStruct((NZ, ROWS + 8, KR), bf16),
            jax.ShapeDtypeStruct((ROWS, 512), bf16),
        ),
        scratch_shapes=[
            pltpu.VMEM((ROWS, 128), f32),
            pltpu.VMEM((ROWS, QR), f32),
            pltpu.VMEM((ROWS, KR), f32),
            pltpu.VMEM((ROWS, ROT), f32),
            pltpu.VMEM((ROWS, 512), f32),
        ],
        compiler_params=params(dimension_semantics=("arbitrary",)),
        name="latents",
    )(tok, gain, qdw, qg, kdw, kg, rw.T, pw)


def angles(table, idx):
    lanes = lax.broadcasted_iota(jnp.int32, (HALF, 128), 1)
    hit = lanes == idx
    coff = table[:, 0:BLOCK]
    soff = table[:, BLOCK : 2 * BLOCK]
    cb = table[:, 2 * BLOCK : 2 * BLOCK + 128]
    sb = table[:, 2 * BLOCK + 128 :]
    cbase = jnp.sum(jnp.where(hit, cb, 0.0), axis=1, keepdims=True)
    sbase = jnp.sum(jnp.where(hit, sb, 0.0), axis=1, keepdims=True)
    return cbase * coff - sbase * soff, sbase * coff + cbase * soff


def column(gain):
    row = jnp.broadcast_to(gain[...].astype(f32).reshape(1, HEAD), (8, HEAD)).astype(bf16)
    eye = (
        lax.broadcasted_iota(jnp.int32, (HEAD, HEAD), 0)
        == lax.broadcasted_iota(jnp.int32, (HEAD, HEAD), 1)
    ).astype(bf16)
    return nt(eye, row)[:, 0:1]


def rotated(v, cosine, sine):
    a = v[NOPE : NOPE + HALF]
    b = v[NOPE + HALF :]
    return jnp.concatenate(
        [v[:NOPE], a * cosine - b * sine, a * sine + b * cosine, jnp.zeros_like(v[:ROT])],
        axis=0,
    )


def queries_body(
    early, own0, own1, own2, own3, two0, two1, two2, two3, wqt, gain, table, out, lat
):
    c = lax.axis_index("c")
    z = lax.axis_index("z")
    here = lax.axis_index("x")
    qgain = column(gain)
    own = (own0, own1, own2, own3)
    other = (two0, two1, two2, two3)
    y = lax.axis_index("y")
    for x in range(NX):
        for k in range(NY):
            piece = slice(k * ROWS, (k + 1) * ROWS)
            at = ((y + NY - k) % NY) * 2 * ROWS
            first = pl.multiple_of(at + c * ROWS, ROWS)
            lat[x, pl.ds(first, ROWS), :] = own[x][piece]
            second = pl.multiple_of(at + (1 - c) * ROWS, ROWS)
            lat[x, pl.ds(second, ROWS), :] = other[x][piece]
        q = nt(wqt[...], lat[x])
        block = (here + NX - x) % NX
        place = z * NX + block
        cosine, sine = angles(table, place)
        at = pl.multiple_of(block * BLOCK, BLOCK)
        for h in range(HEADS):
            v = q[h * HEAD : (h + 1) * HEAD]
            inv = lax.rsqrt(jnp.mean(v * v, axis=0, keepdims=True) + EPS)
            v = v * inv * qgain
            v = rotated(v, cosine, sine) * (LOG2E * HEAD**-0.5)
            out[h, :, pl.ds(at, BLOCK)] = v.astype(bf16)


def queries(early, own, other, wqt, qgain, table):
    return pl.pallas_call(
        queries_body,
        in_specs=[pl.BlockSpec(memory_space=pl.ANY)] + [vmem()] * 11,
        out_specs=vmem(),
        out_shape=pltpu.VMEM((HEADS, 128, NQ), bf16),
        scratch_shapes=[pltpu.VMEM((NX, BLOCK, QR), bf16)],
        compiler_params=params(),
        name="queries",
    )(early, *own, *other, wqt, qgain, table)


def keys_body(count, *refs):
    own, other, wkvt, gain, table, kbuf, vbuf = refs[count:]
    c = lax.axis_index("c")
    x = lax.axis_index("x")
    kgain = column(gain)
    pick = (
        lax.broadcasted_iota(jnp.int32, (ROT, KR), 0)
        == lax.broadcasted_iota(jnp.int32, (ROT, KR), 1) % ROT
    ).astype(bf16)
    group = lax.broadcasted_iota(jnp.int32, (8, KR), 1) // ROT
    ones = (lax.broadcasted_iota(jnp.int32, (VROWS - VAL, BLOCK), 0) == 0).astype(bf16)
    blocks = [(own, k, k, c) for k in range(NY)] + [(other, k, k, 1 - c) for k in range(NY)]
    for b, (ref, at, y_from, c_from) in enumerate(blocks):
        lat, spread = [], []
        for z in range(NZ):
            row = z * (ROWS + 8)
            lat.append(ref[at, row : row + ROWS, :])
            packed = ref[at, row + ROWS : row + ROWS + 8, :].astype(f32)
            spread += [jnp.where(group == g, packed, 0.0) for g in range(ROWS // 8)]
        kv = nt(wkvt[...], jnp.concatenate(lat, axis=0))
        rope = nt(pick, jnp.concatenate(spread, axis=0).astype(bf16))
        rope_square = jnp.sum(rope * rope, axis=0, keepdims=True)
        place = (x * NY + y_from) * 2 + c_from
        cosine, sine = angles(table, place)
        cols = slice(b * BLOCK, (b + 1) * BLOCK)
        for h in range(HEADS):
            plain = kv[h * 128 : h * 128 + NOPE]
            total = jnp.sum(plain * plain, axis=0, keepdims=True) + rope_square
            inv = lax.rsqrt(total * (1.0 / HEAD) + EPS)
            k = jnp.concatenate([plain, rope], axis=0) * inv * kgain
            k = rotated(k, cosine, sine).astype(bf16)
            kbuf[h, cols, :] = k.T
            vbuf[h, 0:VAL, cols] = kv[h * 128 + NOPE : (h + 1) * 128].astype(bf16)
            vbuf[h, VAL:, cols] = ones


def keys_values(after, own, other, wkvt, kgain, table):
    count = 2 * NY * BLOCK

    def body(*refs):
        keys_body(len(after), *refs)

    return pl.pallas_call(
        body,
        in_specs=[pl.BlockSpec(memory_space=pl.ANY)] * len(after) + [vmem()] * 5,
        out_specs=(vmem(), vmem()),
        out_shape=(
            pltpu.VMEM((HEADS, count, 128), bf16),
            pltpu.VMEM((HEADS, VROWS, count), bf16),
        ),
        compiler_params=params(),
        name="keys",
    )(*after, own, other, wkvt, kgain, table)


CHUNK = 256
SUB = 256
TILES = HEADS * (NQ // QTILE)


def attend_body(
    kbuf, vbuf, qt, out, l0, l1, l2, l3, buf0, buf1, acc_s, m_s, logs, msg, sems
):
    bufs = (buf0, buf1)
    pairs = [(kbuf, vbuf)]
    sizes = [kbuf.shape[1]]
    chunks = []
    base = 0
    for (kr, vr), n in zip(pairs, sizes):
        for at in range(0, n, CHUNK):
            size = min(CHUNK, n - at)
            chunks.append((base + at, size, kr, vr, at))
        base += n

    def where(i):
        per = NQ // QTILE
        return i // per, pl.ds(pl.multiple_of((i % per) * QTILE, QTILE), QTILE)

    def score(i, chunk, buf, top):
        row, size, kr, _, at = chunk
        h, col = where(i)
        for sub in range(0, size, SUB):
            s = nn(kr[h, at + sub : at + sub + SUB, :], qt[h, :, col])
            buf[row + sub : row + sub + SUB, :] = s
            top = jnp.maximum(top, jnp.max(s.reshape(SUB // 8, 8, QTILE), axis=0))
        return top

    def weigh(i, chunk, buf, m):
        row, size, _, vr, at = chunk
        h, _ = where(i)
        p = jnp.exp2(buf[row : row + size, :] - m).astype(bf16)
        return nn(vr[h, :, at : at + size], p)

    low = jnp.full((8, QTILE), -1e30, f32)

    def settle(top):
        return jnp.max(top, axis=0, keepdims=True)

    def finish(i, m, acc):
        h, col = where(i)
        acc_s[h, :, col] = acc
        m_s[h, :, col] = m

    def both(i, m, buf, nxt):
        acc = None
        top = low
        for chunk in chunks:
            top = score(i + 1, chunk, nxt, top)
            part = weigh(i, chunk, buf, m)
            acc = part if acc is None else acc + part
        finish(i, m, acc)
        return settle(top)

    top = low
    for chunk in chunks:
        top = score(0, chunk, bufs[0], top)
    m = settle(top)

    def pair(j, m):
        m = both(2 * j, m, bufs[0], bufs[1])
        return both(2 * j + 1, m, bufs[1], bufs[0])

    m = lax.fori_loop(0, (TILES - 1) // 2, pair, m)
    acc = None
    for chunk in chunks:
        part = weigh(TILES - 1, chunk, bufs[0], m)
        acc = part if acc is None else acc + part
    finish(TILES - 1, m, acc)

    for x in range(NX):
        cols = slice(x * BLOCK, (x + 1) * BLOCK)
        parts = []
        stats = []
        for h in range(HEADS):
            total = acc_s[h, VAL : VAL + 1, cols]
            parts.append((acc_s[h, 0:VAL, cols] * (1.0 / total)).astype(bf16))
            lse = (m_s[h, :, cols] + jnp.log2(total)) * LN2
            logs[x, h : h + 1, :] = lse
            hi = lse.astype(bf16)
            rest = lse - hi.astype(f32)
            mid = rest.astype(bf16)
            low_part = (rest - mid.astype(f32)).astype(bf16)
            stats += [hi.astype(f32), mid.astype(f32), low_part.astype(f32)]
        stats.append(jnp.zeros((MSG - HEADS * VAL - 9, BLOCK), f32))
        parts.append(jnp.concatenate(stats, axis=0).astype(bf16))
        rows = jnp.concatenate(parts, axis=0).T
        for y in range(NY):
            msg[x * NY + y, :, :] = rows[y * 2 * ROWS : (y + 1) * 2 * ROWS]
        pltpu.make_async_copy(
            msg.at[x * NY : (x + 1) * NY], out.at[x * NY : (x + 1) * NY], sems.at[x]
        ).start()
    here = lax.axis_index("x")
    for k, ref in enumerate((l0, l1, l2, l3)):
        ref[...] = logs[(here + k) % NX]
    for x in range(NX):
        pltpu.make_async_copy(
            msg.at[x * NY : (x + 1) * NY], out.at[x * NY : (x + 1) * NY], sems.at[x]
        ).wait()


def attend(kbuf, vbuf, qt):
    return pl.pallas_call(
        attend_body,
        in_specs=[vmem()] * 3,
        out_specs=(pl.BlockSpec(memory_space=pl.ANY), *[vmem()] * 4),
        out_shape=(
            jax.ShapeDtypeStruct((NX * NY, 2 * ROWS, MSG), bf16),
            *[jax.ShapeDtypeStruct((8, BLOCK), f32)] * NX,
        ),
        scratch_shapes=[
            pltpu.VMEM((kbuf.shape[1], QTILE), f32),
            pltpu.VMEM((kbuf.shape[1], QTILE), f32),
            pltpu.VMEM((HEADS, VROWS, NQ), f32),
            pltpu.VMEM((HEADS, 1, NQ), f32),
            pltpu.VMEM((NX, 8, BLOCK), f32),
            pltpu.VMEM((NX * NY, 2 * ROWS, MSG), bf16),
            pltpu.SemaphoreType.DMA((NX,)),
        ],
        compiler_params=params(40),
        name="attend",
    )(near(kbuf), near(vbuf), near(qt))


def logsum_body(a, b, c, d, out):
    logs = [r[0:HEADS, :] for r in (a, b, c, d)]
    top = jnp.maximum(jnp.maximum(logs[0], logs[1]), jnp.maximum(logs[2], logs[3]))
    total = sum(jnp.exp(v - top) for v in logs)
    out[...] = top + jnp.log(total)


def logsums(parts):
    return pl.pallas_call(
        logsum_body,
        in_specs=[vmem()] * NX,
        out_specs=vmem(),
        out_shape=jax.ShapeDtypeStruct((HEADS, BLOCK), f32),
        compiler_params=params(),
        name="logsums",
    )(*parts)


PLACES = (0, -1, 1, 2)


def pool_body(own, low, high, keep, send, buf):
    z, here, y0, c = [lax.axis_index(n) for n in "zxyc"]
    first = ((z * NX + here) * NY * 2 + y0 * 2 + c) * ROWS
    x = own[...].astype(f32)
    side = jnp.zeros((8, 512), f32)
    window = jnp.concatenate(
        [side, low[...].astype(f32), x, high[...].astype(f32), side], axis=0
    )
    n = ROWS + 32
    s1 = window[0 : n - 1] + window[1:n]
    s2 = s1[0 : n - 3] + s1[2 : n - 1]
    s4 = s2[0 : n - 7] + s2[4 : n - 3]
    s8 = s4[0 : n - 15] + s4[8 : n - 7]
    w1 = s1[15 : 15 + ROWS]
    w2 = s2[14 : 14 + ROWS]
    w4 = s4[12 : 12 + ROWS]
    w8 = s8[8 : 8 + ROWS]
    group = (lax.broadcasted_iota(jnp.int32, (ROWS, 512), 1) // 64) % 4
    total = jnp.where(
        group == 0, w1, jnp.where(group == 1, w2, jnp.where(group == 2, w4, w8))
    )
    half = jnp.where(group == 0, 1, jnp.where(group == 1, 2, jnp.where(group == 2, 4, 8)))
    place = first + lax.broadcasted_iota(jnp.int32, (ROWS, 512), 0)
    count = (jnp.minimum(place + half, TOKENS) - jnp.maximum(place - half, 0)).astype(f32)
    buf[...] = (total / count - x).astype(bf16)
    even, odd = [], []
    for d in PLACES:
        at = pl.multiple_of(((y0 + NY + d) % NY) * 128, 128)
        tile = buf[:, pl.ds(at, 128)]
        even.append(tile[:, 0:64])
        odd.append(tile[:, 64:128])
    even = jnp.concatenate(even, axis=1)
    odd = jnp.concatenate(odd, axis=1)
    keep[...] = jnp.where(c == 0, even, odd)
    send[...] = jnp.where(c == 0, odd, even)


def pooling(own, low, high):
    return pl.pallas_call(
        pool_body,
        in_specs=[vmem()] * 3,
        out_specs=(vmem(), vmem()),
        out_shape=(
            jax.ShapeDtypeStruct((ROWS, 256), bf16),
            jax.ShapeDtypeStruct((ROWS, 256), bf16),
        ),
        scratch_shapes=[pltpu.VMEM((ROWS, 512), bf16)],
        compiler_params=params(),
        name="pooling",
    )(own, low, high)


def project_body(got, mine, theirs, *refs):
    sources = refs[:8]
    keep, send, wbuf, sems = refs[8:]
    y0 = lax.axis_index("y")
    c = lax.axis_index("c")
    copies = []
    for n, ref in enumerate(sources):
        at = 128 * (n % 2)
        copies.append(
            pltpu.make_async_copy(ref, wbuf.at[n // 2, at : at + 128], sems.at[n])
        )
    for copy in copies:
        copy.start()
    row = lax.broadcasted_iota(jnp.int32, (128, HEADS * VAL), 0)
    head = lax.broadcasted_iota(jnp.int32, (128, HEADS * VAL), 1) // VAL
    spread = ((row >= 64 + 3 * head) & (row < 67 + 3 * head)).astype(bf16)
    inputs = []
    for n, d in enumerate(PLACES):
        slots = [x * NY + (y0 + NY + d) % NY for x in range(NX)]
        logs = [nn(got[slot, :, 128:256], spread) for slot in slots]
        top = jnp.maximum(jnp.maximum(logs[0], logs[1]), jnp.maximum(logs[2], logs[3]))
        weights = [jnp.exp(v - top) for v in logs]
        total = weights[0] + weights[1] + weights[2] + weights[3]
        acc = jnp.zeros((2 * ROWS, HEADS * VAL), f32)
        for slot, w in zip(slots, weights):
            acc = acc + got[slot, :, 0 : HEADS * VAL].astype(f32) * w
        own = mine[:, n * 64 : (n + 1) * 64]
        twin = theirs[:, n * 64 : (n + 1) * 64]
        pool = jnp.concatenate(
            [jnp.where(c == 0, own, twin), jnp.where(c == 0, twin, own)], axis=0
        )
        inputs.append(jnp.concatenate([(acc / total).astype(bf16), pool], axis=1))
    for copy in copies:
        copy.wait()
    for col in range(0, WIDTH, 512):
        cols = slice(col, col + 512)
        result = nn(inputs[0], wbuf[0, :, cols])
        for n in range(1, NY):
            result = result + nn(inputs[n], wbuf[n, :, cols])
        first, second = result[0:ROWS], result[ROWS:]
        keep[:, cols] = jnp.where(c == 0, first, second)
        send[:, cols] = jnp.where(c == 0, second, first).astype(bf16)


def project(got, mine, theirs, weights):
    return pl.pallas_call(
        project_body,
        in_specs=[vmem()] * 3 + [pl.BlockSpec(memory_space=pl.ANY)] * 8,
        out_specs=(vmem(), vmem()),
        out_shape=(
            pltpu.VMEM((ROWS, WIDTH), f32),
            pltpu.VMEM((ROWS, WIDTH), bf16),
        ),
        scratch_shapes=[
            pltpu.VMEM((NY, 256, WIDTH), bf16),
            pltpu.SemaphoreType.DMA((8,)),
        ],
        compiler_params=params(40),
        name="project",
    )(near(got), near(mine), near(theirs), *weights)


def across(x):
    return lax.ppermute(x, "c", [(0, 1), (1, 0)])


def shifted(x, axis, places):
    count = lax.axis_size(axis)
    return lax.ppermute(x, axis, [(i, (i + places) % count) for i in range(count)])


def shards(
    tokens,
    norm_gain,
    query_down_weight,
    query_latent_norm_gain,
    key_value_down_weight,
    key_value_latent_gain,
    w_rope_key,
    w_pool_in,
    query_up_weight,
    key_value_up_weight,
    query_gain,
    key_gain,
    w_pool_mix,
    pool_scale,
    w_out_attn,
    w_out_pool,
):
    wqt = query_up_weight.T
    wkvt = key_value_up_weight.T

    q_all, kv_all, pool_in = latents(
        tokens,
        norm_gain,
        query_down_weight,
        query_latent_norm_gain,
        key_value_down_weight,
        key_value_latent_gain,
        w_rope_key,
        w_pool_in,
    )
    pieces = [q_all] + [shifted(q_all, "y", k) for k in range(1, NY)]
    kv_own = lax.all_to_all(kv_all, "z", 0, 0, tiled=True).reshape(NZ * (ROWS + 8), KR)

    count = NZ * NX * NY * 2
    every = ("z", "x", "y", "c")
    low = lax.ppermute(
        pool_in[ROWS - 8 :], every, [(i, i + 1) for i in range(count - 1)]
    )
    high = lax.ppermute(pool_in[:8], every, [(i + 1, i) for i in range(count - 1)])
    pool_mine, pool_send = pooling(pool_in, low, high)
    pool_theirs = across(pool_send)

    folded = jnp.dot(
        w_pool_mix[0],
        (pool_scale.astype(f32)[:, None] * w_out_pool.astype(f32)).astype(bf16),
        preferred_element_type=f32,
    ).astype(bf16)
    upper = w_out_attn[:128]
    lower = jnp.concatenate([w_out_attn[128:], folded], axis=0)
    upper1 = shifted(upper, "y", 1)
    lower3 = shifted(lower, "y", NY - 1)
    lower1 = shifted(lower, "y", 1)
    upper3 = shifted(upper, "y", NY - 1)
    upper2 = shifted(upper1, "y", 1)
    lower2 = shifted(lower3, "y", NY - 1)
    pieces_w = (upper, lower, upper1, lower1, upper3, lower3, upper2, lower2)

    kv = lax.all_to_all(
        jnp.broadcast_to(kv_own[None], (NY, *kv_own.shape)), "y", 0, 0, tiled=True
    )
    q_side = jnp.concatenate(pieces, axis=0)
    q_own = [q_side] + [shifted(q_side, "x", k) for k in range(1, NX)]
    q_twin = [across(q) for q in q_own]
    kv_twin = across(kv)
    qt = queries(wkvt, q_own, q_twin, wqt, query_gain, query_tables())
    pair = keys_values((), kv, kv_twin, wkvt, key_gain, key_tables())
    message, *logs = attend(*pair, qt)

    got = lax.all_to_all(message, ("x", "y"), 0, 0, tiled=True)
    logs = [logs[0]] + [shifted(logs[k], "x", k) for k in range(1, NX)]
    row_logsum = logsums(logs)
    keep, send = project(got, pool_mine, pool_theirs, pieces_w)
    received = across(send)
    mixed = (keep + received.astype(f32)).astype(bf16)
    return mixed, row_logsum


def solution(mesh):
    fine = Mesh(mesh.devices.reshape(NZ, NX, NY, 2), ("z", "x", "y", "c"))
    tp = ("y", "c")
    placed = (
        P(("z", "x", "y", "c"), None),
        P(),
        P(),
        P(),
        P(),
        P(),
        P(),
        P(),
        P(None, tp),
        P(None, tp),
        P(),
        P(),
        P(tp, None, None),
        P(tp),
        P(tp, None),
        P(tp, None),
    )

    return jax.shard_map(
        shards,
        mesh=fine,
        in_specs=placed,
        out_specs=(P(("z", "x", "y", "c"), None), P(tp, ("z", "x"))),
        check_vma=False,
    )
```

```python
import jax
import jax.numpy as jnp
import numpy as np
from jax import lax
from jax.experimental import pallas as pl
from jax.experimental.pallas import tpu as pltpu
from jax.sharding import Mesh, PartitionSpec as P

NOPE = 64
ROT = 32
HALF = 16
HEAD = 96
VAL = 64
HEADS = 3
QR = 512
KR = 256
EPS = 1e-06
WIDTH = 2048
ROWS = 48
BLOCK = 384
TOKENS = 12288
LOG2E = 1.4426950408889634
LN2 = 0.6931471805599453
MSG = 256
VROWS = 80
QTILE = 512
NX = 4
NY = 4
NZ = 8
NQ = NX * BLOCK

bf16 = jnp.bfloat16
f32 = jnp.float32


def trig_tables(inner_places, outer_step, outer_count):
    freqs = 10000.0 ** (-np.arange(HALF, dtype=np.float64) / HALF)
    inner = freqs[:, None] * inner_places[None, :]
    outer = freqs[:, None] * (outer_step * np.arange(outer_count, dtype=np.float64))[None, :]
    pad = np.zeros((HALF, 128 - outer_count))
    cast = lambda a: a.astype(np.float32)
    parts = [np.cos(inner), np.sin(inner), np.cos(outer), pad, np.sin(outer), pad]
    return cast(np.concatenate(parts, 1))


def query_tables():
    return trig_tables(np.arange(BLOCK, dtype=np.float64), BLOCK, NZ * NX)


def key_tables():
    z = np.arange(NZ, dtype=np.float64)
    places = (NX * BLOCK * z[:, None] + np.arange(ROWS, dtype=np.float64)[None, :]).reshape(-1)
    return trig_tables(places, ROWS, NX * NY * 2)


def near(x):
    return pltpu.with_memory_space_constraint(x, pltpu.VMEM)


def vmem():
    return pl.BlockSpec(memory_space=pltpu.VMEM)


def nt(a, b):
    return lax.dot_general(a, b, (((1,), (1,)), ((), ())), preferred_element_type=f32)


def nn(a, b):
    return lax.dot_general(a, b, (((1,), (0,)), ((), ())), preferred_element_type=f32)


def params(limit=56, **kw):
    return pltpu.CompilerParams(vmem_limit_bytes=limit * 1024 * 1024, **kw)


KSTEP = 1024


def latents_body(
    tok, gain, qdw, qg, kdw, kg, rw, pw, q_out, kv_out, pool_out, inv, aq, ak, ar, ap
):
    k = pl.program_id(0)

    @pl.when(k == 0)
    def _():
        x = tok[...].astype(f32)
        inv[...] = jnp.broadcast_to(
            lax.rsqrt(jnp.mean(x * x, axis=-1, keepdims=True) + EPS), (ROWS, 128)
        )
        aq[...] = jnp.zeros_like(aq)
        ak[...] = jnp.zeros_like(ak)
        ar[...] = jnp.zeros_like(ar)
        ap[...] = jnp.zeros_like(ap)

    cols = pl.ds(pl.multiple_of(k * KSTEP, KSTEP), KSTEP)
    x = tok[:, cols].astype(f32)
    normed = (x * inv[:, 0:1] * gain[cols].astype(f32).reshape(1, KSTEP)).astype(bf16)
    aq[...] += nn(normed, qdw[...])
    ak[...] += nn(normed, kdw[...])
    ar[...] += nt(normed, rw[...])
    ap[...] += nn(normed, pw[...])

    @pl.when(k == pl.num_programs(0) - 1)
    def _():
        def norm(v, g):
            return (
                v
                * lax.rsqrt(jnp.mean(v * v, axis=-1, keepdims=True) + EPS)
                * g.astype(f32).reshape(1, -1)
            ).astype(bf16)

        q = norm(aq[...], qg[...])
        kv = norm(ak[...], kg[...])
        groups = [ar[8 * g : 8 * g + 8, :] for g in range(ROWS // 8)]
        groups.append(jnp.zeros((8, KR - ROT * (ROWS // 8)), f32))
        rope = jnp.concatenate(groups, axis=1).astype(bf16)
        q_out[...] = q
        pool_out[...] = ap[...].astype(bf16)
        for n in range(NZ):
            kv_out[n, 0:ROWS, :] = kv
            kv_out[n, ROWS:, :] = rope


def latents(tok, gain, qdw, qg, kdw, kg, rw, pw):
    steps = WIDTH // KSTEP
    whole = lambda *s: pl.BlockSpec(s, lambda k: (0,) * len(s))
    part = lambda n: pl.BlockSpec((KSTEP, n), lambda k: (k, 0))
    return pl.pallas_call(
        latents_body,
        grid=(steps,),
        in_specs=[
            whole(ROWS, WIDTH),
            whole(WIDTH),
            part(QR),
            whole(QR),
            part(KR),
            whole(KR),
            pl.BlockSpec((ROT, KSTEP), lambda k: (0, k)),
            part(512),
        ],
        out_specs=(
            whole(ROWS, QR),
            whole(NZ, ROWS + 8, KR),
            whole(ROWS, 512),
        ),
        out_shape=(
            jax.ShapeDtypeStruct((ROWS, QR), bf16),
            jax.ShapeDtypeStruct((NZ, ROWS + 8, KR), bf16),
            jax.ShapeDtypeStruct((ROWS, 512), bf16),
        ),
        scratch_shapes=[
            pltpu.VMEM((ROWS, 128), f32),
            pltpu.VMEM((ROWS, QR), f32),
            pltpu.VMEM((ROWS, KR), f32),
            pltpu.VMEM((ROWS, ROT), f32),
            pltpu.VMEM((ROWS, 512), f32),
        ],
        compiler_params=params(dimension_semantics=("arbitrary",)),
        name="latents",
    )(tok, gain, qdw, qg, kdw, kg, rw.T, pw)


def angles(table, idx):
    lanes = lax.broadcasted_iota(jnp.int32, (HALF, 128), 1)
    hit = lanes == idx
    coff = table[:, 0:BLOCK]
    soff = table[:, BLOCK : 2 * BLOCK]
    cb = table[:, 2 * BLOCK : 2 * BLOCK + 128]
    sb = table[:, 2 * BLOCK + 128 :]
    cbase = jnp.sum(jnp.where(hit, cb, 0.0), axis=1, keepdims=True)
    sbase = jnp.sum(jnp.where(hit, sb, 0.0), axis=1, keepdims=True)
    return cbase * coff - sbase * soff, sbase * coff + cbase * soff


def column(gain):
    row = jnp.broadcast_to(gain[...].astype(f32).reshape(1, HEAD), (8, HEAD)).astype(bf16)
    eye = (
        lax.broadcasted_iota(jnp.int32, (HEAD, HEAD), 0)
        == lax.broadcasted_iota(jnp.int32, (HEAD, HEAD), 1)
    ).astype(bf16)
    return nt(eye, row)[:, 0:1]


def rotated(v, cosine, sine):
    a = v[NOPE : NOPE + HALF]
    b = v[NOPE + HALF :]
    return jnp.concatenate(
        [v[:NOPE], a * cosine - b * sine, a * sine + b * cosine, jnp.zeros_like(v[:ROT])],
        axis=0,
    )


def queries_body(
    early, own0, own1, own2, own3, two0, two1, two2, two3, wqt, gain, table, out, lat
):
    c = lax.axis_index("c")
    z = lax.axis_index("z")
    here = lax.axis_index("x")
    qgain = column(gain)
    own = (own0, own1, own2, own3)
    other = (two0, two1, two2, two3)
    y = lax.axis_index("y")
    for x in range(NX):
        for k in range(NY):
            piece = slice(k * ROWS, (k + 1) * ROWS)
            at = ((y + NY - k) % NY) * 2 * ROWS
            first = pl.multiple_of(at + c * ROWS, ROWS)
            lat[x, pl.ds(first, ROWS), :] = own[x][piece]
            second = pl.multiple_of(at + (1 - c) * ROWS, ROWS)
            lat[x, pl.ds(second, ROWS), :] = other[x][piece]
        q = nt(wqt[...], lat[x])
        block = (here + NX - x) % NX
        place = z * NX + block
        cosine, sine = angles(table, place)
        at = pl.multiple_of(block * BLOCK, BLOCK)
        for h in range(HEADS):
            v = q[h * HEAD : (h + 1) * HEAD]
            inv = lax.rsqrt(jnp.mean(v * v, axis=0, keepdims=True) + EPS)
            v = v * inv * qgain
            v = rotated(v, cosine, sine) * (LOG2E * HEAD**-0.5)
            out[h, :, pl.ds(at, BLOCK)] = v.astype(bf16)


def queries(early, own, other, wqt, qgain, table):
    return pl.pallas_call(
        queries_body,
        in_specs=[pl.BlockSpec(memory_space=pl.ANY)] + [vmem()] * 11,
        out_specs=vmem(),
        out_shape=pltpu.VMEM((HEADS, 128, NQ), bf16),
        scratch_shapes=[pltpu.VMEM((NX, BLOCK, QR), bf16)],
        compiler_params=params(),
        name="queries",
    )(early, *own, *other, wqt, qgain, table)


def keys_body(count, *refs):
    own, other, wkvt, gain, table, kbuf, vbuf = refs[count:]
    c = lax.axis_index("c")
    x = lax.axis_index("x")
    kgain = column(gain)
    pick = (
        lax.broadcasted_iota(jnp.int32, (ROT, KR), 0)
        == lax.broadcasted_iota(jnp.int32, (ROT, KR), 1) % ROT
    ).astype(bf16)
    group = lax.broadcasted_iota(jnp.int32, (8, KR), 1) // ROT
    ones = (lax.broadcasted_iota(jnp.int32, (VROWS - VAL, BLOCK), 0) == 0).astype(bf16)
    blocks = [(own, k, k, c) for k in range(NY)] + [(other, k, k, 1 - c) for k in range(NY)]
    for b, (ref, at, y_from, c_from) in enumerate(blocks):
        lat, spread = [], []
        for z in range(NZ):
            row = z * (ROWS + 8)
            lat.append(ref[at, row : row + ROWS, :])
            packed = ref[at, row + ROWS : row + ROWS + 8, :].astype(f32)
            spread += [jnp.where(group == g, packed, 0.0) for g in range(ROWS // 8)]
        kv = nt(wkvt[...], jnp.concatenate(lat, axis=0))
        rope = nt(pick, jnp.concatenate(spread, axis=0).astype(bf16))
        rope_square = jnp.sum(rope * rope, axis=0, keepdims=True)
        place = (x * NY + y_from) * 2 + c_from
        cosine, sine = angles(table, place)
        cols = slice(b * BLOCK, (b + 1) * BLOCK)
        for h in range(HEADS):
            plain = kv[h * 128 : h * 128 + NOPE]
            total = jnp.sum(plain * plain, axis=0, keepdims=True) + rope_square
            inv = lax.rsqrt(total * (1.0 / HEAD) + EPS)
            k = jnp.concatenate([plain, rope], axis=0) * inv * kgain
            k = rotated(k, cosine, sine).astype(bf16)
            kbuf[h, cols, :] = k.T
            vbuf[h, 0:VAL, cols] = kv[h * 128 + NOPE : (h + 1) * 128].astype(bf16)
            vbuf[h, VAL:, cols] = ones


def keys_values(after, own, other, wkvt, kgain, table):
    count = 2 * NY * BLOCK

    def body(*refs):
        keys_body(len(after), *refs)

    return pl.pallas_call(
        body,
        in_specs=[pl.BlockSpec(memory_space=pl.ANY)] * len(after) + [vmem()] * 5,
        out_specs=(vmem(), vmem()),
        out_shape=(
            pltpu.VMEM((HEADS, count, 128), bf16),
            pltpu.VMEM((HEADS, VROWS, count), bf16),
        ),
        compiler_params=params(),
        name="keys",
    )(*after, own, other, wkvt, kgain, table)


CHUNK = 256
SUB = 256
TILES = HEADS * (NQ // QTILE)


def attend_body(
    kbuf, vbuf, qt, out, l0, l1, l2, l3, buf0, buf1, acc_s, m_s, logs, msg, sems
):
    bufs = (buf0, buf1)
    pairs = [(kbuf, vbuf)]
    sizes = [kbuf.shape[1]]
    chunks = []
    base = 0
    for (kr, vr), n in zip(pairs, sizes):
        for at in range(0, n, CHUNK):
            size = min(CHUNK, n - at)
            chunks.append((base + at, size, kr, vr, at))
        base += n

    def where(i):
        per = NQ // QTILE
        return i // per, pl.ds(pl.multiple_of((i % per) * QTILE, QTILE), QTILE)

    def score(i, chunk, buf, top):
        row, size, kr, _, at = chunk
        h, col = where(i)
        for sub in range(0, size, SUB):
            s = nn(kr[h, at + sub : at + sub + SUB, :], qt[h, :, col])
            buf[row + sub : row + sub + SUB, :] = s
            top = jnp.maximum(top, jnp.max(s.reshape(SUB // 8, 8, QTILE), axis=0))
        return top

    def weigh(i, chunk, buf, m):
        row, size, _, vr, at = chunk
        h, _ = where(i)
        p = jnp.exp2(buf[row : row + size, :] - m).astype(bf16)
        return nn(vr[h, :, at : at + size], p)

    low = jnp.full((8, QTILE), -1e30, f32)

    def settle(top):
        return jnp.max(top, axis=0, keepdims=True)

    def finish(i, m, acc):
        h, col = where(i)
        acc_s[h, :, col] = acc
        m_s[h, :, col] = m

    def both(i, m, buf, nxt):
        acc = None
        top = low
        for chunk in chunks:
            top = score(i + 1, chunk, nxt, top)
            part = weigh(i, chunk, buf, m)
            acc = part if acc is None else acc + part
        finish(i, m, acc)
        return settle(top)

    top = low
    for chunk in chunks:
        top = score(0, chunk, bufs[0], top)
    m = settle(top)

    def pair(j, m):
        m = both(2 * j, m, bufs[0], bufs[1])
        return both(2 * j + 1, m, bufs[1], bufs[0])

    m = lax.fori_loop(0, (TILES - 1) // 2, pair, m)
    acc = None
    for chunk in chunks:
        part = weigh(TILES - 1, chunk, bufs[0], m)
        acc = part if acc is None else acc + part
    finish(TILES - 1, m, acc)

    for x in range(NX):
        cols = slice(x * BLOCK, (x + 1) * BLOCK)
        parts = []
        stats = []
        for h in range(HEADS):
            total = acc_s[h, VAL : VAL + 1, cols]
            parts.append((acc_s[h, 0:VAL, cols] * (1.0 / total)).astype(bf16))
            lse = (m_s[h, :, cols] + jnp.log2(total)) * LN2
            logs[x, h : h + 1, :] = lse
            hi = lse.astype(bf16)
            rest = lse - hi.astype(f32)
            mid = rest.astype(bf16)
            low_part = (rest - mid.astype(f32)).astype(bf16)
            stats += [hi.astype(f32), mid.astype(f32), low_part.astype(f32)]
        stats.append(jnp.zeros((MSG - HEADS * VAL - 9, BLOCK), f32))
        parts.append(jnp.concatenate(stats, axis=0).astype(bf16))
        rows = jnp.concatenate(parts, axis=0).T
        for y in range(NY):
            msg[x * NY + y, :, :] = rows[y * 2 * ROWS : (y + 1) * 2 * ROWS]
        pltpu.make_async_copy(
            msg.at[x * NY : (x + 1) * NY], out.at[x * NY : (x + 1) * NY], sems.at[x]
        ).start()
    here = lax.axis_index("x")
    for k, ref in enumerate((l0, l1, l2, l3)):
        ref[...] = logs[(here + k) % NX]
    for x in range(NX):
        pltpu.make_async_copy(
            msg.at[x * NY : (x + 1) * NY], out.at[x * NY : (x + 1) * NY], sems.at[x]
        ).wait()


def attend(kbuf, vbuf, qt):
    return pl.pallas_call(
        attend_body,
        in_specs=[vmem()] * 3,
        out_specs=(pl.BlockSpec(memory_space=pltpu.MemorySpace.HBM), *[vmem()] * 4),
        out_shape=(
            jax.ShapeDtypeStruct((NX * NY, 2 * ROWS, MSG), bf16),
            *[jax.ShapeDtypeStruct((8, BLOCK), f32)] * NX,
        ),
        scratch_shapes=[
            pltpu.VMEM((kbuf.shape[1], QTILE), f32),
            pltpu.VMEM((kbuf.shape[1], QTILE), f32),
            pltpu.VMEM((HEADS, VROWS, NQ), f32),
            pltpu.VMEM((HEADS, 1, NQ), f32),
            pltpu.VMEM((NX, 8, BLOCK), f32),
            pltpu.VMEM((NX * NY, 2 * ROWS, MSG), bf16),
            pltpu.SemaphoreType.DMA((NX,)),
        ],
        compiler_params=params(56),
        name="attend",
    )(near(kbuf), near(vbuf), near(qt))


def logsum_body(a, b, c, d, out):
    logs = [r[0:HEADS, :] for r in (a, b, c, d)]
    top = jnp.maximum(jnp.maximum(logs[0], logs[1]), jnp.maximum(logs[2], logs[3]))
    total = sum(jnp.exp(v - top) for v in logs)
    out[...] = top + jnp.log(total)


def logsums(parts):
    return pl.pallas_call(
        logsum_body,
        in_specs=[vmem()] * NX,
        out_specs=vmem(),
        out_shape=jax.ShapeDtypeStruct((HEADS, BLOCK), f32),
        compiler_params=params(),
        name="logsums",
    )(*parts)


PLACES = (0, -1, 1, 2)


def pool_body(own, low, high, keep, send, buf):
    z, here, y0, c = [lax.axis_index(n) for n in "zxyc"]
    first = ((z * NX + here) * NY * 2 + y0 * 2 + c) * ROWS
    x = own[...].astype(f32)
    side = jnp.zeros((8, 512), f32)
    window = jnp.concatenate(
        [side, low[...].astype(f32), x, high[...].astype(f32), side], axis=0
    )
    n = ROWS + 32
    s1 = window[0 : n - 1] + window[1:n]
    s2 = s1[0 : n - 3] + s1[2 : n - 1]
    s4 = s2[0 : n - 7] + s2[4 : n - 3]
    s8 = s4[0 : n - 15] + s4[8 : n - 7]
    w1 = s1[15 : 15 + ROWS]
    w2 = s2[14 : 14 + ROWS]
    w4 = s4[12 : 12 + ROWS]
    w8 = s8[8 : 8 + ROWS]
    group = (lax.broadcasted_iota(jnp.int32, (ROWS, 512), 1) // 64) % 4
    total = jnp.where(
        group == 0, w1, jnp.where(group == 1, w2, jnp.where(group == 2, w4, w8))
    )
    half = jnp.where(group == 0, 1, jnp.where(group == 1, 2, jnp.where(group == 2, 4, 8)))
    place = first + lax.broadcasted_iota(jnp.int32, (ROWS, 512), 0)
    count = (jnp.minimum(place + half, TOKENS) - jnp.maximum(place - half, 0)).astype(f32)
    buf[...] = (total / count - x).astype(bf16)
    even, odd = [], []
    for d in PLACES:
        at = pl.multiple_of(((y0 + NY + d) % NY) * 128, 128)
        tile = buf[:, pl.ds(at, 128)]
        even.append(tile[:, 0:64])
        odd.append(tile[:, 64:128])
    even = jnp.concatenate(even, axis=1)
    odd = jnp.concatenate(odd, axis=1)
    keep[...] = jnp.where(c == 0, even, odd)
    send[...] = jnp.where(c == 0, odd, even)


def pooling(own, low, high):
    return pl.pallas_call(
        pool_body,
        in_specs=[vmem()] * 3,
        out_specs=(vmem(), vmem()),
        out_shape=(
            jax.ShapeDtypeStruct((ROWS, 256), bf16),
            jax.ShapeDtypeStruct((ROWS, 256), bf16),
        ),
        scratch_shapes=[pltpu.VMEM((ROWS, 512), bf16)],
        compiler_params=params(),
        name="pooling",
    )(own, low, high)


def project_body(got, mine, theirs, *refs):
    upper, lower, upper1, lower3, onward, backward, keep, send, wbuf, sems = refs
    y0 = lax.axis_index("y")
    c = lax.axis_index("c")
    copies = []
    moves = (
        (upper, 0, 0),
        (lower, 0, 1),
        (upper1, 1, 0),
        (onward.at[0:128], 1, 1),
        (backward.at[0:128], 2, 0),
        (lower3, 2, 1),
        (onward.at[128:256], 3, 0),
        (backward.at[128:256], 3, 1),
    )
    for n, (ref, slot, part) in enumerate(moves):
        at = 128 * part
        copies.append(
            pltpu.make_async_copy(ref, wbuf.at[slot, at : at + 128], sems.at[n])
        )
    for copy in copies:
        copy.start()
    row = lax.broadcasted_iota(jnp.int32, (128, HEADS * VAL), 0)
    head = lax.broadcasted_iota(jnp.int32, (128, HEADS * VAL), 1) // VAL
    spread = ((row >= 64 + 3 * head) & (row < 67 + 3 * head)).astype(bf16)
    inputs = []
    for n, d in enumerate(PLACES):
        slots = [x * NY + (y0 + NY + d) % NY for x in range(NX)]
        logs = [nn(got[slot, :, 128:256], spread) for slot in slots]
        top = jnp.maximum(jnp.maximum(logs[0], logs[1]), jnp.maximum(logs[2], logs[3]))
        weights = [jnp.exp(v - top) for v in logs]
        total = weights[0] + weights[1] + weights[2] + weights[3]
        acc = jnp.zeros((2 * ROWS, HEADS * VAL), f32)
        for slot, w in zip(slots, weights):
            acc = acc + got[slot, :, 0 : HEADS * VAL].astype(f32) * w
        own = mine[:, n * 64 : (n + 1) * 64]
        twin = theirs[:, n * 64 : (n + 1) * 64]
        pool = jnp.concatenate(
            [jnp.where(c == 0, own, twin), jnp.where(c == 0, twin, own)], axis=0
        )
        inputs.append(jnp.concatenate([(acc / total).astype(bf16), pool], axis=1))
    for copy in copies:
        copy.wait()
    for col in range(0, WIDTH, 512):
        cols = slice(col, col + 512)
        result = nn(inputs[0], wbuf[0, :, cols])
        for n in range(1, NY):
            result = result + nn(inputs[n], wbuf[n, :, cols])
        first, second = result[0:ROWS], result[ROWS:]
        keep[:, cols] = jnp.where(c == 0, first, second)
        send[:, cols] = jnp.where(c == 0, second, first).astype(bf16)


def project(got, mine, theirs, weights):
    return pl.pallas_call(
        project_body,
        in_specs=[vmem()] * 3 + [pl.BlockSpec(memory_space=pl.ANY)] * 6,
        out_specs=(vmem(), vmem()),
        out_shape=(
            pltpu.VMEM((ROWS, WIDTH), f32),
            pltpu.VMEM((ROWS, WIDTH), bf16),
        ),
        scratch_shapes=[
            pltpu.VMEM((NY, 256, WIDTH), bf16),
            pltpu.SemaphoreType.DMA((8,)),
        ],
        compiler_params=params(40),
        name="project",
    )(near(got), mine, near(theirs), *weights)


def across(x):
    return lax.ppermute(x, "c", [(0, 1), (1, 0)])


def shifted(x, axis, places):
    count = lax.axis_size(axis)
    return lax.ppermute(x, axis, [(i, (i + places) % count) for i in range(count)])


def shards(
    tokens,
    norm_gain,
    query_down_weight,
    query_latent_norm_gain,
    key_value_down_weight,
    key_value_latent_gain,
    w_rope_key,
    w_pool_in,
    query_up_weight,
    key_value_up_weight,
    query_gain,
    key_gain,
    w_pool_mix,
    pool_scale,
    w_out_attn,
    w_out_pool,
):
    wqt = query_up_weight.T
    wkvt = key_value_up_weight.T

    q_all, kv_all, pool_in = latents(
        tokens,
        norm_gain,
        query_down_weight,
        query_latent_norm_gain,
        key_value_down_weight,
        key_value_latent_gain,
        w_rope_key,
        w_pool_in,
    )
    pieces = [q_all] + [shifted(q_all, "y", k) for k in range(1, NY)]
    kv_own = lax.all_to_all(kv_all, "z", 0, 0, tiled=True).reshape(NZ * (ROWS + 8), KR)

    count = NZ * NX * NY * 2
    every = ("z", "x", "y", "c")
    low = lax.ppermute(
        pool_in[ROWS - 8 :], every, [(i, i + 1) for i in range(count - 1)]
    )
    high = lax.ppermute(pool_in[:8], every, [(i + 1, i) for i in range(count - 1)])
    pool_mine, pool_send = pooling(pool_in, low, high)
    pool_theirs = across(pool_send)

    folded = jnp.dot(
        w_pool_mix[0],
        (pool_scale.astype(f32)[:, None] * w_out_pool.astype(f32)).astype(bf16),
        preferred_element_type=f32,
    ).astype(bf16)
    upper = w_out_attn[:128]
    lower = jnp.concatenate([w_out_attn[128:], folded], axis=0)
    upper1 = shifted(upper, "y", 1)
    lower3 = shifted(lower, "y", NY - 1)
    onward = jnp.concatenate([lower, upper1], axis=0)
    backward = jnp.concatenate([upper, lower3], axis=0)
    onward = shifted(onward, "y", 1)
    backward = shifted(backward, "y", NY - 1)
    pieces_w = (upper, lower, upper1, lower3, onward, backward)

    kv = lax.all_to_all(
        jnp.broadcast_to(kv_own[None], (NY, *kv_own.shape)), "y", 0, 0, tiled=True
    )
    q_side = jnp.concatenate(pieces, axis=0)
    q_own = [q_side] + [shifted(q_side, "x", k) for k in range(1, NX)]
    q_twin = [across(q) for q in q_own]
    kv_twin = across(kv)
    qt = queries(wkvt, q_own, q_twin, wqt, query_gain, query_tables())
    pair = keys_values((), kv, kv_twin, wkvt, key_gain, key_tables())
    message, *logs = attend(*pair, qt)

    got = lax.all_to_all(message, ("x", "y"), 0, 0, tiled=True)
    logs = [logs[0]] + [shifted(logs[k], "x", k) for k in range(1, NX)]
    row_logsum = logsums(logs)
    keep, send = project(got, pool_mine, pool_theirs, pieces_w)
    received = across(send)
    mixed = (keep + received.astype(f32)).astype(bf16)
    return mixed, row_logsum


def solution(mesh):
    fine = Mesh(mesh.devices.reshape(NZ, NX, NY, 2), ("z", "x", "y", "c"))
    tp = ("y", "c")
    placed = (
        P(("z", "x", "y", "c"), None),
        P(),
        P(),
        P(),
        P(),
        P(),
        P(),
        P(),
        P(None, tp),
        P(None, tp),
        P(),
        P(),
        P(tp, None, None),
        P(tp),
        P(tp, None),
        P(tp, None),
    )

    return jax.shard_map(
        shards,
        mesh=fine,
        in_specs=placed,
        out_specs=(P(("z", "x", "y", "c"), None), P(tp, ("z", "x"))),
        check_vma=False,
    )
```

```python
import jax
import jax.numpy as jnp
import numpy as np
from jax import lax
from jax.experimental import pallas as pl
from jax.experimental.pallas import tpu as pltpu
from jax.sharding import Mesh, PartitionSpec as P

NOPE = 64
ROT = 32
HALF = 16
HEAD = 96
VAL = 64
HEADS = 3
QR = 512
KR = 256
EPS = 1e-06
WIDTH = 2048
ROWS = 48
BLOCK = 384
TOKENS = 12288
LOG2E = 1.4426950408889634
LN2 = 0.6931471805599453
MSG = 256
VROWS = 80
QTILE = 512
NX = 4
NY = 4
NZ = 8
NQ = NX * BLOCK

bf16 = jnp.bfloat16
f32 = jnp.float32


def trig_tables(inner_places, outer_step, outer_count):
    freqs = 10000.0 ** (-np.arange(HALF, dtype=np.float64) / HALF)
    inner = freqs[:, None] * inner_places[None, :]
    outer = freqs[:, None] * (outer_step * np.arange(outer_count, dtype=np.float64))[None, :]
    pad = np.zeros((HALF, 128 - outer_count))
    cast = lambda a: a.astype(np.float32)
    parts = [np.cos(inner), np.sin(inner), np.cos(outer), pad, np.sin(outer), pad]
    return cast(np.concatenate(parts, 1))


def query_tables():
    return trig_tables(np.arange(BLOCK, dtype=np.float64), BLOCK, NZ * NX)


def key_tables():
    z = np.arange(NZ, dtype=np.float64)
    places = (NX * BLOCK * z[:, None] + np.arange(ROWS, dtype=np.float64)[None, :]).reshape(-1)
    return trig_tables(places, ROWS, NX * NY * 2)


def near(x):
    return pltpu.with_memory_space_constraint(x, pltpu.VMEM)


def vmem():
    return pl.BlockSpec(memory_space=pltpu.VMEM)


def nt(a, b):
    return lax.dot_general(a, b, (((1,), (1,)), ((), ())), preferred_element_type=f32)


def nn(a, b):
    return lax.dot_general(a, b, (((1,), (0,)), ((), ())), preferred_element_type=f32)


def params(limit=56, **kw):
    return pltpu.CompilerParams(vmem_limit_bytes=limit * 1024 * 1024, **kw)


KSTEP = 1024


def latents_body(
    tok, gain, qdw, qg, kdw, kg, rw, pw, q_out, kv_out, pool_out, inv, aq, ak, ar, ap
):
    k = pl.program_id(0)

    @pl.when(k == 0)
    def _():
        x = tok[...].astype(f32)
        inv[...] = jnp.broadcast_to(
            lax.rsqrt(jnp.mean(x * x, axis=-1, keepdims=True) + EPS), (ROWS, 128)
        )
        aq[...] = jnp.zeros_like(aq)
        ak[...] = jnp.zeros_like(ak)
        ar[...] = jnp.zeros_like(ar)
        ap[...] = jnp.zeros_like(ap)

    cols = pl.ds(pl.multiple_of(k * KSTEP, KSTEP), KSTEP)
    x = tok[:, cols].astype(f32)
    normed = (x * inv[:, 0:1] * gain[cols].astype(f32).reshape(1, KSTEP)).astype(bf16)
    aq[...] += nn(normed, qdw[...])
    ak[...] += nn(normed, kdw[...])
    ar[...] += nt(normed, rw[...])
    ap[...] += nn(normed, pw[...])

    @pl.when(k == pl.num_programs(0) - 1)
    def _():
        def norm(v, g):
            return (
                v
                * lax.rsqrt(jnp.mean(v * v, axis=-1, keepdims=True) + EPS)
                * g.astype(f32).reshape(1, -1)
            ).astype(bf16)

        q = norm(aq[...], qg[...])
        kv = norm(ak[...], kg[...])
        groups = [ar[8 * g : 8 * g + 8, :] for g in range(ROWS // 8)]
        groups.append(jnp.zeros((8, KR - ROT * (ROWS // 8)), f32))
        rope = jnp.concatenate(groups, axis=1).astype(bf16)
        q_out[...] = q
        pool_out[...] = ap[...].astype(bf16)
        for n in range(NZ):
            kv_out[n, 0:ROWS, :] = kv
            kv_out[n, ROWS:, :] = rope


def latents(tok, gain, qdw, qg, kdw, kg, rw, pw):
    steps = WIDTH // KSTEP
    whole = lambda *s: pl.BlockSpec(s, lambda k: (0,) * len(s))
    part = lambda n: pl.BlockSpec((KSTEP, n), lambda k: (k, 0))
    return pl.pallas_call(
        latents_body,
        grid=(steps,),
        in_specs=[
            whole(ROWS, WIDTH),
            whole(WIDTH),
            part(QR),
            whole(QR),
            part(KR),
            whole(KR),
            pl.BlockSpec((ROT, KSTEP), lambda k: (0, k)),
            part(512),
        ],
        out_specs=(
            whole(ROWS, QR),
            whole(NZ, ROWS + 8, KR),
            whole(ROWS, 512),
        ),
        out_shape=(
            jax.ShapeDtypeStruct((ROWS, QR), bf16),
            jax.ShapeDtypeStruct((NZ, ROWS + 8, KR), bf16),
            jax.ShapeDtypeStruct((ROWS, 512), bf16),
        ),
        scratch_shapes=[
            pltpu.VMEM((ROWS, 128), f32),
            pltpu.VMEM((ROWS, QR), f32),
            pltpu.VMEM((ROWS, KR), f32),
            pltpu.VMEM((ROWS, ROT), f32),
            pltpu.VMEM((ROWS, 512), f32),
        ],
        compiler_params=params(dimension_semantics=("arbitrary",)),
        name="latents",
    )(tok, gain, qdw, qg, kdw, kg, rw.T, pw)


def angles(table, idx):
    lanes = lax.broadcasted_iota(jnp.int32, (HALF, 128), 1)
    hit = lanes == idx
    coff = table[:, 0:BLOCK]
    soff = table[:, BLOCK : 2 * BLOCK]
    cb = table[:, 2 * BLOCK : 2 * BLOCK + 128]
    sb = table[:, 2 * BLOCK + 128 :]
    cbase = jnp.sum(jnp.where(hit, cb, 0.0), axis=1, keepdims=True)
    sbase = jnp.sum(jnp.where(hit, sb, 0.0), axis=1, keepdims=True)
    return cbase * coff - sbase * soff, sbase * coff + cbase * soff


def column(gain):
    row = jnp.broadcast_to(gain[...].astype(f32).reshape(1, HEAD), (8, HEAD)).astype(bf16)
    eye = (
        lax.broadcasted_iota(jnp.int32, (HEAD, HEAD), 0)
        == lax.broadcasted_iota(jnp.int32, (HEAD, HEAD), 1)
    ).astype(bf16)
    return nt(eye, row)[:, 0:1]


def rotated(v, cosine, sine):
    a = v[NOPE : NOPE + HALF]
    b = v[NOPE + HALF :]
    return jnp.concatenate(
        [v[:NOPE], a * cosine - b * sine, a * sine + b * cosine, jnp.zeros_like(v[:ROT])],
        axis=0,
    )


def queries_body(
    early, own0, own1, own2, own3, two0, two1, two2, two3, wqt, gain, table, out, lat
):
    c = lax.axis_index("c")
    z = lax.axis_index("z")
    here = lax.axis_index("x")
    qgain = column(gain)
    own = (own0, own1, own2, own3)
    other = (two0, two1, two2, two3)
    y = lax.axis_index("y")
    for x in range(NX):
        for k in range(NY):
            piece = slice(k * ROWS, (k + 1) * ROWS)
            at = ((y + NY - k) % NY) * 2 * ROWS
            first = pl.multiple_of(at + c * ROWS, ROWS)
            lat[x, pl.ds(first, ROWS), :] = own[x][piece]
            second = pl.multiple_of(at + (1 - c) * ROWS, ROWS)
            lat[x, pl.ds(second, ROWS), :] = other[x][piece]
        q = nt(wqt[...], lat[x])
        block = (here + NX - x) % NX
        place = z * NX + block
        cosine, sine = angles(table, place)
        at = pl.multiple_of(block * BLOCK, BLOCK)
        for h in range(HEADS):
            v = q[h * HEAD : (h + 1) * HEAD]
            inv = lax.rsqrt(jnp.mean(v * v, axis=0, keepdims=True) + EPS)
            v = v * inv * qgain
            v = rotated(v, cosine, sine) * (LOG2E * HEAD**-0.5)
            out[h, :, pl.ds(at, BLOCK)] = v.astype(bf16)


def queries(early, own, other, wqt, qgain, table):
    return pl.pallas_call(
        queries_body,
        in_specs=[pl.BlockSpec(memory_space=pl.ANY)] + [vmem()] * 11,
        out_specs=vmem(),
        out_shape=pltpu.VMEM((HEADS, 128, NQ), bf16),
        scratch_shapes=[pltpu.VMEM((NX, BLOCK, QR), bf16)],
        compiler_params=params(),
        name="queries",
    )(early, *own, *other, wqt, qgain, table)


def keys_body(count, *refs):
    own, other, wkv, gain, table, kbuf, vbuf = refs[count:]
    c = lax.axis_index("c")
    x = lax.axis_index("x")
    kgain = column(gain)
    pick = (
        lax.broadcasted_iota(jnp.int32, (ROT, KR), 0)
        == lax.broadcasted_iota(jnp.int32, (ROT, KR), 1) % ROT
    ).astype(bf16)
    group = lax.broadcasted_iota(jnp.int32, (8, KR), 1) // ROT
    wt = wkv[...].T
    ones = (lax.broadcasted_iota(jnp.int32, (VROWS - VAL, BLOCK), 0) == 0).astype(bf16)
    blocks = [(own, k, k, c) for k in range(NY)] + [(other, k, k, 1 - c) for k in range(NY)]
    for b, (ref, at, y_from, c_from) in enumerate(blocks):
        lat, spread = [], []
        for z in range(NZ):
            row = z * (ROWS + 8)
            lat.append(ref[at, row : row + ROWS, :])
            packed = ref[at, row + ROWS : row + ROWS + 8, :].astype(f32)
            spread += [jnp.where(group == g, packed, 0.0) for g in range(ROWS // 8)]
        kv = nt(wt, jnp.concatenate(lat, axis=0))
        rope = nt(pick, jnp.concatenate(spread, axis=0).astype(bf16))
        rope_square = jnp.sum(rope * rope, axis=0, keepdims=True)
        place = (x * NY + y_from) * 2 + c_from
        cosine, sine = angles(table, place)
        cols = slice(b * BLOCK, (b + 1) * BLOCK)
        for h in range(HEADS):
            plain = kv[h * 128 : h * 128 + NOPE]
            total = jnp.sum(plain * plain, axis=0, keepdims=True) + rope_square
            inv = lax.rsqrt(total * (1.0 / HEAD) + EPS)
            k = jnp.concatenate([plain, rope], axis=0) * inv * kgain
            k = rotated(k, cosine, sine).astype(bf16)
            kbuf[h, cols, :] = k.T
            vbuf[h, 0:VAL, cols] = kv[h * 128 + NOPE : (h + 1) * 128].astype(bf16)
            vbuf[h, VAL:, cols] = ones


def keys_values(after, own, other, wkvt, kgain, table):
    count = 2 * NY * BLOCK

    def body(*refs):
        keys_body(len(after), *refs)

    return pl.pallas_call(
        body,
        in_specs=[pl.BlockSpec(memory_space=pl.ANY)] * len(after) + [vmem()] * 5,
        out_specs=(vmem(), vmem()),
        out_shape=(
            pltpu.VMEM((HEADS, count, 128), bf16),
            pltpu.VMEM((HEADS, VROWS, count), bf16),
        ),
        compiler_params=params(),
        name="keys",
    )(*after, own, other, wkvt, kgain, table)


CHUNK = 256
SUB = 256
TILES = HEADS * (NQ // QTILE)


def attend_body(
    kbuf, vbuf, qt, out, l0, l1, l2, l3, buf0, buf1, acc_s, m_s, logs, msg, sems
):
    bufs = (buf0, buf1)
    pairs = [(kbuf, vbuf)]
    sizes = [kbuf.shape[1]]
    chunks = []
    base = 0
    for (kr, vr), n in zip(pairs, sizes):
        for at in range(0, n, CHUNK):
            size = min(CHUNK, n - at)
            chunks.append((base + at, size, kr, vr, at))
        base += n

    def where(i):
        per = NQ // QTILE
        return i // per, pl.ds(pl.multiple_of((i % per) * QTILE, QTILE), QTILE)

    def score(i, chunk, buf, top):
        row, size, kr, _, at = chunk
        h, col = where(i)
        for sub in range(0, size, SUB):
            s = nn(kr[h, at + sub : at + sub + SUB, :], qt[h, :, col])
            buf[row + sub : row + sub + SUB, :] = s
            top = jnp.maximum(top, jnp.max(s.reshape(SUB // 8, 8, QTILE), axis=0))
        return top

    def weigh(i, chunk, buf, m):
        row, size, _, vr, at = chunk
        h, _ = where(i)
        p = jnp.exp2(buf[row : row + size, :] - m).astype(bf16)
        return nn(vr[h, :, at : at + size], p)

    low = jnp.full((8, QTILE), -1e30, f32)

    def settle(top):
        return jnp.max(top, axis=0, keepdims=True)

    def finish(i, m, acc):
        h, col = where(i)
        acc_s[h, :, col] = acc
        m_s[h, :, col] = m

    def both(i, m, buf, nxt):
        acc = None
        top = low
        for chunk in chunks:
            top = score(i + 1, chunk, nxt, top)
            part = weigh(i, chunk, buf, m)
            acc = part if acc is None else acc + part
        finish(i, m, acc)
        return settle(top)

    top = low
    for chunk in chunks:
        top = score(0, chunk, bufs[0], top)
    m = settle(top)

    def pair(j, m):
        m = both(2 * j, m, bufs[0], bufs[1])
        return both(2 * j + 1, m, bufs[1], bufs[0])

    m = lax.fori_loop(0, (TILES - 1) // 2, pair, m)
    acc = None
    for chunk in chunks:
        part = weigh(TILES - 1, chunk, bufs[0], m)
        acc = part if acc is None else acc + part
    finish(TILES - 1, m, acc)

    for x in range(NX):
        cols = slice(x * BLOCK, (x + 1) * BLOCK)
        parts = []
        stats = []
        for h in range(HEADS):
            total = acc_s[h, VAL : VAL + 1, cols]
            parts.append((acc_s[h, 0:VAL, cols] * (1.0 / total)).astype(bf16))
            lse = (m_s[h, :, cols] + jnp.log2(total)) * LN2
            logs[x, h : h + 1, :] = lse
            hi = lse.astype(bf16)
            rest = lse - hi.astype(f32)
            mid = rest.astype(bf16)
            low_part = (rest - mid.astype(f32)).astype(bf16)
            stats += [hi.astype(f32), mid.astype(f32), low_part.astype(f32)]
        stats.append(jnp.zeros((MSG - HEADS * VAL - 9, BLOCK), f32))
        parts.append(jnp.concatenate(stats, axis=0).astype(bf16))
        rows = jnp.concatenate(parts, axis=0).T
        for y in range(NY):
            msg[x * NY + y, :, :] = rows[y * 2 * ROWS : (y + 1) * 2 * ROWS]
        pltpu.make_async_copy(
            msg.at[x * NY : (x + 1) * NY], out.at[x * NY : (x + 1) * NY], sems.at[x]
        ).start()
    here = lax.axis_index("x")
    for k, ref in enumerate((l0, l1, l2, l3)):
        ref[...] = logs[(here + k) % NX]
    for x in range(NX):
        pltpu.make_async_copy(
            msg.at[x * NY : (x + 1) * NY], out.at[x * NY : (x + 1) * NY], sems.at[x]
        ).wait()


def attend(kbuf, vbuf, qt):
    return pl.pallas_call(
        attend_body,
        in_specs=[vmem()] * 3,
        out_specs=(pl.BlockSpec(memory_space=pltpu.MemorySpace.HBM), *[vmem()] * 4),
        out_shape=(
            jax.ShapeDtypeStruct((NX * NY, 2 * ROWS, MSG), bf16),
            *[jax.ShapeDtypeStruct((8, BLOCK), f32)] * NX,
        ),
        scratch_shapes=[
            pltpu.VMEM((kbuf.shape[1], QTILE), f32),
            pltpu.VMEM((kbuf.shape[1], QTILE), f32),
            pltpu.VMEM((HEADS, VROWS, NQ), f32),
            pltpu.VMEM((HEADS, 1, NQ), f32),
            pltpu.VMEM((NX, 8, BLOCK), f32),
            pltpu.VMEM((NX * NY, 2 * ROWS, MSG), bf16),
            pltpu.SemaphoreType.DMA((NX,)),
        ],
        compiler_params=params(56),
        name="attend",
    )(near(kbuf), near(vbuf), near(qt))


def logsum_body(a, b, c, d, out):
    logs = [r[0:HEADS, :] for r in (a, b, c, d)]
    top = jnp.maximum(jnp.maximum(logs[0], logs[1]), jnp.maximum(logs[2], logs[3]))
    total = sum(jnp.exp(v - top) for v in logs)
    out[...] = top + jnp.log(total)


def logsums(parts):
    return pl.pallas_call(
        logsum_body,
        in_specs=[vmem()] * NX,
        out_specs=vmem(),
        out_shape=jax.ShapeDtypeStruct((HEADS, BLOCK), f32),
        compiler_params=params(),
        name="logsums",
    )(*parts)


PLACES = (0, -1, 1, 2)


def pool_body(own, low, high, keep, send, buf):
    z, here, y0, c = [lax.axis_index(n) for n in "zxyc"]
    first = ((z * NX + here) * NY * 2 + y0 * 2 + c) * ROWS
    x = own[...].astype(f32)
    side = jnp.zeros((8, 512), f32)
    window = jnp.concatenate(
        [side, low[...].astype(f32), x, high[...].astype(f32), side], axis=0
    )
    n = ROWS + 32
    s1 = window[0 : n - 1] + window[1:n]
    s2 = s1[0 : n - 3] + s1[2 : n - 1]
    s4 = s2[0 : n - 7] + s2[4 : n - 3]
    s8 = s4[0 : n - 15] + s4[8 : n - 7]
    w1 = s1[15 : 15 + ROWS]
    w2 = s2[14 : 14 + ROWS]
    w4 = s4[12 : 12 + ROWS]
    w8 = s8[8 : 8 + ROWS]
    group = (lax.broadcasted_iota(jnp.int32, (ROWS, 512), 1) // 64) % 4
    total = jnp.where(
        group == 0, w1, jnp.where(group == 1, w2, jnp.where(group == 2, w4, w8))
    )
    half = jnp.where(group == 0, 1, jnp.where(group == 1, 2, jnp.where(group == 2, 4, 8)))
    place = first + lax.broadcasted_iota(jnp.int32, (ROWS, 512), 0)
    count = (jnp.minimum(place + half, TOKENS) - jnp.maximum(place - half, 0)).astype(f32)
    buf[...] = (total / count - x).astype(bf16)
    even, odd = [], []
    for d in PLACES:
        at = pl.multiple_of(((y0 + NY + d) % NY) * 128, 128)
        tile = buf[:, pl.ds(at, 128)]
        even.append(tile[:, 0:64])
        odd.append(tile[:, 64:128])
    even = jnp.concatenate(even, axis=1)
    odd = jnp.concatenate(odd, axis=1)
    keep[...] = jnp.where(c == 0, even, odd)
    send[...] = jnp.where(c == 0, odd, even)


def pooling(own, low, high):
    return pl.pallas_call(
        pool_body,
        in_specs=[vmem()] * 3,
        out_specs=(vmem(), vmem()),
        out_shape=(
            pltpu.VMEM((ROWS, 256), bf16),
            jax.ShapeDtypeStruct((ROWS, 256), bf16),
        ),
        scratch_shapes=[pltpu.VMEM((ROWS, 512), bf16)],
        compiler_params=params(),
        name="pooling",
    )(own, low, high)


def project_body(got, mine, theirs, *refs):
    upper, lower, upper1, lower3, onward, backward, keep, send, wbuf, sems = refs
    y0 = lax.axis_index("y")
    c = lax.axis_index("c")
    copies = []
    moves = (
        (upper, 0, 0),
        (lower, 0, 1),
        (upper1, 1, 0),
        (onward.at[0:128], 1, 1),
        (backward.at[0:128], 2, 0),
        (lower3, 2, 1),
        (onward.at[128:256], 3, 0),
        (backward.at[128:256], 3, 1),
    )
    for n, (ref, slot, part) in enumerate(moves):
        at = 128 * part
        copies.append(
            pltpu.make_async_copy(ref, wbuf.at[slot, at : at + 128], sems.at[n])
        )
    for copy in copies:
        copy.start()
    row = lax.broadcasted_iota(jnp.int32, (128, HEADS * VAL), 0)
    head = lax.broadcasted_iota(jnp.int32, (128, HEADS * VAL), 1) // VAL
    spread = ((row >= 64 + 3 * head) & (row < 67 + 3 * head)).astype(bf16)
    inputs = []
    for n, d in enumerate(PLACES):
        slots = [x * NY + (y0 + NY + d) % NY for x in range(NX)]
        logs = [nn(got[slot, :, 128:256], spread) for slot in slots]
        top = jnp.maximum(jnp.maximum(logs[0], logs[1]), jnp.maximum(logs[2], logs[3]))
        weights = [jnp.exp(v - top) for v in logs]
        total = weights[0] + weights[1] + weights[2] + weights[3]
        acc = jnp.zeros((2 * ROWS, HEADS * VAL), f32)
        for slot, w in zip(slots, weights):
            acc = acc + got[slot, :, 0 : HEADS * VAL].astype(f32) * w
        own = mine[:, n * 64 : (n + 1) * 64]
        twin = theirs[:, n * 64 : (n + 1) * 64]
        pool = jnp.concatenate(
            [jnp.where(c == 0, own, twin), jnp.where(c == 0, twin, own)], axis=0
        )
        inputs.append(jnp.concatenate([(acc / total).astype(bf16), pool], axis=1))
    for copy in copies:
        copy.wait()
    for col in range(0, WIDTH, 512):
        cols = slice(col, col + 512)
        result = nn(inputs[0], wbuf[0, :, cols])
        for n in range(1, NY):
            result = result + nn(inputs[n], wbuf[n, :, cols])
        first, second = result[0:ROWS], result[ROWS:]
        keep[:, cols] = jnp.where(c == 0, first, second)
        send[:, cols] = jnp.where(c == 0, second, first).astype(bf16)


def project(got, mine, theirs, weights):
    return pl.pallas_call(
        project_body,
        in_specs=[vmem()] * 3 + [pl.BlockSpec(memory_space=pl.ANY)] * 6,
        out_specs=(vmem(), vmem()),
        out_shape=(
            pltpu.VMEM((ROWS, WIDTH), f32),
            pltpu.VMEM((ROWS, WIDTH), bf16),
        ),
        scratch_shapes=[
            pltpu.VMEM((NY, 256, WIDTH), bf16),
            pltpu.SemaphoreType.DMA((8,)),
        ],
        compiler_params=params(40),
        name="project",
    )(near(got), near(mine), near(theirs), *weights)


def across(x):
    return lax.ppermute(x, "c", [(0, 1), (1, 0)])


def shifted(x, axis, places):
    count = lax.axis_size(axis)
    return lax.ppermute(x, axis, [(i, (i + places) % count) for i in range(count)])


def shards(
    tokens,
    norm_gain,
    query_down_weight,
    query_latent_norm_gain,
    key_value_down_weight,
    key_value_latent_gain,
    w_rope_key,
    w_pool_in,
    query_up_weight,
    key_value_up_weight,
    query_gain,
    key_gain,
    w_pool_mix,
    pool_scale,
    w_out_attn,
    w_out_pool,
):
    wqt = query_up_weight.T

    q_all, kv_all, pool_in = latents(
        tokens,
        norm_gain,
        query_down_weight,
        query_latent_norm_gain,
        key_value_down_weight,
        key_value_latent_gain,
        w_rope_key,
        w_pool_in,
    )
    pieces = [q_all] + [shifted(q_all, "y", k) for k in range(1, NY)]
    kv_own = lax.all_to_all(kv_all, "z", 0, 0, tiled=True).reshape(NZ * (ROWS + 8), KR)

    count = NZ * NX * NY * 2
    every = ("z", "x", "y", "c")
    low = lax.ppermute(
        pool_in[ROWS - 8 :], every, [(i, i + 1) for i in range(count - 1)]
    )
    high = lax.ppermute(pool_in[:8], every, [(i + 1, i) for i in range(count - 1)])
    pool_mine, pool_send = pooling(pool_in, low, high)
    pool_theirs = across(pool_send)

    folded = jnp.dot(
        w_pool_mix[0],
        (pool_scale.astype(f32)[:, None] * w_out_pool.astype(f32)).astype(bf16),
        preferred_element_type=f32,
    ).astype(bf16)
    upper = w_out_attn[:128]
    lower = jnp.concatenate([w_out_attn[128:], folded], axis=0)
    upper1 = shifted(upper, "y", 1)
    lower3 = shifted(lower, "y", NY - 1)
    onward = jnp.concatenate([lower, upper1], axis=0)
    backward = jnp.concatenate([upper, lower3], axis=0)
    onward = shifted(onward, "y", 1)
    backward = shifted(backward, "y", NY - 1)
    pieces_w = (upper, lower, upper1, lower3, onward, backward)

    kv = lax.all_to_all(
        jnp.broadcast_to(kv_own[None], (NY, *kv_own.shape)), "y", 0, 0, tiled=True
    )
    q_side = jnp.concatenate(pieces, axis=0)
    q_own = [q_side] + [shifted(q_side, "x", k) for k in range(1, NX)]
    q_twin = [across(q) for q in q_own]
    kv_twin = across(kv)
    qt = queries(key_value_up_weight, q_own, q_twin, wqt, query_gain, query_tables())
    pair = keys_values((), kv, kv_twin, key_value_up_weight, key_gain, key_tables())
    message, *logs = attend(*pair, qt)

    got = lax.all_to_all(message, ("x", "y"), 0, 0, tiled=True)
    logs = [logs[0]] + [shifted(logs[k], "x", k) for k in range(1, NX)]
    row_logsum = logsums(logs)
    keep, send = project(got, pool_mine, pool_theirs, pieces_w)
    received = across(send)
    mixed = (keep + received.astype(f32)).astype(bf16)
    return mixed, row_logsum


def solution(mesh):
    fine = Mesh(mesh.devices.reshape(NZ, NX, NY, 2), ("z", "x", "y", "c"))
    tp = ("y", "c")
    placed = (
        P(("z", "x", "y", "c"), None),
        P(),
        P(),
        P(),
        P(),
        P(),
        P(),
        P(),
        P(None, tp),
        P(None, tp),
        P(),
        P(),
        P(tp, None, None),
        P(tp),
        P(tp, None),
        P(tp, None),
    )

    return jax.shard_map(
        shards,
        mesh=fine,
        in_specs=placed,
        out_specs=(P(("z", "x", "y", "c"), None), P(tp, ("z", "x"))),
        check_vma=False,
    )
```
